256 devices in a mesh: sp: 64 (over z, y, core), tp: 4 (over x).
Axes of the slice: x: 4, y: 4, z: 8, core: 2. Of those that a mesh axis runs over, the one named last changes fastest.
Arguments:
- tokens: bfloat16 [49152, 2048], P('sp'), may hold values from -6 to 6
- input_gain: bfloat16 [2048], replicated, may hold values from 0.099609375 to 1.8984375
- gate_weight: bfloat16 [2048, 2048], P('sp', 'tp'), may hold values from -0.125 to 0.125
- value_weight: bfloat16 [2048, 2048], P('sp', 'tp'), may hold values from -0.125 to 0.125
- inflow_weight: bfloat16 [2048, 4, 128], P('sp', 'tp'), may hold values from -0.125 to 0.125
- readout_weight: bfloat16 [2048, 4, 128], P('sp', 'tp'), may hold values from -0.125 to 0.125
- step_weight: bfloat16 [2048, 2, 32], P('sp', None, 'tp'), may hold values from -0.125 to 0.125
- conv_values: bfloat16 [5, 2048], P(None, 'tp'), may hold values from -2.5 to 2.5
- conv_inflow: bfloat16 [5, 4, 128], P(None, 'tp'), may hold values from -2.5 to 2.5
- conv_readout: bfloat16 [5, 4, 128], P(None, 'tp'), may hold values from -2.5 to 2.5
- log_rate: float32 [2, 49152, 32], P(None, 'sp', 'tp'), may hold values from -20 to 0
- group_gain: bfloat16 [2048], P('tp'), may hold values from 0.099609375 to 1.8984375
- query_weight: bfloat16 [2048, 2048], P('sp', 'tp'), may hold values from -8 to 8
- key_weight: bfloat16 [2048, 512], P('sp', 'tp'), may hold values from -8 to 8
- vector_weight: bfloat16 [2048, 512], P('sp', 'tp'), may hold values from -0.125 to 0.125
- sink_logit: float32 [32], P('tp'), may hold values from 3 to 7
- state_out: bfloat16 [2048, 2048], P('tp', 'sp'), may hold values from -0.125 to 0.125
- window_out: bfloat16 [2048, 2048], P('tp', 'sp'), may hold values from -1 to 1
Outputs:
- mixed: bfloat16 [49152, 2048], P('sp', 'tp')
- log_total: float32 [49152, 32], P('sp', 'tp')
The draws below stay inside these ranges and needn't reach their ends.
All inputs are finite; a program needn't handle non-finite values.
Results may differ from the reference program's by a relative error of at most 0.015.
The reference program's roundings to bfloat16 on the way count: a program that leaves them out, or rounds other values in their place, can miss the bound.
Values may be sent and summed in bfloat16 or wider, within the bound.
A program may use at most 128 MiB of HBM per device.

```python
import jax
import jax.numpy as jnp
from jax import lax

D = 2048
SSD_HEADS = 32
HEAD_DIM = 64
GROUPS = 4
STATE = 128
CONV = 5
SSD_BLOCK = 128
ATT_HEADS = 32
KV_HEADS = 8
WINDOW = 128
QBLOCK = 256
GRID_W = 64
TOK_DEV = 768
TOKENS = 49152
INNER = 2048
ATT_WIDTH = 2048
KV_WIDTH = 512
N_TP = 4


def shared_query(key):
    base = jax.random.normal(jax.random.fold_in(key, 11), (D, ATT_HEADS, HEAD_DIM), jnp.float32)
    return base * D ** (-0.5)


def draw_query_weight(key, part):
    base = jnp.clip(shared_query(key), -8.0, 8.0)
    return base.reshape(D, ATT_HEADS * HEAD_DIM).astype(jnp.bfloat16)


def draw_key_weight(key, part):
    fresh = jax.random.normal(jax.random.fold_in(key, 12), (D, KV_HEADS, HEAD_DIM), jnp.float32) * D ** (-0.5)
    return jnp.clip(fresh, -8.0, 8.0).reshape(D, KV_HEADS * HEAD_DIM).astype(jnp.bfloat16)


def draw_log_rate(key, part):
    tensor_shape = (2, TOKENS, SSD_HEADS)
    per_group = SSD_HEADS // GROUPS
    chance = 0.5
    ranking = jax.random.permutation(jax.random.fold_in(key, 20), GROUPS)
    quick_group = jax.random.uniform(jax.random.fold_in(key, 21), (GROUPS,), jnp.float32) < chance
    quick_group = jnp.where(ranking == 0, True, jnp.where(ranking == 1, False, quick_group))
    quick_level = jnp.broadcast_to(jnp.repeat(quick_group, per_group)[None, None, :], (2, 1, SSD_HEADS))
    fast_level = jnp.log(jax.random.uniform(jax.random.fold_in(key, 22), (2, 1, SSD_HEADS), jnp.float32, 1.0 / 100.0, 1.0 / 40.0))
    slow_level = jnp.log(jax.random.uniform(jax.random.fold_in(key, 23), (2, 1, SSD_HEADS), jnp.float32, 0.3, 1.5) / TOKENS)
    depth_level = jnp.where(quick_level, fast_level, slow_level)
    blocks = TOKENS // TOK_DEV
    offset_shift = jax.random.uniform(jax.random.fold_in(key, 24), (2, blocks, 1, SSD_HEADS), jnp.float32, -0.7, 0.7)
    offset_shift = jnp.broadcast_to(offset_shift, (2, blocks, TOK_DEV, SSD_HEADS)).reshape(tensor_shape)
    coarse_rough = jax.random.uniform(jax.random.fold_in(key, 25), tensor_shape, jnp.float32, -0.3, 0.3)
    label_marks = jax.random.randint(jax.random.fold_in(key, 26), (1, TOKENS, 1), 0, TOKENS) < 6
    spike_amount = jnp.log(jax.random.uniform(jax.random.fold_in(key, 27), tensor_shape, jnp.float32, 0.3, 1.0))
    final_result = jnp.where(label_marks & jnp.logical_not(quick_level), spike_amount, depth_level + offset_shift + coarse_rough)
    return jnp.clip(final_result, -20.0, 0.0)


def steps_of(own_key, dims, split, least, top_value):
    def one(axis_at, shards_of):
        draws = jax.random.uniform(jax.random.fold_in(jax.random.fold_in(own_key, 6), axis_at), (shards_of,), jnp.float32, least / len(split), top_value / len(split))
        return jnp.repeat(jnp.exp(draws), dims[axis_at] // shards_of).reshape((-1,) + (1,) * (len(dims) - axis_at - 1))

    factor_of = one(*split[0])
    for cut in split[1:]:
        factor_of = factor_of * one(*cut)
    return factor_of


def centred(key, shape, scale, bound, shards=(), kind=jnp.bfloat16):
    factor_of = steps_of(key, shape, shards, -0.22, 0.18) if shards else 1.0
    array = jax.random.normal(key, shape, jnp.float32) * scale * factor_of
    return jnp.minimum(jnp.maximum(array, -bound), bound).astype(kind)


def setup_inputs(seed: int = 0) -> dict:
    key_list = jax.random.split(jax.random.key(seed), 19)
    tokens = centred(key_list[0], (TOKENS, D), 1.0, 6.0, ((0, 64),))
    input_gain = jnp.clip(1.0 + 0.18 * jax.random.normal(key_list[1], (D,), jnp.float32), 0.099609375, 1.8984375).astype(jnp.bfloat16)
    gate_weight = centred(key_list[2], (D, INNER), D ** -0.5, 0.125, ((0, 64), (1, 4)))
    value_weight = centred(key_list[3], (D, INNER), D ** -0.5, 0.125, ((0, 64), (1, 4)))
    inflow_weight = centred(key_list[4], (D, GROUPS, STATE), D ** -0.5, 0.125, ((0, 64), (1, 4)))
    readout_weight = centred(key_list[5], (D, GROUPS, STATE), D ** -0.5, 0.125, ((0, 64), (1, 4)))
    step_weight = centred(key_list[6], (D, 2, SSD_HEADS), D ** -0.5, 0.125, ((0, 64), (2, 4)))
    conv_values = centred(key_list[7], (CONV, INNER), CONV ** -0.5, 2.5, ((1, 4),))
    conv_inflow = centred(key_list[8], (CONV, GROUPS, STATE), CONV ** -0.5, 2.5, ((1, 4),))
    conv_readout = centred(key_list[9], (CONV, GROUPS, STATE), CONV ** -0.5, 2.5, ((1, 4),))
    log_rate = draw_log_rate(jax.random.fold_in(key_list[18], 71), 0)
    group_gain = jnp.clip(1.0 + 0.18 * jax.random.normal(key_list[11], (INNER,), jnp.float32), 0.099609375, 1.8984375).astype(jnp.bfloat16)
    query_weight = draw_query_weight(jax.random.fold_in(key_list[18], 71), 0)
    key_weight = draw_key_weight(jax.random.fold_in(key_list[18], 71), 0)
    vector_weight = centred(key_list[14], (D, KV_WIDTH), D ** -0.5, 0.125, ((0, 64), (1, 4)))
    sink_logit = jnp.clip(3.0 + 4.0 * jax.random.uniform(key_list[15], (ATT_HEADS,), jnp.float32) ** steps_of(key_list[15], (ATT_HEADS,), ((0, 4),), -0.2, 0.2), 3.0, 7.0)
    state_out = centred(key_list[16], (INNER, D), INNER ** -0.5, 0.125, ((0, 4), (1, 64)))
    window_out = centred(key_list[17], (ATT_WIDTH, D), (ATT_WIDTH // 64) ** -0.5, 1.0, ((0, 4), (1, 64)))
    return {"tokens": tokens, "input_gain": input_gain, "gate_weight": gate_weight, "value_weight": value_weight, "inflow_weight": inflow_weight, "readout_weight": readout_weight, "step_weight": step_weight, "conv_values": conv_values, "conv_inflow": conv_inflow, "conv_readout": conv_readout, "log_rate": log_rate, "group_gain": group_gain, "query_weight": query_weight, "key_weight": key_weight, "vector_weight": vector_weight, "sink_logit": sink_logit, "state_out": state_out, "window_out": window_out}


EPS = 1e-06
ROPE_BASE = 10000.0
HIGH = lax.Precision.HIGH

def rope_pairs(part, angle):
    half = part.shape[-1] // 2
    cosine = jnp.cos(angle)[:, None, :]
    sine = jnp.sin(angle)[:, None, :]
    first = part[..., :half]
    second = part[..., half:]
    return jnp.concatenate([first * cosine - second * sine, second * cosine + first * sine], axis=-1)

def axial_rope(heads, positions):
    width = heads.shape[-1]
    quarter = width // 4
    freqs = ROPE_BASE ** (-jnp.arange(quarter).astype(jnp.float32) / quarter)
    row_angle = (positions // GRID_W).astype(jnp.float32)[:, None] * freqs
    col_angle = (positions % GRID_W).astype(jnp.float32)[:, None] * freqs
    half = width // 2
    wide = heads.astype(jnp.float32)
    turned = jnp.concatenate([rope_pairs(wide[..., :half], row_angle), rope_pairs(wide[..., half:], col_angle)], axis=-1)
    return turned.astype(jnp.bfloat16)

def block_ssd(state, inputs):
    xdt, decay, inflow, readout = inputs
    length = decay.shape[0]
    heads = xdt.shape[1]
    groups = inflow.shape[1]
    repeat = heads // groups
    cum = jnp.cumsum(decay, axis=0)
    seg = cum[:, None, :] - cum[None, :, :]
    lower = jnp.arange(length)[:, None] >= jnp.arange(length)[None, :]
    weight = jnp.exp(jnp.where(lower[:, :, None], seg, -jnp.inf))
    intersection = jnp.einsum('lgn,sgn->lsg', readout.astype(jnp.bfloat16), inflow.astype(jnp.bfloat16), preferred_element_type=jnp.float32)
    intersection = jnp.repeat(intersection, repeat, axis=2)
    final_result = jnp.einsum('lsh,shp->lhp', intersection * weight, xdt, precision=HIGH)
    read_heads = jnp.repeat(readout, repeat, axis=1)
    final_result = final_result + jnp.exp(cum)[:, :, None] * jnp.einsum('lhn,hpn->lhp', read_heads, state, precision=HIGH)
    write_heads = jnp.repeat(inflow, repeat, axis=1)
    to_end = jnp.exp(cum[-1][None, :] - cum)
    fresh = jnp.einsum('shp,shn->hpn', xdt * to_end[:, :, None], write_heads, precision=HIGH)
    return (jnp.exp(cum[-1])[:, None, None] * state + fresh, final_result)

def run_blocks(xdt, decay, inflow, readout):
    count = decay.shape[0]
    blocks = count // SSD_BLOCK
    start_state = jnp.zeros((SSD_HEADS, HEAD_DIM, STATE), jnp.float32)
    shaped = (xdt.reshape(blocks, SSD_BLOCK, SSD_HEADS, HEAD_DIM), decay.reshape(blocks, SSD_BLOCK, SSD_HEADS), inflow.reshape(blocks, SSD_BLOCK, GROUPS, STATE), readout.reshape(blocks, SSD_BLOCK, GROUPS, STATE))
    final_state, final_result = lax.scan(block_ssd, start_state, shaped)
    return final_result.reshape(count, SSD_HEADS, HEAD_DIM)

def reference(tokens, input_gain, gate_weight, value_weight, inflow_weight, readout_weight, step_weight, conv_values, conv_inflow, conv_readout, log_rate, group_gain, query_weight, key_weight, vector_weight, sink_logit, state_out, window_out):
    count = tokens.shape[0]
    wide = tokens.astype(jnp.float32)
    normed = (wide * lax.rsqrt(lax.optimization_barrier(jnp.mean(wide * wide, axis=1, keepdims=True)) + EPS) * input_gain.astype(jnp.float32)).astype(jnp.bfloat16)

    def project(weight):
        return jnp.dot(normed, weight.reshape(weight.shape[0], -1), preferred_element_type=jnp.float32)
    gate = project(gate_weight).astype(jnp.bfloat16)
    conv_input = jnp.concatenate([project(value_weight), project(inflow_weight), project(readout_weight)], axis=1).astype(jnp.bfloat16)
    step = jax.nn.softplus(project(step_weight)).reshape(count, 2, SSD_HEADS)
    taps = jnp.concatenate([conv_values, conv_inflow.reshape(CONV, -1), conv_readout.reshape(CONV, -1)], axis=1).astype(jnp.float32)
    reach = CONV // 2
    padded = jnp.pad(conv_input.astype(jnp.float32), ((reach, reach), (0, 0)))
    conv_sum = padded[0:count] * taps[0]
    for tap in range(1, CONV):
        conv_sum = conv_sum + padded[tap:tap + count] * taps[tap]
    conv_out = lax.optimization_barrier(jax.nn.silu(conv_sum).astype(jnp.bfloat16)).astype(jnp.float32)
    xs = conv_out[:, :INNER].reshape(count, SSD_HEADS, HEAD_DIM)
    inflow = conv_out[:, INNER:INNER + GROUPS * STATE].reshape(count, GROUPS, STATE)
    readout = conv_out[:, INNER + GROUPS * STATE:].reshape(count, GROUPS, STATE)
    decay = -jnp.exp(log_rate) * jnp.transpose(step, (1, 0, 2))
    forward = run_blocks(xs * step[:, 0, :, None], decay[0], inflow, readout)
    backward = jnp.flip(run_blocks(jnp.flip(xs * step[:, 1, :, None], 0), jnp.flip(decay[1], 0), jnp.flip(inflow, 0), jnp.flip(readout, 0)), 0)
    combined = (forward + backward).reshape(count, INNER) * jax.nn.silu(gate.astype(jnp.float32))
    grouped = combined.reshape(count, GROUPS, -1)
    grouped = grouped * lax.rsqrt(lax.optimization_barrier(jnp.mean(grouped * grouped, axis=2, keepdims=True)) + EPS)
    state_features = (grouped.reshape(count, INNER) * group_gain.astype(jnp.float32)).astype(jnp.bfloat16)
    repeat = ATT_HEADS // KV_HEADS
    positions = jnp.arange(count, dtype=jnp.int32)
    queries = axial_rope(project(query_weight).astype(jnp.bfloat16).reshape(count, ATT_HEADS, HEAD_DIM), positions)
    keys = axial_rope(project(key_weight).astype(jnp.bfloat16).reshape(count, KV_HEADS, HEAD_DIM), positions)
    vectors = project(vector_weight).astype(jnp.bfloat16).reshape(count, KV_HEADS, HEAD_DIM)
    key_pad = jnp.pad(keys, ((WINDOW, WINDOW), (0, 0), (0, 0)))
    vector_pad = jnp.pad(vectors, ((WINDOW, WINDOW), (0, 0), (0, 0)))
    grouped_q = queries.reshape(count, KV_HEADS, repeat, HEAD_DIM)
    band = QBLOCK + 2 * WINDOW
    sinks = sink_logit.reshape(KV_HEADS, repeat, 1, 1)

    def attend(index):
        start = (index * QBLOCK).astype(jnp.int32)
        block_q = lax.dynamic_slice_in_dim(grouped_q, start, QBLOCK, 0).astype(jnp.float32)
        block_k = lax.dynamic_slice_in_dim(key_pad, start, band, 0).astype(jnp.float32)
        block_v = lax.dynamic_slice_in_dim(vector_pad, start, band, 0).astype(jnp.float32)
        scores = jnp.einsum('qkrd,skd->krqs', block_q, block_k) * HEAD_DIM ** (-0.5)
        query_pos = start + jnp.arange(QBLOCK, dtype=jnp.int32)
        key_pos = start - WINDOW + jnp.arange(band, dtype=jnp.int32)
        valid = (jnp.abs(query_pos[:, None] - key_pos[None, :]) <= WINDOW) & (key_pos >= 0)[None, :] & (key_pos < count)[None, :]
        scores = jnp.where(valid, scores, -jnp.inf)
        top = jnp.maximum(lax.optimization_barrier(jnp.max(scores, axis=-1, keepdims=True)), sinks)
        expo = jnp.exp(scores - top)
        total = lax.optimization_barrier(jnp.sum(expo, axis=-1, keepdims=True)) + jnp.exp(sinks - top)
        probs = lax.optimization_barrier(expo.astype(jnp.bfloat16)).astype(jnp.float32)
        values = jnp.einsum('krqs,skd->qkrd', probs, block_v) / jnp.transpose(total, (2, 0, 1, 3))
        logs = jnp.transpose((top + jnp.log(total))[..., 0], (2, 0, 1)).reshape(QBLOCK, -1)
        return (values.astype(jnp.bfloat16).reshape(QBLOCK, -1), logs)
    feats, logs = lax.map(attend, jnp.arange(count // QBLOCK, dtype=jnp.int32))
    window_features = feats.reshape(count, ATT_WIDTH)
    log_total = logs.reshape(count, ATT_HEADS)
    state_cols = INNER // N_TP
    window_cols = ATT_WIDTH // N_TP
    summed = jnp.zeros((count, D), jnp.float32)
    for group in range(N_TP):
        part = jnp.dot(state_features[:, group * state_cols:(group + 1) * state_cols], state_out[group * state_cols:(group + 1) * state_cols], preferred_element_type=jnp.float32)
        part = part + jnp.dot(window_features[:, group * window_cols:(group + 1) * window_cols], window_out[group * window_cols:(group + 1) * window_cols], preferred_element_type=jnp.float32)
        summed = summed + lax.optimization_barrier(part.astype(jnp.bfloat16)).astype(jnp.float32)
    return (summed.astype(jnp.bfloat16), log_total)
```

```python
import functools

import jax
import jax.numpy as jnp
from jax import lax
from jax.experimental import pallas as pl
from jax.experimental.pallas import tpu as pltpu
from jax.sharding import Mesh
from jax.sharding import PartitionSpec as P

HEAD_DIM = 64
STATE = 128
HEADS = 8
BLOCK = 128
WINDOW = 128
GRID_W = 64
HALO = 16
SP = ("sp_0", "sp_1", "sp_2")
EPS = 1e-06
ROPE_BASE = 10000.0
F32 = jnp.float32
BF16 = jnp.bfloat16
MSG = STATE + 16


def dot(a, b, dims=((1,), (0,)), precision=None):
    return lax.dot_general(
        a, b, (dims, ((), ())), preferred_element_type=F32, precision=precision
    )


def split_bf16(value, parts):
    pieces = []
    for _ in range(parts):
        piece = value.astype(BF16)
        pieces.append(piece)
        value = value - piece.astype(F32)
    return pieces


def spread(value, spread_matrix, parts):
    pieces = [p.astype(F32) for p in split_bf16(value, parts)]
    joined = jnp.concatenate(pieces, axis=1).astype(BF16)
    matrix = jnp.concatenate([spread_matrix] * parts, axis=0)
    return dot(joined, matrix)


def spread_matrix():
    rows = jnp.arange(2 * HEADS)[:, None]
    cols = jnp.arange(2 * HEADS * HEAD_DIM)[None, :] // HEAD_DIM
    return (rows == cols).astype(BF16)


def project_kernel(tok_ref, gain_ref, w_ref, ws_ref, out_ref, step_ref, normed):
    @pl.when(pl.program_id(0) == 0)
    def _():
        def one(i, carry):
            rows = pl.ds(i * BLOCK, BLOCK)
            wide = tok_ref[rows, :].astype(F32)
            scale = lax.rsqrt(jnp.mean(wide * wide, axis=1, keepdims=True) + EPS)
            normed[rows, :] = (wide * scale * gain_ref[...]).astype(BF16)
            return carry

        lax.fori_loop(0, tok_ref.shape[0] // BLOCK, one, 0)
        step_ref[...] = dot(normed[...], ws_ref[...])

    out_ref[...] = dot(normed[...], w_ref[...]).astype(BF16)


def project(tokens, gain, weights, step_weights):
    count, width = tokens.shape
    columns = weights.shape[1]
    tile = 256
    return pl.pallas_call(
        project_kernel,
        grid=(columns // tile,),
        in_specs=[
            pl.BlockSpec((count, width), lambda j: (0, 0), pipeline_mode=pl.Buffered(1)),
            pl.BlockSpec((1, width), lambda j: (0, 0)),
            pl.BlockSpec((width, tile), lambda j: (0, j)),
            pl.BlockSpec((width, 128), lambda j: (0, 0), pipeline_mode=pl.Buffered(1)),
        ],
        out_specs=[
            pl.BlockSpec((count, tile), lambda j: (0, j)),
            pl.BlockSpec((count, 128), lambda j: (0, 0)),
        ],
        out_shape=[
            jax.ShapeDtypeStruct((count, columns), BF16),
            jax.ShapeDtypeStruct((count, 128), F32),
        ],
        scratch_shapes=[pltpu.VMEM((count, width), BF16)],
        compiler_params=pltpu.CompilerParams(vmem_limit_bytes=16 << 20),
        cost_estimate=pl.CostEstimate(
            flops=2 * count * width * (columns + 128),
            bytes_accessed=2 * (count * width + width * columns + count * columns),
            transcendentals=0,
        ),
        name="project",
    )(tokens, gain, weights, step_weights)


def conv_state_kernel(
    cin_ref, before_ref, after_ref, taps_ref, step_ref, rate_ref, e_ref,
    conv_ref, col_ref, row_ref, piece_ref, etot_ref, msg_ref, win, near,
):
    count = cin_ref.shape[0]
    blocks = count // BLOCK
    channels = HEADS * HEAD_DIM
    spread_m = e_ref[...]
    lane16 = lax.broadcasted_iota(jnp.int32, (BLOCK, 2 * HEADS), 1)
    forward16 = lane16 < HEADS
    tri = (
        lax.broadcasted_iota(jnp.int32, (BLOCK, BLOCK), 0)
        >= lax.broadcasted_iota(jnp.int32, (BLOCK, BLOCK), 1)
    ).astype(F32)
    win[pl.ds(0, HALO), :] = before_ref[...].astype(F32)
    win[pl.ds(HALO + count, HALO), :] = after_ref[...].astype(F32)

    def fill(i, carry):
        start = pl.multiple_of(i * BLOCK, BLOCK)
        win[pl.ds(HALO + start, BLOCK), :] = cin_ref[pl.ds(start, BLOCK), :].astype(F32)
        return carry

    lax.fori_loop(0, blocks, fill, 0)

    def one(i, total):
        start = pl.multiple_of(i * BLOCK, BLOCK)
        rows = pl.ds(start, BLOCK)
        near[...] = win[pl.ds(start, BLOCK + 2 * HALO), :]
        acc = near[HALO - 2 : HALO - 2 + BLOCK, :] * taps_ref[0:1, :]
        for tap in range(1, 5):
            first = HALO - 2 + tap
            acc = acc + near[first : first + BLOCK, :] * taps_ref[tap : tap + 1, :]
        conv = (acc * jax.nn.sigmoid(acc)).astype(BF16)
        conv_ref[rows, :] = conv
        raw = step_ref[rows, 0 : 2 * HEADS]
        step = jnp.maximum(raw, 0.0) + jnp.log1p(jnp.exp(-jnp.abs(raw)))
        decay = -jnp.exp(rate_ref[rows, :]) * step
        cum = dot(tri, decay, precision=lax.Precision.HIGHEST)
        tot = cum[BLOCK - 1 : BLOCK, :]
        col = jnp.where(forward16, cum, cum - decay)
        col_ref[rows, 0 : 2 * HEADS] = col
        col_ref[rows, 2 * HEADS : 4 * HEADS] = jnp.broadcast_to(tot, (BLOCK, 2 * HEADS))
        both = jnp.concatenate([col, step, jnp.zeros((BLOCK, 128 - 4 * HEADS), F32)], axis=1)
        row_ref[i] = both.T[0 : 4 * HEADS, :]
        weight = jnp.exp(jnp.where(forward16, tot - col, col)) * step
        wide = spread(weight, spread_m, 2)
        xs = conv[:, 0:channels].astype(F32)
        scaled = (jnp.concatenate([xs, xs], axis=1) * wide).astype(BF16)
        inflow = conv[:, channels : channels + STATE]
        piece_ref[i] = dot(inflow, scaled, ((0,), (0,)))
        etot_ref[i] = spread(jnp.exp(jnp.broadcast_to(tot, (8, 2 * HEADS))), spread_m, 3)
        return total + tot

    total = lax.fori_loop(0, blocks, one, jnp.zeros((1, 2 * HEADS), F32))
    forward = piece_ref[0, :, 0:channels]
    backward = piece_ref[blocks - 1, :, channels : 2 * channels]
    for i in range(1, blocks):
        forward = etot_ref[i, 0:1, 0:channels] * forward + piece_ref[i, :, 0:channels]
        k = blocks - 1 - i
        backward = (
            etot_ref[k, 0:1, channels : 2 * channels] * backward
            + piece_ref[k, :, channels : 2 * channels]
        )
    spread_total = spread(jnp.broadcast_to(total, (16, 2 * HEADS)), spread_m, 3)
    hi, mid, lo = split_bf16(spread_total, 3)
    which = lax.broadcasted_iota(jnp.int32, (16, 2 * channels), 0)
    tail = jnp.where(
        which == 0, hi.astype(F32), jnp.where(which == 1, mid.astype(F32), lo.astype(F32))
    ).astype(BF16)
    for e, state in enumerate((forward, backward)):
        for pair in range(channels // 128):
            lanes = slice(pair * 128, pair * 128 + 128)
            msg_ref[e, pair, 0:STATE, :] = state[:, lanes].astype(BF16)
            msg_ref[e, pair, STATE:MSG, :] = tail[:, e * channels + pair * 128 : e * channels + pair * 128 + 128]


def conv_state(proj, before, after, taps, step_raw, rate, spread_m):
    count = proj.shape[0]
    width = before.shape[1]
    blocks = count // BLOCK
    channels = HEADS * HEAD_DIM
    whole = lambda shape: pl.BlockSpec(shape, lambda i: (0,) * len(shape))
    return pl.pallas_call(
        conv_state_kernel,
        grid=(1,),
        in_specs=[
            pl.BlockSpec((count, width), lambda i: (0, 0)),
            whole((HALO, width)),
            whole((HALO, width)),
            whole(taps.shape),
            whole(step_raw.shape),
            whole(rate.shape),
            whole(spread_m.shape),
        ],
        out_specs=[
            whole((count, width)),
            whole((count, 4 * HEADS)),
            whole((blocks, 4 * HEADS, BLOCK)),
            whole((blocks, STATE, 2 * channels)),
            whole((blocks, 8, 2 * channels)),
            whole((2, channels // 128, MSG, 128)),
        ],
        out_shape=[
            jax.ShapeDtypeStruct((count, width), BF16),
            jax.ShapeDtypeStruct((count, 4 * HEADS), F32),
            jax.ShapeDtypeStruct((blocks, 4 * HEADS, BLOCK), F32),
            jax.ShapeDtypeStruct((blocks, STATE, 2 * channels), F32),
            jax.ShapeDtypeStruct((blocks, 8, 2 * channels), F32),
            jax.ShapeDtypeStruct((2, channels // 128, MSG, 128), BF16),
        ],
        scratch_shapes=[
            pltpu.VMEM((count + 2 * HALO, width), F32),
            pltpu.VMEM((BLOCK + 2 * HALO, width), F32),
        ],
        compiler_params=pltpu.CompilerParams(vmem_limit_bytes=18 << 20),
        cost_estimate=pl.CostEstimate(
            flops=2 * count * STATE * 2 * channels, bytes_accessed=12 << 20, transcendentals=0
        ),
        name="conv_state",
    )(proj, before, after, taps, step_raw, rate, spread_m)


def mix_kernel(
    conv_ref, col_ref, row_ref, piece_ref, etot_ref, in_ref, gate_ref, gain_ref, e_ref,
    out_ref, held,
):
    count = conv_ref.shape[0]
    blocks = count // BLOCK
    channels = HEADS * HEAD_DIM
    spread_m = e_ref[...]
    for e in range(2):
        state = jnp.concatenate(
            [in_ref[e, p].astype(F32) for p in range(channels // 128)], axis=1
        )
        lanes = slice(e * channels, (e + 1) * channels)
        for i in range(blocks) if e == 0 else reversed(range(blocks)):
            held[i, :, lanes] = state.astype(BF16)
            state = etot_ref[i, 0:1, lanes] * state + piece_ref[i, :, lanes]
    row_at = lax.broadcasted_iota(jnp.int32, (BLOCK, BLOCK), 0)
    col_at = lax.broadcasted_iota(jnp.int32, (BLOCK, BLOCK), 1)
    lower = row_at >= col_at
    diagonal = row_at == col_at
    first_half = col_at < HEAD_DIM
    forward16 = lax.broadcasted_iota(jnp.int32, (BLOCK, 2 * HEADS), 1) < HEADS

    def one(i, carry):
        rows = pl.ds(pl.multiple_of(i * BLOCK, BLOCK), BLOCK)
        inflow = conv_ref[rows, channels : channels + STATE]
        readout = conv_ref[rows, channels + STATE : channels + 2 * STATE]
        inner = dot(readout, inflow, ((1,), (1,)))
        col = col_ref[rows, 0 : 2 * HEADS]
        tot = col_ref[rows, 2 * HEADS : 4 * HEADS]
        reach = spread(jnp.exp(jnp.where(forward16, col, tot - col)), spread_m, 2)
        far = dot(readout, held[i]) * reach
        parts = []
        for pair in range(HEADS // 2):
            weights = []
            for h in (2 * pair, 2 * pair + 1):
                b = HEADS + h
                arg = jnp.where(
                    lower,
                    col[:, h : h + 1] - row_ref[i, h : h + 1, :],
                    row_ref[i, b : b + 1, :] - col[:, b : b + 1],
                )
                step_f = row_ref[i, 2 * HEADS + h : 2 * HEADS + h + 1, :]
                step_b = row_ref[i, 2 * HEADS + b : 2 * HEADS + b + 1, :]
                step = jnp.where(lower, step_f, step_b) + jnp.where(diagonal, step_b, 0.0)
                weights.append((inner * jnp.exp(arg) * step).astype(BF16))
            xs = conv_ref[rows, pair * 128 : pair * 128 + 128]
            zero = jnp.zeros_like(xs)
            stacked = jnp.concatenate(
                [jnp.where(first_half, xs, zero), jnp.where(first_half, zero, xs)], axis=0
            )
            parts.append(dot(jnp.concatenate(weights, axis=1), stacked))
        y = jnp.concatenate(parts, axis=1) + far[:, 0:channels] + far[:, channels:]
        gate = gate_ref[rows, :].astype(F32)
        y = y * (gate * jax.nn.sigmoid(gate))
        y = y * lax.rsqrt(jnp.mean(y * y, axis=1, keepdims=True) + EPS)
        out_ref[rows, :] = (y * gain_ref[...]).astype(BF16)
        return carry

    lax.fori_loop(0, blocks, one, 0)


def mix(conv, col, row, piece, etot, incoming, proj, gate_block, gain, spread_m):
    count = conv.shape[0]
    blocks = count // BLOCK
    channels = HEADS * HEAD_DIM
    whole = lambda shape: pl.BlockSpec(shape, lambda i: (0,) * len(shape))
    return pl.pallas_call(
        mix_kernel,
        grid=(1,),
        in_specs=[
            whole(conv.shape), whole(col.shape), whole(row.shape), whole(piece.shape),
            whole(etot.shape), whole(incoming.shape),
            pl.BlockSpec((count, channels), lambda i: (0, gate_block)),
            whole(gain.shape), whole(spread_m.shape),
        ],
        out_specs=whole((count, channels)),
        out_shape=jax.ShapeDtypeStruct((count, channels), BF16),
        scratch_shapes=[pltpu.VMEM((blocks, STATE, 2 * channels), BF16)],
        compiler_params=pltpu.CompilerParams(vmem_limit_bytes=16 << 20),
        cost_estimate=pl.CostEstimate(
            flops=2 * count * BLOCK * 4 * channels, bytes_accessed=8 << 20, transcendentals=0
        ),
        name="mix",
    )(conv, col, row, piece, etot, incoming, proj, gain, spread_m)


def rope_tables(first_row, grid_rows):
    quarter = HEAD_DIM // 4
    lane = jnp.arange(2 * HEAD_DIM)
    freqs = ROPE_BASE ** (-(lane % quarter).astype(F32) / quarter)
    sign = jnp.where(lane % (2 * quarter) < quarter, -1.0, 1.0)
    row_angle = (first_row + jnp.arange(grid_rows, dtype=jnp.int32)).astype(F32)[:, None] * freqs
    col_angle = jnp.arange(GRID_W, dtype=jnp.int32).astype(F32)[:, None] * freqs
    return (
        jnp.stack([jnp.cos(row_angle), jnp.sin(row_angle) * sign]),
        jnp.stack([jnp.cos(col_angle), jnp.sin(col_angle) * sign]),
    )


def attend_kernel(
    at_ref, q_ref, kv_ref, before_ref, after_ref, by_row_ref, by_col_ref, sink_ref,
    out_ref, log_ref, keys, values,
):
    count = kv_ref.shape[0]
    blocks = count // BLOCK
    lane = lax.broadcasted_iota(jnp.int32, (BLOCK, 128), 1)
    low_quarter = lane % 32 < 16
    first_half = lane < HEAD_DIM
    row_lane = (lane % HEAD_DIM < 32)[0:GRID_W]

    def tables(slot):
        out = []
        for kind in range(2):
            parts = []
            for r in range(BLOCK // GRID_W):
                row = by_row_ref[kind, pl.ds(slot * (BLOCK // GRID_W) + r, 1), :]
                parts.append(jnp.where(row_lane, row, by_col_ref[kind]))
            out.append(jnp.concatenate(parts, axis=0))
        return out

    def turn(value, table):
        wide = value.astype(F32)
        other = jnp.where(low_quarter, pltpu.roll(wide, 112, 1), pltpu.roll(wide, 16, 1))
        return (wide * table[0] + other * table[1]).astype(BF16)

    def store(raw, slot):
        rows = pl.ds(pl.multiple_of(slot * BLOCK, BLOCK), BLOCK)
        key = turn(raw[:, 0:128], tables(slot)).astype(F32)
        swapped = pltpu.roll(key, 64, 1)
        keys[0, rows, :] = jnp.where(first_half, key, swapped).astype(BF16)
        keys[1, rows, :] = jnp.where(first_half, swapped, key).astype(BF16)
        values[:, rows] = raw[:, 128:256].astype(F32).T.astype(BF16)

    store(before_ref[...], 0)
    store(after_ref[...], blocks + 1)

    def fill(i, carry):
        store(kv_ref[pl.ds(pl.multiple_of(i * BLOCK, BLOCK), BLOCK), :], i + 1)
        return carry

    lax.fori_loop(0, blocks, fill, 0)
    key_at = lax.broadcasted_iota(jnp.int32, (3 * BLOCK, 2 * BLOCK), 0)
    query_at = lax.broadcasted_iota(jnp.int32, (3 * BLOCK, 2 * BLOCK), 1) % BLOCK
    in_band = (key_at >= query_at) & (key_at <= query_at + 2 * WINDOW)
    start_at = at_ref[0]
    end_at = at_ref[1]

    def one(i, carry):
        start = pl.multiple_of(i * BLOCK, BLOCK)
        rows = pl.ds(start, BLOCK)
        here = key_at + (start - WINDOW)
        valid = in_band & (here >= start_at) & (here < end_at)
        table = tables(i + 1)
        band = pl.ds(start, 3 * BLOCK)
        for pair in range(HEADS // 2):
            group = pair // 2
            lanes = slice(pair * 128, pair * 128 + 128)
            q = (turn(q_ref[rows, lanes], table).astype(F32) * HEAD_DIM ** (-0.5)).astype(BF16)
            zero = jnp.zeros_like(q)
            both = jnp.concatenate(
                [jnp.where(first_half, q, zero), jnp.where(first_half, zero, q)], axis=0
            )
            scores = dot(keys[group, band, :], both, ((1,), (1,)))
            scores = jnp.where(valid, scores, -1e30)
            sink = sink_ref[pair : pair + 1, :]
            top = jnp.maximum(jnp.max(scores, axis=0, keepdims=True), sink)
            expo = jnp.exp(scores - top)
            total = jnp.sum(expo, axis=0, keepdims=True) + jnp.exp(sink - top)
            mine = values[group * HEAD_DIM : (group + 1) * HEAD_DIM, band]
            o = dot(mine, expo.astype(BF16)) / total
            turned = jnp.concatenate([o[:, 0:BLOCK], o[:, BLOCK:]], axis=0).T
            out_ref[rows, lanes] = turned.astype(BF16)
            log = top + jnp.log(total)
            log_ref[2 * pair : 2 * pair + 1, rows] = log[:, 0:BLOCK]
            log_ref[2 * pair + 1 : 2 * pair + 2, rows] = log[:, BLOCK:]
        return carry

    lax.fori_loop(0, blocks, one, 0)


def attend(limits, proj, q_block, kv_block, before, after, tables, sinks):
    count = proj.shape[0]
    channels = HEADS * HEAD_DIM
    whole = lambda shape: pl.BlockSpec(shape, lambda i, *_: (0,) * len(shape))
    smem = pl.BlockSpec(memory_space=pltpu.SMEM)
    by_row, by_col = tables
    wide_sinks = jnp.repeat(sinks.reshape(HEADS // 2, 2), BLOCK, axis=1)
    return pl.pallas_call(
        attend_kernel,
        grid=(1,),
        in_specs=[
            smem,
            pl.BlockSpec((count, channels), lambda i: (0, q_block)),
            pl.BlockSpec((count, 256), lambda i: (0, kv_block)),
            whole(before.shape), whole(after.shape), whole(by_row.shape), whole(by_col.shape),
            whole(wide_sinks.shape),
        ],
        out_specs=[whole((count, channels)), whole((HEADS, count))],
        out_shape=[
            jax.ShapeDtypeStruct((count, channels), BF16),
            jax.ShapeDtypeStruct((HEADS, count), F32),
        ],
        scratch_shapes=[
            pltpu.VMEM((2, count + 2 * BLOCK, 128), BF16),
            pltpu.VMEM((128, count + 2 * BLOCK), BF16),
        ],
        compiler_params=pltpu.CompilerParams(vmem_limit_bytes=12 << 20),
        cost_estimate=pl.CostEstimate(
            flops=4 * count * 3 * BLOCK * channels, bytes_accessed=4 << 20, transcendentals=0
        ),
        name="attend",
    )(limits, proj, proj, before, after, by_row, by_col, wide_sinks)


def exchange_kernel(
    msg_ref, out_ref, part, turned, by_y, summed, by_z, back, arrived, nxt, final, carry,
    part_sem, y_sem, z_sem, back_sem, final_sem,
):
    z, y, c = (lax.axis_index(a) for a in SP)
    length_z, length_y = lax.axis_size(SP[0]), lax.axis_size(SP[1])
    forward = c == 0
    other = 1 - c
    order_z = jnp.where(forward, z, length_z - 1 - z)
    mesh_id = pl.DeviceIdType.MESH
    peers = [{SP[2]: other}]
    peers += [{SP[1]: lax.rem(y + k, length_y)} for k in range(1, length_y)]
    peers += [{SP[0]: lax.rem(z + k, length_z)} for k in range(1, length_z)]
    barrier = pltpu.get_barrier_semaphore()
    for peer in peers:
        pl.semaphore_signal(barrier, inc=1, device_id=peer, device_id_type=mesh_id)
    pl.semaphore_wait(barrier, len(peers))

    def send(src, dst, sems, peer):
        copy = pltpu.make_async_remote_copy(
            src_ref=src, dst_ref=dst, send_sem=sems.at[0], recv_sem=sems.at[1],
            device_id=peer, device_id_type=mesh_id,
        )
        copy.start()
        return copy

    def state_of(ref, *at):
        return ref[(*at, slice(0, STATE), slice(None))].astype(F32)

    def decay_of(ref, *at):
        tail = ref[(*at, slice(STATE, MSG), slice(None))].astype(F32)
        return tail[0:1] + tail[1:2] + tail[2:3]

    def put(ref, state, decay, *at):
        ref[(*at, slice(0, STATE), slice(None))] = state.astype(BF16)
        hi, mid, lo = (p.astype(F32) for p in split_bf16(decay, 3))
        which = lax.broadcasted_iota(jnp.int32, (MSG - STATE, 128), 0)
        tail = jnp.where(which == 0, hi, jnp.where(which == 1, mid, lo))
        ref[(*at, slice(STATE, MSG), slice(None))] = tail.astype(BF16)

    pairs = msg_ref.shape[1]
    copy = send(msg_ref.at[other], part, part_sem, {SP[2]: other})
    copy.wait()
    for j in range(pairs):
        decay = decay_of(part, j)
        put(
            turned,
            jnp.exp(decay) * state_of(msg_ref, c, j) + state_of(part, j),
            decay + decay_of(msg_ref, c, j),
            j,
        )
    copies = []
    for k in range(1, length_y):
        to = lax.rem(y + k, length_y)
        copies.append(send(turned.at[to], by_y.at[k], y_sem.at[k], {SP[1]: to}))
    by_y[0] = turned[y]
    for copy in copies:
        copy.wait()
    before = []
    state = jnp.zeros((STATE, 128), F32)
    decay = jnp.zeros((1, 128), F32)
    for q in range(length_y):
        before.append((state, decay))
        slot = jnp.where(forward, lax.rem(y - q + length_y, length_y), lax.rem(y + 1 + q, length_y))
        step = decay_of(by_y, slot)
        state = jnp.exp(step) * state + state_of(by_y, slot)
        decay = decay + step
    put(summed, state, decay)
    for k in range(1, length_z):
        to = lax.rem(z + k, length_z)

        @pl.when((z + k >= length_z) == (c == 1))
        def _():
            send(summed, by_z.at[k], z_sem.at[k], {SP[0]: to})

    carry[...] = jnp.zeros_like(carry)
    for distance in reversed(range(1, length_z)):
        slot = jnp.where(forward, distance, length_z - distance)

        @pl.when(order_z >= distance)
        def _():
            pltpu.make_async_remote_copy(
                src_ref=summed, dst_ref=by_z.at[slot], send_sem=z_sem.at[slot, 0],
                recv_sem=z_sem.at[slot, 1], device_id={SP[0]: z}, device_id_type=mesh_id,
            ).wait_recv()
            carry[...] = jnp.exp(decay_of(by_z, slot)) * carry[...] + state_of(by_z, slot)

    for k in range(1, length_z):
        to = lax.rem(z + k, length_z)

        @pl.when((z + k >= length_z) == (c == 1))
        def _():
            pltpu.make_async_remote_copy(
                src_ref=summed, dst_ref=by_z.at[k], send_sem=z_sem.at[k, 0],
                recv_sem=z_sem.at[k, 1], device_id={SP[0]: to}, device_id_type=mesh_id,
            ).wait_send()

    incoming = carry[...]
    for q in range(length_y):
        to = jnp.where(forward, q, length_y - 1 - q)
        state, decay = before[q]
        back[to] = (jnp.exp(decay) * incoming + state).astype(BF16)
    copies = []
    for k in range(1, length_y):
        to = lax.rem(y + k, length_y)
        copies.append(send(back.at[to], arrived.at[k], back_sem.at[k], {SP[1]: to}))
    arrived[0] = back[y]
    for copy in copies:
        copy.wait()
    for j in range(pairs):
        state = arrived[lax.rem(y - j + length_y, length_y)]
        out_ref[c, j] = state
        nxt[j] = (
            jnp.exp(decay_of(msg_ref, c, j)) * state.astype(F32) + state_of(msg_ref, c, j)
        ).astype(BF16)
    send(nxt, final, final_sem, {SP[2]: other}).wait()
    out_ref[other] = final[...]


def exchange(message, length_z, length_y):
    pairs = message.shape[1]
    tile = (STATE, 128)
    full = (MSG, 128)
    dma = pltpu.SemaphoreType.DMA
    return pl.pallas_call(
        exchange_kernel,
        in_specs=[pl.BlockSpec(memory_space=pltpu.VMEM)],
        out_specs=pl.BlockSpec(memory_space=pltpu.VMEM),
        out_shape=jax.ShapeDtypeStruct((2, pairs, *tile), BF16),
        scratch_shapes=[
            pltpu.VMEM((pairs, *full), BF16),
            pltpu.VMEM((pairs, *full), BF16),
            pltpu.VMEM((length_y, *full), BF16),
            pltpu.VMEM(full, BF16),
            pltpu.VMEM((length_z, *full), BF16),
            pltpu.VMEM((length_y, *tile), BF16),
            pltpu.VMEM((length_y, *tile), BF16),
            pltpu.VMEM((pairs, *tile), BF16),
            pltpu.VMEM((pairs, *tile), BF16),
            pltpu.VMEM(tile, F32),
            dma((2,)), dma((length_y, 2)), dma((length_z, 2)), dma((length_y, 2)), dma((2,)),
        ],
        compiler_params=pltpu.CompilerParams(
            collective_id=1, has_side_effects=True, vmem_limit_bytes=8 << 20
        ),
        cost_estimate=pl.CostEstimate(flops=1 << 24, bytes_accessed=1 << 20, transcendentals=0),
        name="exchange",
    )(message)


def neighbours(tail, head):
    count = lax.axis_size(SP)
    up = [(i, i + 1) for i in range(count - 1)]
    down = [(i + 1, i) for i in range(count - 1)]
    return lax.ppermute(tail, SP, up), lax.ppermute(head, SP, down)


def flatten_rows(weight):
    return weight.reshape(weight.shape[0], -1)


def shards(
    tokens, input_gain, gate_weight, value_weight, inflow_weight, readout_weight, step_weight,
    conv_values, conv_inflow, conv_readout, log_rate, group_gain, query_weight, key_weight,
    vector_weight, sink_logit, state_out, window_out,
):
    count = tokens.shape[0]
    place = lax.axis_index(SP)
    total = count * lax.axis_size(SP)
    length_z, length_y = lax.axis_size(SP[0]), lax.axis_size(SP[1])
    out_stack = jnp.concatenate([state_out, window_out], axis=0).T
    shard = jnp.concatenate(
        [
            value_weight, flatten_rows(inflow_weight), flatten_rows(readout_weight),
            key_weight, vector_weight, gate_weight, query_weight,
            jnp.pad(flatten_rows(step_weight), ((0, 0), (0, 128 - 2 * HEADS))), out_stack,
        ],
        axis=1,
    )
    gathered = lax.all_gather(shard, SP, axis=0, tiled=True)
    weights = gathered[:, 0:2048]
    step_weights = gathered[:, 2048:2176]
    out_weights = gathered[:, 2176:3200]
    proj, step_raw = project(tokens, input_gain.astype(F32)[None], weights, step_weights)
    conv_before, conv_after = neighbours(proj[-HALO:, 0:768], proj[:HALO, 0:768])
    kv_before, kv_after = neighbours(proj[-WINDOW:, 768:1024], proj[:WINDOW, 768:1024])
    spread_m = spread_matrix()
    rate = jnp.concatenate([log_rate[0], log_rate[1]], axis=1)
    taps = jnp.concatenate(
        [conv_values, flatten_rows(conv_inflow), flatten_rows(conv_readout)], axis=1
    )
    taps = jnp.pad(taps.astype(F32), ((0, 3), (0, 0)))
    conv, col, row, piece, etot, message = conv_state(
        proj, conv_before, conv_after, taps, step_raw, rate, spread_m
    )
    incoming = exchange(message, length_z, length_y)
    limits = jnp.stack([-place * count, total - place * count]).astype(jnp.int32)
    tables = rope_tables((place * count - WINDOW) // GRID_W, (count + 2 * WINDOW) // GRID_W)
    window, logs = attend(limits, proj, 3, 3, kv_before, kv_after, tables, sink_logit)
    state = mix(
        conv, col, row, piece, etot, incoming, proj, 2, group_gain.astype(F32)[None], spread_m
    )
    half = HEADS * HEAD_DIM
    terms = dot(state, out_weights[:, :half], ((1,), (1,))) + dot(
        window, out_weights[:, half:], ((1,), (1,))
    )
    n = lax.axis_size("tp")
    parts = jnp.moveaxis(terms.astype(BF16).reshape(count, n, -1), 1, 0)
    arrived = lax.all_to_all(parts, "tp", split_axis=0, concat_axis=0, tiled=True)
    mixed = arrived.astype(F32).sum(axis=0).astype(BF16)
    return mixed, logs.T


def solution(mesh):
    torus = Mesh(mesh.devices.reshape(8, 4, 2, mesh.shape["tp"]), (*SP, "tp"))
    return jax.shard_map(
        shards,
        mesh=torus,
        in_specs=(
            P(SP, None), P(), P(SP, "tp"), P(SP, "tp"), P(SP, "tp", None), P(SP, "tp", None),
            P(SP, None, "tp"), P(None, "tp"), P(None, "tp", None), P(None, "tp", None),
            P(None, SP, "tp"), P("tp"), P(SP, "tp"), P(SP, "tp"), P(SP, "tp"), P("tp"),
            P("tp", SP), P("tp", SP),
        ),
        out_specs=(P(SP, "tp"), P(SP, "tp")),
        check_vma=False,
    )
```

```python
import functools

import jax
import jax.numpy as jnp
from jax import lax
from jax.experimental import pallas as pl
from jax.experimental.pallas import tpu as pltpu
from jax.sharding import Mesh
from jax.sharding import PartitionSpec as P

HEAD_DIM = 64
STATE = 128
HEADS = 8
BLOCK = 128
WINDOW = 128
GRID_W = 64
HALO = 16
SP = ("sp_0", "sp_1", "sp_2")
EPS = 1e-06
ROPE_BASE = 10000.0
F32 = jnp.float32
BF16 = jnp.bfloat16
MSG = STATE + 16
KV_AT = 768


def dot(a, b, dims=((1,), (0,)), precision=None):
    return lax.dot_general(
        a, b, (dims, ((), ())), preferred_element_type=F32, precision=precision
    )


def split_bf16(value, parts):
    pieces = []
    for _ in range(parts):
        piece = value.astype(BF16)
        pieces.append(piece)
        value = value - piece.astype(F32)
    return pieces


def spread(value, spread_matrix, parts):
    pieces = [p.astype(F32) for p in split_bf16(value, parts)]
    joined = jnp.concatenate(pieces, axis=1).astype(BF16)
    matrix = jnp.concatenate([spread_matrix] * parts, axis=0)
    return dot(joined, matrix)


def spread_matrix():
    rows = jnp.arange(2 * HEADS)[:, None]
    cols = jnp.arange(2 * HEADS * HEAD_DIM)[None, :] // HEAD_DIM
    return (rows == cols).astype(BF16)


def project_kernel(tok_ref, before_ref, after_ref, gain_ref, a_ref, b_ref, out_ref, step_ref, normed):
    count = tok_ref.shape[0]
    place = lax.axis_index(SP)
    tile = 256

    def norm(value):
        wide = value.astype(F32)
        scale = lax.rsqrt(jnp.mean(wide * wide, axis=1, keepdims=True) + EPS)
        return wide * scale * gain_ref[...]

    def one(i, carry):
        rows = pl.ds(pl.multiple_of(i * BLOCK, BLOCK), BLOCK)
        normed[rows, :] = norm(tok_ref[rows, :]).astype(BF16)
        return carry

    lax.fori_loop(0, count // BLOCK, one, 0)
    before = jnp.where(place > 0, norm(before_ref[...]), 0.0)
    normed[count : count + HALO, :] = before.astype(BF16)
    after = jnp.where(place < lax.axis_size(SP) - 1, norm(after_ref[...]), 0.0)
    normed[count + HALO : count + 2 * HALO, :] = after.astype(BF16)

    def column(j, carry):
        cols = pl.ds(pl.multiple_of(j * tile, tile), tile)
        out_ref[:, cols] = dot(normed[...], a_ref[:, cols]).astype(BF16)
        return carry

    tiles = WIDTH_A // tile
    lax.fori_loop(0, tiles, column, 0)
    step_ref[...] = dot(normed[0:count, :], a_ref[:, tiles * tile : WIDTH_A])
    out_ref[:, tiles * tile : (tiles + 1) * tile] = dot(
        normed[...], b_ref[:, WIDTH_B - tile : WIDTH_B]
    ).astype(BF16)


def project(tokens, before, after, gain, a, b):
    count, width = tokens.shape
    columns = 2048
    vmem = pl.BlockSpec(memory_space=pltpu.VMEM)
    return pl.pallas_call(
        project_kernel,
        in_specs=[vmem] * 6,
        out_specs=[vmem] * 2,
        out_shape=[
            jax.ShapeDtypeStruct((count + 2 * HALO, columns), BF16),
            jax.ShapeDtypeStruct((count, 128), F32),
        ],
        scratch_shapes=[pltpu.VMEM((count + 2 * HALO, width), BF16)],
        compiler_params=pltpu.CompilerParams(vmem_limit_bytes=12 << 20),
        cost_estimate=pl.CostEstimate(
            flops=2 * count * width * (columns + 128),
            bytes_accessed=2 * (count * width + width * columns + count * columns),
            transcendentals=0,
        ),
        name="project",
    )(tokens, before, after, gain, a, b)


def conv_state_kernel(
    cin_ref, taps_ref, step_ref, rate_ref, e_ref,
    conv_ref, col_ref, row_ref, piece_ref, etot_ref, msg_ref, win, near,
):
    count = cin_ref.shape[0] - 2 * HALO
    blocks = count // BLOCK
    channels = HEADS * HEAD_DIM
    spread_m = e_ref[...]
    lane16 = lax.broadcasted_iota(jnp.int32, (BLOCK, 2 * HEADS), 1)
    forward16 = lane16 < HEADS
    tri = (
        lax.broadcasted_iota(jnp.int32, (BLOCK, BLOCK), 0)
        >= lax.broadcasted_iota(jnp.int32, (BLOCK, BLOCK), 1)
    ).astype(F32)
    win[pl.ds(0, HALO), :] = cin_ref[pl.ds(count, HALO), :].astype(F32)
    win[pl.ds(HALO + count, HALO), :] = cin_ref[pl.ds(count + HALO, HALO), :].astype(F32)

    def fill(i, carry):
        start = pl.multiple_of(i * BLOCK, BLOCK)
        win[pl.ds(HALO + start, BLOCK), :] = cin_ref[pl.ds(start, BLOCK), :].astype(F32)
        return carry

    lax.fori_loop(0, blocks, fill, 0)

    def one(i, total):
        start = pl.multiple_of(i * BLOCK, BLOCK)
        rows = pl.ds(start, BLOCK)
        near[...] = win[pl.ds(start, BLOCK + 2 * HALO), :]
        acc = near[HALO - 2 : HALO - 2 + BLOCK, :] * taps_ref[0:1, :]
        for tap in range(1, 5):
            first = HALO - 2 + tap
            acc = acc + near[first : first + BLOCK, :] * taps_ref[tap : tap + 1, :]
        conv = (acc * jax.nn.sigmoid(acc)).astype(BF16)
        conv_ref[rows, :] = conv
        raw = step_ref[rows, 0 : 2 * HEADS]
        step = jnp.maximum(raw, 0.0) + jnp.log1p(jnp.exp(-jnp.abs(raw)))
        decay = -jnp.exp(rate_ref[rows, :]) * step
        cum = dot(tri, decay, precision=lax.Precision.HIGHEST)
        tot = cum[BLOCK - 1 : BLOCK, :]
        col = jnp.where(forward16, cum, cum - decay)
        col_ref[rows, 0 : 2 * HEADS] = col
        col_ref[rows, 2 * HEADS : 4 * HEADS] = jnp.broadcast_to(tot, (BLOCK, 2 * HEADS))
        both = jnp.concatenate([col, step, jnp.zeros((BLOCK, 128 - 4 * HEADS), F32)], axis=1)
        row_ref[i] = both.T[0 : 4 * HEADS, :]
        weight = jnp.exp(jnp.where(forward16, tot - col, col)) * step
        wide = spread(weight, spread_m, 2)
        xs = conv[:, 0:channels].astype(F32)
        scaled = (jnp.concatenate([xs, xs], axis=1) * wide).astype(BF16)
        inflow = conv[:, channels : channels + STATE]
        piece_ref[i] = dot(inflow, scaled, ((0,), (0,)))
        etot_ref[i] = spread(jnp.exp(jnp.broadcast_to(tot, (8, 2 * HEADS))), spread_m, 3)
        return total + tot

    total = lax.fori_loop(0, blocks, one, jnp.zeros((1, 2 * HEADS), F32))
    forward = piece_ref[0, :, 0:channels]
    backward = piece_ref[blocks - 1, :, channels : 2 * channels]
    for i in range(1, blocks):
        forward = etot_ref[i, 0:1, 0:channels] * forward + piece_ref[i, :, 0:channels]
        k = blocks - 1 - i
        backward = (
            etot_ref[k, 0:1, channels : 2 * channels] * backward
            + piece_ref[k, :, channels : 2 * channels]
        )
    spread_total = spread(jnp.broadcast_to(total, (16, 2 * HEADS)), spread_m, 3)
    hi, mid, lo = split_bf16(spread_total, 3)
    which = lax.broadcasted_iota(jnp.int32, (16, 2 * channels), 0)
    tail = jnp.where(
        which == 0, hi.astype(F32), jnp.where(which == 1, mid.astype(F32), lo.astype(F32))
    ).astype(BF16)
    for e, state in enumerate((forward, backward)):
        for pair in range(channels // 128):
            lanes = slice(pair * 128, pair * 128 + 128)
            msg_ref[e, pair, 0:STATE, :] = state[:, lanes].astype(BF16)
            msg_ref[e, pair, STATE:MSG, :] = tail[:, e * channels + pair * 128 : e * channels + pair * 128 + 128]


def conv_state(proj, taps, step_raw, rate, spread_m):
    count = step_raw.shape[0]
    width = taps.shape[1]
    blocks = count // BLOCK
    channels = HEADS * HEAD_DIM
    whole = lambda shape: pl.BlockSpec(shape, lambda i: (0,) * len(shape))
    return pl.pallas_call(
        conv_state_kernel,
        grid=(1,),
        in_specs=[
            pl.BlockSpec((proj.shape[0], width), lambda i: (0, 0)),
            whole(taps.shape),
            whole(step_raw.shape),
            whole(rate.shape),
            whole(spread_m.shape),
        ],
        out_specs=[
            whole((count, width)),
            whole((count, 4 * HEADS)),
            whole((blocks, 4 * HEADS, BLOCK)),
            whole((blocks, STATE, 2 * channels)),
            whole((blocks, 8, 2 * channels)),
            whole((2, channels // 128, MSG, 128)),
        ],
        out_shape=[
            jax.ShapeDtypeStruct((count, width), BF16),
            jax.ShapeDtypeStruct((count, 4 * HEADS), F32),
            jax.ShapeDtypeStruct((blocks, 4 * HEADS, BLOCK), F32),
            jax.ShapeDtypeStruct((blocks, STATE, 2 * channels), F32),
            jax.ShapeDtypeStruct((blocks, 8, 2 * channels), F32),
            jax.ShapeDtypeStruct((2, channels // 128, MSG, 128), BF16),
        ],
        scratch_shapes=[
            pltpu.VMEM((count + 2 * HALO, width), F32),
            pltpu.VMEM((BLOCK + 2 * HALO, width), F32),
        ],
        compiler_params=pltpu.CompilerParams(vmem_limit_bytes=18 << 20),
        cost_estimate=pl.CostEstimate(
            flops=2 * count * STATE * 2 * channels, bytes_accessed=12 << 20, transcendentals=0
        ),
        name="conv_state",
    )(proj, taps, step_raw, rate, spread_m)


def mix_kernel(
    conv_ref, col_ref, row_ref, piece_ref, etot_ref, in_ref, gate_ref, gain_ref, e_ref,
    out_ref, held,
):
    count = conv_ref.shape[0]
    blocks = count // BLOCK
    channels = HEADS * HEAD_DIM
    spread_m = e_ref[...]
    for e in range(2):
        state = jnp.concatenate(
            [in_ref[e, p].astype(F32) for p in range(channels // 128)], axis=1
        )
        lanes = slice(e * channels, (e + 1) * channels)
        for i in range(blocks) if e == 0 else reversed(range(blocks)):
            held[i, :, lanes] = state.astype(BF16)
            state = etot_ref[i, 0:1, lanes] * state + piece_ref[i, :, lanes]
    row_at = lax.broadcasted_iota(jnp.int32, (BLOCK, BLOCK), 0)
    col_at = lax.broadcasted_iota(jnp.int32, (BLOCK, BLOCK), 1)
    lower = row_at >= col_at
    diagonal = row_at == col_at
    first_half = col_at < HEAD_DIM
    forward16 = lax.broadcasted_iota(jnp.int32, (BLOCK, 2 * HEADS), 1) < HEADS

    def one(i, carry):
        rows = pl.ds(pl.multiple_of(i * BLOCK, BLOCK), BLOCK)
        inflow = conv_ref[rows, channels : channels + STATE]
        readout = conv_ref[rows, channels + STATE : channels + 2 * STATE]
        inner = dot(readout, inflow, ((1,), (1,)))
        col = col_ref[rows, 0 : 2 * HEADS]
        tot = col_ref[rows, 2 * HEADS : 4 * HEADS]
        reach = spread(jnp.exp(jnp.where(forward16, col, tot - col)), spread_m, 2)
        far = dot(readout, held[i]) * reach
        parts = []
        for pair in range(HEADS // 2):
            weights = []
            for h in (2 * pair, 2 * pair + 1):
                b = HEADS + h
                arg = jnp.where(
                    lower,
                    col[:, h : h + 1] - row_ref[i, h : h + 1, :],
                    row_ref[i, b : b + 1, :] - col[:, b : b + 1],
                )
                step_f = row_ref[i, 2 * HEADS + h : 2 * HEADS + h + 1, :]
                step_b = row_ref[i, 2 * HEADS + b : 2 * HEADS + b + 1, :]
                step = jnp.where(lower, step_f, step_b) + jnp.where(diagonal, step_b, 0.0)
                weights.append((inner * jnp.exp(arg) * step).astype(BF16))
            xs = conv_ref[rows, pair * 128 : pair * 128 + 128]
            zero = jnp.zeros_like(xs)
            stacked = jnp.concatenate(
                [jnp.where(first_half, xs, zero), jnp.where(first_half, zero, xs)], axis=0
            )
            parts.append(dot(jnp.concatenate(weights, axis=1), stacked))
        y = jnp.concatenate(parts, axis=1) + far[:, 0:channels] + far[:, channels:]
        gate = gate_ref[rows, :].astype(F32)
        y = y * (gate * jax.nn.sigmoid(gate))
        y = y * lax.rsqrt(jnp.mean(y * y, axis=1, keepdims=True) + EPS)
        out_ref[rows, :] = (y * gain_ref[...]).astype(BF16)
        return carry

    lax.fori_loop(0, blocks, one, 0)


def mix(conv, col, row, piece, etot, incoming, proj, gate_block, gain, spread_m):
    count = conv.shape[0]
    blocks = count // BLOCK
    channels = HEADS * HEAD_DIM
    whole = lambda shape: pl.BlockSpec(shape, lambda i: (0,) * len(shape))
    return pl.pallas_call(
        mix_kernel,
        grid=(1,),
        in_specs=[
            whole(conv.shape), whole(col.shape), whole(row.shape), whole(piece.shape),
            whole(etot.shape), whole(incoming.shape),
            pl.BlockSpec((count, channels), lambda i: (0, gate_block)),
            whole(gain.shape), whole(spread_m.shape),
        ],
        out_specs=whole((count, channels)),
        out_shape=jax.ShapeDtypeStruct((count, channels), BF16),
        scratch_shapes=[pltpu.VMEM((blocks, STATE, 2 * channels), BF16)],
        compiler_params=pltpu.CompilerParams(vmem_limit_bytes=16 << 20),
        cost_estimate=pl.CostEstimate(
            flops=2 * count * BLOCK * 4 * channels, bytes_accessed=8 << 20, transcendentals=0
        ),
        name="mix",
    )(conv, col, row, piece, etot, incoming, proj, gain, spread_m)


def rope_tables(first_row, grid_rows):
    quarter = HEAD_DIM // 4
    lane = jnp.arange(2 * HEAD_DIM)
    freqs = ROPE_BASE ** (-(lane % quarter).astype(F32) / quarter)
    sign = jnp.where(lane % (2 * quarter) < quarter, -1.0, 1.0)
    row_angle = (first_row + jnp.arange(grid_rows, dtype=jnp.int32)).astype(F32)[:, None] * freqs
    col_angle = jnp.arange(GRID_W, dtype=jnp.int32).astype(F32)[:, None] * freqs
    return (
        jnp.stack([jnp.cos(row_angle), jnp.sin(row_angle) * sign]),
        jnp.stack([jnp.cos(col_angle), jnp.sin(col_angle) * sign]),
    )


def attend_kernel(
    q_ref, kv_ref, before_ref, after_ref, by_row_ref, by_col_ref, sink_ref,
    out_ref, log_ref, keys, values,
):
    count = q_ref.shape[0]
    blocks = count // BLOCK
    place = lax.axis_index(SP)
    lane = lax.broadcasted_iota(jnp.int32, (BLOCK, 128), 1)
    low_quarter = lane % 32 < 16
    first_half = lane < HEAD_DIM
    row_lane = (lane % HEAD_DIM < 32)[0:GRID_W]

    def tables(slot):
        out = []
        for kind in range(2):
            parts = []
            for r in range(BLOCK // GRID_W):
                row = by_row_ref[kind, pl.ds(slot * (BLOCK // GRID_W) + r, 1), :]
                parts.append(jnp.where(row_lane, row, by_col_ref[kind]))
            out.append(jnp.concatenate(parts, axis=0))
        return out

    def turn(value, table):
        wide = value.astype(F32)
        other = jnp.where(low_quarter, pltpu.roll(wide, 112, 1), pltpu.roll(wide, 16, 1))
        return (wide * table[0] + other * table[1]).astype(BF16)

    def store(raw, slot):
        rows = pl.ds(pl.multiple_of(slot * BLOCK, BLOCK), BLOCK)
        key = turn(raw[:, 0:128], tables(slot)).astype(F32)
        swapped = pltpu.roll(key, 64, 1)
        keys[0, rows, :] = jnp.where(first_half, key, swapped).astype(BF16)
        keys[1, rows, :] = jnp.where(first_half, swapped, key).astype(BF16)
        values[:, rows] = raw[:, 128:256].astype(F32).T.astype(BF16)

    store(before_ref[...], 0)
    store(after_ref[...], blocks + 1)

    def fill(i, carry):
        store(kv_ref[pl.ds(pl.multiple_of(i * BLOCK, BLOCK), BLOCK), :], i + 1)
        return carry

    lax.fori_loop(0, blocks, fill, 0)
    key_at = lax.broadcasted_iota(jnp.int32, (3 * BLOCK, 2 * BLOCK), 0)
    query_at = lax.broadcasted_iota(jnp.int32, (3 * BLOCK, 2 * BLOCK), 1) % BLOCK
    in_band = (key_at >= query_at) & (key_at <= query_at + 2 * WINDOW)
    start_at = -place * count
    end_at = start_at + count * lax.axis_size(SP)

    def one(i, carry):
        start = pl.multiple_of(i * BLOCK, BLOCK)
        rows = pl.ds(start, BLOCK)
        here = key_at + (start - WINDOW)
        valid = in_band & (here >= start_at) & (here < end_at)
        table = tables(i + 1)
        band = pl.ds(start, 3 * BLOCK)
        for pair in range(HEADS // 2):
            group = pair // 2
            lanes = slice(pair * 128, pair * 128 + 128)
            q = (turn(q_ref[rows, lanes], table).astype(F32) * HEAD_DIM ** (-0.5)).astype(BF16)
            zero = jnp.zeros_like(q)
            both = jnp.concatenate(
                [jnp.where(first_half, q, zero), jnp.where(first_half, zero, q)], axis=0
            )
            scores = dot(keys[group, band, :], both, ((1,), (1,)))
            scores = jnp.where(valid, scores, -1e30)
            sink = sink_ref[pair : pair + 1, :]
            top = jnp.maximum(jnp.max(scores, axis=0, keepdims=True), sink)
            expo = jnp.exp(scores - top)
            total = jnp.sum(expo, axis=0, keepdims=True) + jnp.exp(sink - top)
            mine = values[group * HEAD_DIM : (group + 1) * HEAD_DIM, band]
            o = dot(mine, expo.astype(BF16)) / total
            turned = jnp.concatenate([o[:, 0:BLOCK], o[:, BLOCK:]], axis=0).T
            out_ref[rows, lanes] = turned.astype(BF16)
            log = top + jnp.log(total)
            log_ref[2 * pair : 2 * pair + 1, rows] = log[:, 0:BLOCK]
            log_ref[2 * pair + 1 : 2 * pair + 2, rows] = log[:, BLOCK:]
        return carry

    lax.fori_loop(0, blocks, one, 0)


def attend(count, proj, q_block, kv_block, before, after, tables, sinks):
    channels = HEADS * HEAD_DIM
    whole = lambda shape: pl.BlockSpec(shape, lambda i, *_: (0,) * len(shape))
    by_row, by_col = tables
    wide_sinks = jnp.repeat(sinks.reshape(HEADS // 2, 2), BLOCK, axis=1)
    return pl.pallas_call(
        attend_kernel,
        grid=(1,),
        in_specs=[
            pl.BlockSpec((count, channels), lambda i: (0, q_block)),
            pl.BlockSpec((count, 256), lambda i: (0, kv_block)),
            whole(before.shape), whole(after.shape), whole(by_row.shape), whole(by_col.shape),
            whole(wide_sinks.shape),
        ],
        out_specs=[whole((count, channels)), whole((HEADS, count))],
        out_shape=[
            jax.ShapeDtypeStruct((count, channels), BF16),
            jax.ShapeDtypeStruct((HEADS, count), F32),
        ],
        scratch_shapes=[
            pltpu.VMEM((2, count + 2 * BLOCK, 128), BF16),
            pltpu.VMEM((128, count + 2 * BLOCK), BF16),
        ],
        compiler_params=pltpu.CompilerParams(vmem_limit_bytes=12 << 20),
        cost_estimate=pl.CostEstimate(
            flops=4 * count * 3 * BLOCK * channels, bytes_accessed=4 << 20, transcendentals=0
        ),
        name="attend",
    )(proj, proj, before, after, by_row, by_col, wide_sinks)


LINKS = ("z+", "z-", "y+", "y-")
WIDTH_A = 1920
WIDTH_B = 1280


def ring(kind, link_axis, other_at, length, total, cut):
    out = []
    for sign in (1, -1):
        previous = None
        for step in range(length // 2):
            last = step == length // 2 - 1
            cols = (0, total)
            if last:
                cols = (0, cut) if sign == 1 else (cut, total)
            name = (kind, link_axis, other_at, sign, step)
            out.append(dict(
                name=name, kind=kind, axis=link_axis, sign=sign,
                along=-sign * step, other=other_at, cols=cols, after=previous,
            ))
            previous = name
    return out


def transfers(length_z, length_y):
    sends = []
    for kind, first, length, second, length2, total, cut in (
        ("A", "z", length_z, "y", length_y, WIDTH_A, 1024),
        ("B", "y", length_y, "z", length_z, WIDTH_B, 640),
    ):
        sends += ring(kind, first, 0, length, total, cut)
        for offset in range(-(length // 2) + 1, length // 2 + 1):
            sends += ring(kind, second, offset, length2, total, cut)
    for s in sends:
        length, first = (length_z, "z") if s["kind"] == "A" else (length_y, "y")
        s["needs"] = []
        if s["after"] is not None:
            s["needs"] = [s["after"]]
        elif s["axis"] != first and s["other"] != 0:
            d = s["other"]
            if abs(d) == length // 2:
                s["needs"] = [(s["kind"], first, 0, sign, length // 2 - 1) for sign in (1, -1)]
            else:
                s["needs"] = [(s["kind"], first, 0, -1 if d > 0 else 1, abs(d) - 1)]
    return sends


def arrival_order(sends):
    import heapq

    rate, hop = 46.6e3, 1.9
    free = dict.fromkeys(LINKS, 0.0)
    left = {s["name"]: len(s["needs"]) for s in sends}
    followers = {}
    for s in sends:
        for need in s["needs"]:
            followers.setdefault(need, []).append(s)
    heap, order, first = [], [], []

    def start(s, now):
        link = s["axis"] + ("+" if s["sign"] == 1 else "-")
        size = 32 * 2 * (s["cols"][1] - s["cols"][0])
        free[link] = max(free[link], now) + size / rate
        heapq.heappush(heap, (free[link] + hop, len(order), str(s["name"]), s["name"]))

    def rank(s):
        return (s["axis"] != ("z" if s["kind"] == "A" else "y"), s["kind"] != "A")

    for s in sorted((s for s in sends if not s["needs"]), key=rank):
        first.append(s)
        start(s, 0.0)
    end = 0.0
    while heap:
        now, _, _, name = heapq.heappop(heap)
        ready = []
        for s in sorted(followers.get(name, []), key=rank):
            left[s["name"]] -= 1
            if left[s["name"]] == 0:
                ready.append(s)
                start(s, now)
        order.append((name, ready))
        end = now
    return first, order, end


def gather_kernel(
    lengths, edges_ref, value_ref, inflow_ref, readout_ref, key_ref, vector_ref, gate_ref,
    query_ref, step_ref, turned_ref,
    a_ref, b_ref, before_ref, after_ref, send_sem, recv_sem, core_send, core_recv, edge_sem,
):
    length_z, length_y = lengths
    z, y, c = (lax.axis_index(a) for a in SP)
    other = 1 - c
    mesh_id = pl.DeviceIdType.MESH

    def wrap(value, length):
        return lax.rem(value + length, length)

    steps = {"z": (SP[0], z, length_z), "y": (SP[1], y, length_y)}

    def towards(axis, sign):
        name, at, length = steps[axis]
        return {name: wrap(at + sign, length)}

    flat = (z * length_y + y) * 2 + c
    count = length_z * length_y * 2

    def device_at(index):
        index = wrap(index, count)
        return {
            SP[0]: index // (2 * length_y),
            SP[1]: lax.rem(index // 2, length_y),
            SP[2]: lax.rem(index, 2),
        }

    peers = [{SP[2]: other}] + [towards(a, s) for a in ("z", "y") for s in (1, -1)]
    peers += [device_at(flat + 1), device_at(flat - 1)]
    barrier = pltpu.get_barrier_semaphore()
    for peer in peers:
        pl.semaphore_signal(barrier, inc=1, device_id=peer, device_id_type=mesh_id)

    own_a, own_b = a_ref.at[z, y, c], b_ref.at[z, y, c]
    column = 0
    for ref in (value_ref, inflow_ref, readout_ref, key_ref, vector_ref, gate_ref):
        own_a[:, column : column + ref.shape[1]] = ref[...]
        column += ref.shape[1]
    half = query_ref.shape[1] // 2
    own_a[:, column : column + half] = query_ref[:, 0:half]
    own_a[:, column + half : WIDTH_A] = step_ref[...]
    own_b[:, 0 : turned_ref.shape[1]] = turned_ref[...]
    own_b[:, turned_ref.shape[1] : WIDTH_B] = query_ref[:, half : 2 * half]
    pl.semaphore_wait(barrier, len(peers))

    sends = transfers(length_z, length_y)
    number = {s["name"]: i for i, s in enumerate(sends)}
    by_name = {s["name"]: s for s in sends}

    def block(s, shift):
        along = s["along"] - shift * s["sign"]
        dz, dy = (along, s["other"]) if s["axis"] == "z" else (s["other"], along)
        ref = a_ref if s["kind"] == "A" else b_ref
        cols = pl.ds(s["cols"][0], s["cols"][1] - s["cols"][0])
        return ref.at[wrap(z + dz, length_z), wrap(y + dy, length_y), c, :, cols]

    def copy_of(s, shift):
        i = number[s["name"]]
        ref = block(s, shift)
        return pltpu.make_async_remote_copy(
            src_ref=ref, dst_ref=ref, send_sem=send_sem.at[i], recv_sem=recv_sem.at[i],
            device_id=towards(s["axis"], s["sign"]), device_id_type=mesh_id,
        )

    edge_rows = edges_ref.shape[0] // 2
    edge_copies = []
    for k, (index, dst) in enumerate(((flat - 1, after_ref), (flat + 1, before_ref))):
        edge_copies.append(pltpu.make_async_remote_copy(
            src_ref=edges_ref.at[pl.ds(k * edge_rows, edge_rows)], dst_ref=dst,
            send_sem=edge_sem.at[k, 0], recv_sem=edge_sem.at[k, 1],
            device_id=device_at(index), device_id_type=mesh_id,
        ))

    first, order, _ = arrival_order(sends)
    started = []
    for s in first:
        copy = copy_of(s, 0)
        copy.start()
        started.append(copy)
    for copy in edge_copies:
        copy.start()

    waiting = {}
    for kind, first_axis, length, second in (("A", "z", length_z, "y"), ("B", "y", length_y, "z")):
        for offset in range(-(length // 2) + 1, length // 2 + 1):
            names = [s["name"] for s in sends
                     if s["kind"] == kind and s["axis"] == second and s["other"] == offset]
            waiting[(kind, offset)] = set(names)
    keys = list(waiting)

    def core_copy(key):
        kind, offset = key
        i = keys.index(key)
        if kind == "A":
            src = a_ref.at[wrap(z + offset, length_z), :, c]
        else:
            src = b_ref.at[:, wrap(y + offset, length_y), c]
        return src, i

    def send_core(key):
        src, i = core_copy(key)
        copy = pltpu.make_async_remote_copy(
            src_ref=src, dst_ref=src, send_sem=core_send.at[i], recv_sem=core_recv.at[i],
            device_id={SP[2]: other}, device_id_type=mesh_id,
        )
        copy.start()
        started.append(copy)

    def wait_core(key):
        kind, offset = key
        i = keys.index(key)
        if kind == "A":
            dst = a_ref.at[wrap(z + offset, length_z), :, other]
        else:
            dst = b_ref.at[:, wrap(y + offset, length_y), other]
        pltpu.make_async_remote_copy(
            src_ref=dst, dst_ref=dst, send_sem=core_send.at[i], recv_sem=core_recv.at[i],
            device_id={SP[2]: other}, device_id_type=mesh_id,
        ).wait_recv()

    for name, ready in order:
        copy_of(by_name[name], 1).wait_recv()
        for s in ready:
            copy = copy_of(s, 0)
            copy.start()
            started.append(copy)
        for key in keys:
            if name in waiting[key]:
                waiting[key].remove(name)
                if not waiting[key]:
                    send_core(key)
    for copy in started:
        copy.wait_send()
    for key in keys:
        wait_core(key)
    for copy in edge_copies:
        copy.wait()


def gather(length_z, length_y, edges, *shards):
    sends = transfers(length_z, length_y)
    groups = length_z + length_y
    vmem = pl.BlockSpec(memory_space=pltpu.VMEM)
    dma = pltpu.SemaphoreType.DMA
    lead = (length_z, length_y, 2, 32)
    edge = (edges.shape[0] // 2, edges.shape[1])
    a, b, before, after = pl.pallas_call(
        functools.partial(gather_kernel, (length_z, length_y)),
        in_specs=[vmem] * (1 + len(shards)),
        out_specs=[vmem] * 4,
        out_shape=[
            jax.ShapeDtypeStruct((*lead, WIDTH_A), BF16),
            jax.ShapeDtypeStruct((*lead, WIDTH_B), BF16),
            jax.ShapeDtypeStruct(edge, BF16),
            jax.ShapeDtypeStruct(edge, BF16),
        ],
        scratch_shapes=[
            dma((len(sends),)), dma((len(sends),)), dma((groups,)), dma((groups,)), dma((2, 2)),
        ],
        compiler_params=pltpu.CompilerParams(
            collective_id=2, has_side_effects=True, vmem_limit_bytes=20 << 20
        ),
        cost_estimate=pl.CostEstimate(flops=1 << 24, bytes_accessed=24 << 20, transcendentals=0),
        name="gather",
    )(edges, *shards)
    return a.reshape(-1, WIDTH_A), b.reshape(-1, WIDTH_B), before, after


def exchange_kernel(
    rows, msg_ref, proj_ref, out_ref, kv_before_ref, kv_after_ref, part, turned, by_y, summed, by_z, back, arrived, nxt, final, carry,
    part_sem, y_sem, z_sem, back_sem, final_sem, kv_sem,
):
    z, y, c = (lax.axis_index(a) for a in SP)
    length_z, length_y = lax.axis_size(SP[0]), lax.axis_size(SP[1])
    forward = c == 0
    other = 1 - c
    order_z = jnp.where(forward, z, length_z - 1 - z)
    mesh_id = pl.DeviceIdType.MESH
    peers = [{SP[2]: other}]
    peers += [{SP[1]: lax.rem(y + k, length_y)} for k in range(1, length_y)]
    peers += [{SP[0]: lax.rem(z + k, length_z)} for k in range(1, length_z)]
    flat = (z * length_y + y) * 2 + c
    count = length_z * length_y * 2

    def device_at(index):
        index = lax.rem(index + count, count)
        return {
            SP[0]: index // (2 * length_y),
            SP[1]: lax.rem(index // 2, length_y),
            SP[2]: lax.rem(index, 2),
        }

    peers += [device_at(flat + 1), device_at(flat - 1)]
    barrier = pltpu.get_barrier_semaphore()
    for peer in peers:
        pl.semaphore_signal(barrier, inc=1, device_id=peer, device_id_type=mesh_id)
    pl.semaphore_wait(barrier, len(peers))

    def send(src, dst, sems, peer):
        copy = pltpu.make_async_remote_copy(
            src_ref=src, dst_ref=dst, send_sem=sems.at[0], recv_sem=sems.at[1],
            device_id=peer, device_id_type=mesh_id,
        )
        copy.start()
        return copy

    def state_of(ref, *at):
        return ref[(*at, slice(0, STATE), slice(None))].astype(F32)

    def decay_of(ref, *at):
        tail = ref[(*at, slice(STATE, MSG), slice(None))].astype(F32)
        return tail[0:1] + tail[1:2] + tail[2:3]

    def put(ref, state, decay, *at):
        ref[(*at, slice(0, STATE), slice(None))] = state.astype(BF16)
        hi, mid, lo = (p.astype(F32) for p in split_bf16(decay, 3))
        which = lax.broadcasted_iota(jnp.int32, (MSG - STATE, 128), 0)
        tail = jnp.where(which == 0, hi, jnp.where(which == 1, mid, lo))
        ref[(*at, slice(STATE, MSG), slice(None))] = tail.astype(BF16)

    pairs = msg_ref.shape[1]
    copy = send(msg_ref.at[other], part, part_sem, {SP[2]: other})
    kv_cols = pl.ds(KV_AT, kv_before_ref.shape[1])
    kv_copies = [
        send(
            proj_ref.at[pl.ds(rows - WINDOW, WINDOW), kv_cols], kv_before_ref, kv_sem.at[0],
            device_at(flat + 1),
        ),
        send(proj_ref.at[pl.ds(0, WINDOW), kv_cols], kv_after_ref, kv_sem.at[1], device_at(flat - 1)),
    ]
    copy.wait()
    for j in range(pairs):
        decay = decay_of(part, j)
        put(
            turned,
            jnp.exp(decay) * state_of(msg_ref, c, j) + state_of(part, j),
            decay + decay_of(msg_ref, c, j),
            j,
        )
    copies = []
    for k in range(1, length_y):
        to = lax.rem(y + k, length_y)
        copies.append(send(turned.at[to], by_y.at[k], y_sem.at[k], {SP[1]: to}))
    by_y[0] = turned[y]
    for copy in copies:
        copy.wait()
    before = []
    state = jnp.zeros((STATE, 128), F32)
    decay = jnp.zeros((1, 128), F32)
    for q in range(length_y):
        before.append((state, decay))
        slot = jnp.where(forward, lax.rem(y - q + length_y, length_y), lax.rem(y + 1 + q, length_y))
        step = decay_of(by_y, slot)
        state = jnp.exp(step) * state + state_of(by_y, slot)
        decay = decay + step
    put(summed, state, decay)
    for k in range(1, length_z):
        to = lax.rem(z + k, length_z)

        @pl.when((z + k >= length_z) == (c == 1))
        def _():
            send(summed, by_z.at[k], z_sem.at[k], {SP[0]: to})

    carry[...] = jnp.zeros_like(carry)
    for distance in reversed(range(1, length_z)):
        slot = jnp.where(forward, distance, length_z - distance)

        @pl.when(order_z >= distance)
        def _():
            pltpu.make_async_remote_copy(
                src_ref=summed, dst_ref=by_z.at[slot], send_sem=z_sem.at[slot, 0],
                recv_sem=z_sem.at[slot, 1], device_id={SP[0]: z}, device_id_type=mesh_id,
            ).wait_recv()
            carry[...] = jnp.exp(decay_of(by_z, slot)) * carry[...] + state_of(by_z, slot)

    for k in range(1, length_z):
        to = lax.rem(z + k, length_z)

        @pl.when((z + k >= length_z) == (c == 1))
        def _():
            pltpu.make_async_remote_copy(
                src_ref=summed, dst_ref=by_z.at[k], send_sem=z_sem.at[k, 0],
                recv_sem=z_sem.at[k, 1], device_id={SP[0]: to}, device_id_type=mesh_id,
            ).wait_send()

    incoming = carry[...]
    for q in range(length_y):
        to = jnp.where(forward, q, length_y - 1 - q)
        state, decay = before[q]
        back[to] = (jnp.exp(decay) * incoming + state).astype(BF16)
    copies = []
    for k in range(1, length_y):
        to = lax.rem(y + k, length_y)
        copies.append(send(back.at[to], arrived.at[k], back_sem.at[k], {SP[1]: to}))
    arrived[0] = back[y]
    for copy in copies:
        copy.wait()
    for j in range(pairs):
        state = arrived[lax.rem(y - j + length_y, length_y)]
        out_ref[c, j] = state
        nxt[j] = (
            jnp.exp(decay_of(msg_ref, c, j)) * state.astype(F32) + state_of(msg_ref, c, j)
        ).astype(BF16)
    send(nxt, final, final_sem, {SP[2]: other}).wait()
    out_ref[other] = final[...]
    for copy in kv_copies:
        copy.wait()


def exchange(message, proj, rows, length_z, length_y):
    pairs = message.shape[1]
    tile = (STATE, 128)
    full = (MSG, 128)
    dma = pltpu.SemaphoreType.DMA
    return pl.pallas_call(
        functools.partial(exchange_kernel, rows),
        in_specs=[pl.BlockSpec(memory_space=pltpu.VMEM)] * 2,
        out_specs=[pl.BlockSpec(memory_space=pltpu.VMEM)] * 3,
        out_shape=[
            jax.ShapeDtypeStruct((2, pairs, *tile), BF16),
            jax.ShapeDtypeStruct((WINDOW, 256), BF16),
            jax.ShapeDtypeStruct((WINDOW, 256), BF16),
        ],
        scratch_shapes=[
            pltpu.VMEM((pairs, *full), BF16),
            pltpu.VMEM((pairs, *full), BF16),
            pltpu.VMEM((length_y, *full), BF16),
            pltpu.VMEM(full, BF16),
            pltpu.VMEM((length_z, *full), BF16),
            pltpu.VMEM((length_y, *tile), BF16),
            pltpu.VMEM((length_y, *tile), BF16),
            pltpu.VMEM((pairs, *tile), BF16),
            pltpu.VMEM((pairs, *tile), BF16),
            pltpu.VMEM(tile, F32),
            dma((2,)), dma((length_y, 2)), dma((length_z, 2)), dma((length_y, 2)), dma((2,)),
            dma((2, 2)),
        ],
        compiler_params=pltpu.CompilerParams(
            collective_id=1, has_side_effects=True, vmem_limit_bytes=8 << 20
        ),
        cost_estimate=pl.CostEstimate(flops=1 << 24, bytes_accessed=1 << 20, transcendentals=0),
        name="exchange",
    )(message, proj)


def finish_kernel(state_ref, window_ref, w_ref, out_ref, *refs):
    far_out, far_in, near_out, near_in, far_sem, near_sem = refs
    n = lax.axis_size("tp")
    me = lax.axis_index("tp")
    mesh_id = pl.DeviceIdType.MESH
    sides = (1, -1)
    count, channels = state_ref.shape
    width = w_ref.shape[0] // n
    half = width // 2
    chunk = far_out.shape[2]
    chunks = count // chunk

    def at(step):
        return lax.rem(me + step + n, n)

    barrier = pltpu.get_barrier_semaphore()
    for side in sides:
        pl.semaphore_signal(barrier, inc=1, device_id={"tp": at(side)}, device_id_type=mesh_id)
    pl.semaphore_wait(barrier, 2)

    def terms(rows, to):
        outs = pl.ds(pl.multiple_of(to * width, width), width)
        return dot(state_ref[rows, :], w_ref[outs, 0:channels], ((1,), (1,))) + dot(
            window_ref[rows, :], w_ref[outs, channels : 2 * channels], ((1,), (1,))
        )

    def far_copy(i, k):
        return pltpu.make_async_remote_copy(
            src_ref=far_out.at[k, i], dst_ref=far_in.at[k, i], send_sem=far_sem.at[k, i, 0],
            recv_sem=far_sem.at[k, i, 1], device_id={"tp": at(sides[k])}, device_id_type=mesh_id,
        )

    def near_copy(i, k):
        return pltpu.make_async_remote_copy(
            src_ref=near_out.at[k, i], dst_ref=near_in.at[k, i], send_sem=near_sem.at[k, i, 0],
            recv_sem=near_sem.at[k, i, 1], device_id={"tp": at(sides[k])}, device_id_type=mesh_id,
        )

    def send_far(i, carry):
        rows = pl.ds(pl.multiple_of(i * chunk, chunk), chunk)
        value = terms(rows, at(2)).astype(BF16)
        for k in range(2):
            far_out[k, i] = value[:, k * half : (k + 1) * half]
            far_copy(i, k).start()
        return carry

    lax.fori_loop(0, chunks, send_far, 0)

    def send_near(i, carry):
        rows = pl.ds(pl.multiple_of(i * chunk, chunk), chunk)
        for k in range(2):
            value = terms(rows, at(sides[k])).astype(BF16).astype(F32)
            lanes = slice(k * half, (k + 1) * half)
            far_copy(i, k).wait_recv()
            near_out[k, i] = value.astype(BF16)
            near_out[k, i, :, lanes] = (value[:, lanes] + far_in[k, i].astype(F32)).astype(BF16)
            near_copy(i, k).start()
        return carry

    lax.fori_loop(0, chunks, send_near, 0)

    def collect(i, carry):
        rows = pl.ds(pl.multiple_of(i * chunk, chunk), chunk)
        value = terms(rows, me).astype(BF16).astype(F32)
        for k in range(2):
            near_copy(i, k).wait_recv()
            value = value + near_in[k, i].astype(F32)
        out_ref[rows, :] = value.astype(BF16)
        for k in range(2):
            far_copy(i, k).wait_send()
            near_copy(i, k).wait_send()
        return carry

    lax.fori_loop(0, chunks, collect, 0)


def finish(state, window, weights, n):
    count, channels = state.shape
    width = weights.shape[0] // n
    chunk = 128
    chunks = count // chunk
    vmem = pl.BlockSpec(memory_space=pltpu.VMEM)
    dma = pltpu.SemaphoreType.DMA
    return pl.pallas_call(
        finish_kernel,
        in_specs=[vmem] * 3,
        out_specs=vmem,
        out_shape=jax.ShapeDtypeStruct((count, width), BF16),
        scratch_shapes=[
            pltpu.VMEM((2, chunks, chunk, width // 2), BF16),
            pltpu.VMEM((2, chunks, chunk, width // 2), BF16),
            pltpu.VMEM((2, chunks, chunk, width), BF16),
            pltpu.VMEM((2, chunks, chunk, width), BF16),
            dma((2, chunks, 2)), dma((2, chunks, 2)),
        ],
        compiler_params=pltpu.CompilerParams(
            collective_id=3, has_side_effects=True, vmem_limit_bytes=24 << 20
        ),
        cost_estimate=pl.CostEstimate(
            flops=4 * count * channels * width * n, bytes_accessed=8 << 20, transcendentals=0
        ),
        name="finish",
    )(state, window, weights)


def flatten_rows(weight):
    return weight.reshape(weight.shape[0], -1)


def shards(
    tokens, input_gain, gate_weight, value_weight, inflow_weight, readout_weight, step_weight,
    conv_values, conv_inflow, conv_readout, log_rate, group_gain, query_weight, key_weight,
    vector_weight, sink_logit, state_out, window_out,
):
    count = tokens.shape[0]
    place = lax.axis_index(SP)
    length_z, length_y = lax.axis_size(SP[0]), lax.axis_size(SP[1])
    spread_m = spread_matrix()
    rate = jnp.concatenate([log_rate[0], log_rate[1]], axis=1)
    taps = jnp.concatenate(
        [conv_values, flatten_rows(conv_inflow), flatten_rows(conv_readout)], axis=1
    )
    taps = jnp.pad(taps.astype(F32), ((0, 3), (0, 0)))
    tables = rope_tables((place * count - WINDOW) // GRID_W, (count + 2 * WINDOW) // GRID_W)
    edges = jnp.concatenate([tokens[:HALO], tokens[-HALO:]], axis=0)
    a, b, before, after = gather(
        length_z, length_y, edges, value_weight, flatten_rows(inflow_weight),
        flatten_rows(readout_weight), key_weight, vector_weight, gate_weight, query_weight,
        jnp.pad(flatten_rows(step_weight), ((0, 0), (0, 128 - 2 * HEADS))),
        jnp.concatenate([state_out, window_out], axis=0).T,
    )
    proj, step_raw = project(tokens, before, after, input_gain.astype(F32)[None], a, b)
    conv, col, row, piece, etot, message = conv_state(proj, taps, step_raw, rate, spread_m)
    incoming, kv_before, kv_after = exchange(message, proj, count, length_z, length_y)
    window, logs = attend(count, proj, 3, 3, kv_before, kv_after, tables, sink_logit)
    state = mix(
        conv, col, row, piece, etot, incoming, proj, 2, group_gain.astype(F32)[None], spread_m
    )
    mixed = finish(state, window, b, lax.axis_size("tp"))
    return mixed, logs.T


def solution(mesh):
    torus = Mesh(mesh.devices.reshape(8, 4, 2, mesh.shape["tp"]), (*SP, "tp"))
    return jax.shard_map(
        shards,
        mesh=torus,
        in_specs=(
            P(SP, None), P(), P(SP, "tp"), P(SP, "tp"), P(SP, "tp", None), P(SP, "tp", None),
            P(SP, None, "tp"), P(None, "tp"), P(None, "tp", None), P(None, "tp", None),
            P(None, SP, "tp"), P("tp"), P(SP, "tp"), P(SP, "tp"), P(SP, "tp"), P("tp"),
            P("tp", SP), P("tp", SP),
        ),
        out_specs=(P(SP, "tp"), P(SP, "tp")),
        check_vma=False,
    )
```

```python
import functools

import jax
import jax.numpy as jnp
from jax import lax
from jax.experimental import pallas as pl
from jax.experimental.pallas import tpu as pltpu
from jax.sharding import Mesh
from jax.sharding import PartitionSpec as P

HEAD_DIM = 64
STATE = 128
HEADS = 8
BLOCK = 128
WINDOW = 128
GRID_W = 64
HALO = 16
SP = ("sp_0", "sp_1", "sp_2")
EPS = 1e-06
ROPE_BASE = 10000.0
F32 = jnp.float32
BF16 = jnp.bfloat16
MSG = STATE + 16
KV_AT = 768
GATE_AT = 1024
Q_AT = 1536


def dot(a, b, dims=((1,), (0,)), precision=None):
    return lax.dot_general(
        a, b, (dims, ((), ())), preferred_element_type=F32, precision=precision
    )


def split_bf16(value, parts):
    pieces = []
    for _ in range(parts):
        piece = value.astype(BF16)
        pieces.append(piece)
        value = value - piece.astype(F32)
    return pieces


def spread(value, spread_matrix, parts):
    pieces = [p.astype(F32) for p in split_bf16(value, parts)]
    joined = jnp.concatenate(pieces, axis=1).astype(BF16)
    matrix = jnp.concatenate([spread_matrix] * parts, axis=0)
    return dot(joined, matrix)


def spread_matrix():
    shape = (2 * HEADS, 2 * HEADS * HEAD_DIM)
    rows = lax.broadcasted_iota(jnp.int32, shape, 0)
    first = lax.broadcasted_iota(jnp.int32, shape, 1) - rows * HEAD_DIM
    return jnp.where((first >= 0) & (first < HEAD_DIM), 1.0, 0.0).astype(BF16)


def project_kernel(normed, a_ref, b_ref, out_ref, step_ref):
    count = step_ref.shape[0]
    tile = 256

    def column(j, carry):
        cols = pl.ds(pl.multiple_of(j * tile, tile), tile)
        out_ref[:, cols] = dot(normed[...], a_ref[:, cols]).astype(BF16)
        return carry

    tiles = WIDTH_A // tile
    lax.fori_loop(0, tiles, column, 0)
    step_ref[...] = dot(normed[0:count, :], a_ref[:, tiles * tile : WIDTH_A])
    out_ref[:, tiles * tile : (tiles + 1) * tile] = dot(
        normed[...], b_ref[:, WIDTH_B - tile : WIDTH_B]
    ).astype(BF16)


def project(normed, count, a, b):
    rows, width = normed.shape
    columns = 2048
    vmem = pl.BlockSpec(memory_space=pltpu.VMEM)
    return pl.pallas_call(
        project_kernel,
        in_specs=[vmem] * 3,
        out_specs=[vmem] * 2,
        out_shape=[
            jax.ShapeDtypeStruct((rows, columns), BF16),
            jax.ShapeDtypeStruct((count, 128), F32),
        ],
        compiler_params=pltpu.CompilerParams(vmem_limit_bytes=12 << 20),
        cost_estimate=pl.CostEstimate(
            flops=2 * rows * width * (columns + 128),
            bytes_accessed=2 * (rows * width + width * columns + rows * columns),
            transcendentals=0,
        ),
        name="project",
    )(normed, a, b)


def conv_state_kernel(
    cin_ref, taps_x_ref, taps_b_ref, taps_c_ref, step_ref, rate_ref,
    conv_ref, col_ref, row_ref, piece_ref, etot_ref, msg_ref, win, near,
):
    count = cin_ref.shape[0] - 2 * HALO
    blocks = count // BLOCK
    channels = HEADS * HEAD_DIM
    spread_m = spread_matrix()
    taps = jnp.concatenate([t[...].astype(F32) for t in (taps_x_ref, taps_b_ref, taps_c_ref)], axis=1)
    lane16 = lax.broadcasted_iota(jnp.int32, (BLOCK, 2 * HEADS), 1)
    forward16 = lane16 < HEADS
    tri = (
        lax.broadcasted_iota(jnp.int32, (BLOCK, BLOCK), 0)
        >= lax.broadcasted_iota(jnp.int32, (BLOCK, BLOCK), 1)
    ).astype(F32)
    win[pl.ds(0, HALO), :] = cin_ref[pl.ds(count, HALO), :].astype(F32)
    win[pl.ds(HALO + count, HALO), :] = cin_ref[pl.ds(count + HALO, HALO), :].astype(F32)

    def fill(i, carry):
        start = pl.multiple_of(i * BLOCK, BLOCK)
        win[pl.ds(HALO + start, BLOCK), :] = cin_ref[pl.ds(start, BLOCK), :].astype(F32)
        return carry

    lax.fori_loop(0, blocks, fill, 0)

    def one(i, total):
        start = pl.multiple_of(i * BLOCK, BLOCK)
        rows = pl.ds(start, BLOCK)
        near[...] = win[pl.ds(start, BLOCK + 2 * HALO), :]
        acc = near[HALO - 2 : HALO - 2 + BLOCK, :] * taps[0:1, :]
        for tap in range(1, 5):
            first = HALO - 2 + tap
            acc = acc + near[first : first + BLOCK, :] * taps[tap : tap + 1, :]
        conv = (acc * jax.nn.sigmoid(acc)).astype(BF16)
        conv_ref[rows, :] = conv
        raw = step_ref[rows, 0 : 2 * HEADS]
        step = jnp.maximum(raw, 0.0) + jnp.log1p(jnp.exp(-jnp.abs(raw)))
        rate = jnp.concatenate([rate_ref[:, rows], jnp.zeros((BLOCK - 2 * HEADS, BLOCK), F32)], axis=0)
        decay = -jnp.exp(rate.T[:, 0 : 2 * HEADS]) * step
        cum = dot(tri, decay, precision=lax.Precision.HIGHEST)
        tot = cum[BLOCK - 1 : BLOCK, :]
        col = jnp.where(forward16, cum, cum - decay)
        col_ref[rows, 0 : 2 * HEADS] = col
        col_ref[rows, 2 * HEADS : 4 * HEADS] = jnp.broadcast_to(tot, (BLOCK, 2 * HEADS))
        both = jnp.concatenate([col, step, jnp.zeros((BLOCK, 128 - 4 * HEADS), F32)], axis=1)
        row_ref[i] = both.T[0 : 4 * HEADS, :]
        weight = jnp.exp(jnp.where(forward16, tot - col, col)) * step
        wide = spread(weight, spread_m, 2)
        xs = conv[:, 0:channels].astype(F32)
        scaled = (jnp.concatenate([xs, xs], axis=1) * wide).astype(BF16)
        inflow = conv[:, channels : channels + STATE]
        piece_ref[i] = dot(inflow, scaled, ((0,), (0,)))
        etot_ref[i] = spread(jnp.exp(jnp.broadcast_to(tot, (8, 2 * HEADS))), spread_m, 3)
        return total + tot

    total = lax.fori_loop(0, blocks, one, jnp.zeros((1, 2 * HEADS), F32))
    forward = piece_ref[0, :, 0:channels]
    backward = piece_ref[blocks - 1, :, channels : 2 * channels]
    for i in range(1, blocks):
        forward = etot_ref[i, 0:1, 0:channels] * forward + piece_ref[i, :, 0:channels]
        k = blocks - 1 - i
        backward = (
            etot_ref[k, 0:1, channels : 2 * channels] * backward
            + piece_ref[k, :, channels : 2 * channels]
        )
    spread_total = spread(jnp.broadcast_to(total, (16, 2 * HEADS)), spread_m, 3)
    hi, mid, lo = split_bf16(spread_total, 3)
    which = lax.broadcasted_iota(jnp.int32, (16, 2 * channels), 0)
    tail = jnp.where(
        which == 0, hi.astype(F32), jnp.where(which == 1, mid.astype(F32), lo.astype(F32))
    ).astype(BF16)
    for e, state in enumerate((forward, backward)):
        for pair in range(channels // 128):
            lanes = slice(pair * 128, pair * 128 + 128)
            msg_ref[e, pair, 0:STATE, :] = state[:, lanes].astype(BF16)
            msg_ref[e, pair, STATE:MSG, :] = tail[:, e * channels + pair * 128 : e * channels + pair * 128 + 128]


def conv_state(proj, taps, step_raw, rate):
    count = step_raw.shape[0]
    width = sum(t.shape[1] for t in taps)
    blocks = count // BLOCK
    channels = HEADS * HEAD_DIM
    whole = lambda shape: pl.BlockSpec(shape, lambda i: (0,) * len(shape))
    return pl.pallas_call(
        conv_state_kernel,
        grid=(1,),
        in_specs=[
            pl.BlockSpec((proj.shape[0], width), lambda i: (0, 0)),
            *(whole(t.shape) for t in taps),
            whole(step_raw.shape),
            whole(rate.shape),
        ],
        out_specs=[
            whole((count, width)),
            whole((count, 4 * HEADS)),
            whole((blocks, 4 * HEADS, BLOCK)),
            whole((blocks, STATE, 2 * channels)),
            whole((blocks, 8, 2 * channels)),
            whole((2, channels // 128, MSG, 128)),
        ],
        out_shape=[
            jax.ShapeDtypeStruct((count, width), BF16),
            jax.ShapeDtypeStruct((count, 4 * HEADS), F32),
            jax.ShapeDtypeStruct((blocks, 4 * HEADS, BLOCK), F32),
            jax.ShapeDtypeStruct((blocks, STATE, 2 * channels), F32),
            jax.ShapeDtypeStruct((blocks, 8, 2 * channels), F32),
            jax.ShapeDtypeStruct((2, channels // 128, MSG, 128), BF16),
        ],
        scratch_shapes=[
            pltpu.VMEM((count + 2 * HALO, width), F32),
            pltpu.VMEM((BLOCK + 2 * HALO, width), F32),
        ],
        compiler_params=pltpu.CompilerParams(vmem_limit_bytes=18 << 20),
        cost_estimate=pl.CostEstimate(
            flops=2 * count * STATE * 2 * channels, bytes_accessed=12 << 20, transcendentals=0
        ),
        name="conv_state",
    )(proj, *taps, step_raw, rate)


def mixer(conv_ref, col_ref, row_ref, piece_ref, etot_ref, in_ref, proj_ref, gain_ref, out_ref, held):
    count = conv_ref.shape[0]
    blocks = count // BLOCK
    channels = HEADS * HEAD_DIM
    spread_m = spread_matrix()
    gain = gain_ref[...].astype(F32)
    for e in range(2):
        state = jnp.concatenate(
            [in_ref[e, p].astype(F32) for p in range(channels // 128)], axis=1
        )
        lanes = slice(e * channels, (e + 1) * channels)
        for i in range(blocks) if e == 0 else reversed(range(blocks)):
            held[i, :, lanes] = state.astype(BF16)
            state = etot_ref[i, 0:1, lanes] * state + piece_ref[i, :, lanes]
    row_at = lax.broadcasted_iota(jnp.int32, (BLOCK, BLOCK), 0)
    col_at = lax.broadcasted_iota(jnp.int32, (BLOCK, BLOCK), 1)
    lower = row_at >= col_at
    diagonal = row_at == col_at
    first_half = col_at < HEAD_DIM
    forward16 = lax.broadcasted_iota(jnp.int32, (BLOCK, 2 * HEADS), 1) < HEADS

    def one(i):
        rows = pl.ds(pl.multiple_of(i * BLOCK, BLOCK), BLOCK)
        inflow = conv_ref[rows, channels : channels + STATE]
        readout = conv_ref[rows, channels + STATE : channels + 2 * STATE]
        inner = dot(readout, inflow, ((1,), (1,)))
        col = col_ref[rows, 0 : 2 * HEADS]
        tot = col_ref[rows, 2 * HEADS : 4 * HEADS]
        reach = spread(jnp.exp(jnp.where(forward16, col, tot - col)), spread_m, 2)
        far = dot(readout, held[i]) * reach
        parts = []
        for pair in range(HEADS // 2):
            weights = []
            for h in (2 * pair, 2 * pair + 1):
                b = HEADS + h
                arg = jnp.where(
                    lower,
                    col[:, h : h + 1] - row_ref[i, h : h + 1, :],
                    row_ref[i, b : b + 1, :] - col[:, b : b + 1],
                )
                step_f = row_ref[i, 2 * HEADS + h : 2 * HEADS + h + 1, :]
                step_b = row_ref[i, 2 * HEADS + b : 2 * HEADS + b + 1, :]
                step = jnp.where(lower, step_f, step_b) + jnp.where(diagonal, step_b, 0.0)
                weights.append((inner * jnp.exp(arg) * step).astype(BF16))
            xs = conv_ref[rows, pair * 128 : pair * 128 + 128]
            zero = jnp.zeros_like(xs)
            stacked = jnp.concatenate(
                [jnp.where(first_half, xs, zero), jnp.where(first_half, zero, xs)], axis=0
            )
            parts.append(dot(jnp.concatenate(weights, axis=1), stacked))
        y = jnp.concatenate(parts, axis=1) + far[:, 0:channels] + far[:, channels:]
        gate = proj_ref[rows, GATE_AT : GATE_AT + channels].astype(F32)
        y = y * (gate * jax.nn.sigmoid(gate))
        y = y * lax.rsqrt(jnp.mean(y * y, axis=1, keepdims=True) + EPS)
        out_ref[rows, :] = (y * gain).astype(BF16)

    return one


def attention(
    count, proj_ref, before_ref, after_ref, freq_ref, sink_ref,
    out_ref, log_ref, keys, values, by_row, by_col,
):
    blocks = count // BLOCK
    place = lax.axis_index(SP)
    lane = lax.broadcasted_iota(jnp.int32, (BLOCK, 128), 1)
    low_quarter = lane % 32 < 16
    first_half = lane < HEAD_DIM
    row_lane = (lane % HEAD_DIM < 32)[0:GRID_W]

    grid_rows = by_row.shape[1]
    first_row = place * (count // GRID_W) - WINDOW // GRID_W
    sign = jnp.where(low_quarter, -1.0, 1.0)
    for ref, first, length in ((by_row, first_row, grid_rows), (by_col, 0, GRID_W)):
        at = lax.broadcasted_iota(jnp.int32, (length, 128), 0) + first
        angle = at.astype(F32) * freq_ref[0:1, :]
        ref[0] = jnp.cos(angle)
        ref[1] = jnp.sin(angle) * sign[0:length]

    def tables(slot):
        out = []
        for kind in range(2):
            parts = []
            for r in range(BLOCK // GRID_W):
                row = by_row[kind, pl.ds(slot * (BLOCK // GRID_W) + r, 1), :]
                parts.append(jnp.where(row_lane, row, by_col[kind]))
            out.append(jnp.concatenate(parts, axis=0))
        return out

    def turn(value, table):
        wide = value.astype(F32)
        other = jnp.where(low_quarter, pltpu.roll(wide, 112, 1), pltpu.roll(wide, 16, 1))
        return (wide * table[0] + other * table[1]).astype(BF16)

    def store(raw, slot):
        rows = pl.ds(pl.multiple_of(slot * BLOCK, BLOCK), BLOCK)
        key = turn(raw[:, 0:128], tables(slot)).astype(F32)
        swapped = pltpu.roll(key, 64, 1)
        keys[0, rows, :] = jnp.where(first_half, key, swapped).astype(BF16)
        keys[1, rows, :] = jnp.where(first_half, swapped, key).astype(BF16)
        values[:, rows] = raw[:, 128:256].astype(F32).T.astype(BF16)

    def own_keys():
        def fill(i, carry):
            rows = pl.ds(pl.multiple_of(i * BLOCK, BLOCK), BLOCK)
            store(proj_ref[rows, KV_AT : KV_AT + 256], i + 1)
            return carry

        lax.fori_loop(0, blocks, fill, 0)

    def edge_keys():
        store(before_ref[...], 0)
        store(after_ref[...], blocks + 1)

    key_at = lax.broadcasted_iota(jnp.int32, (3 * BLOCK, 2 * BLOCK), 0)
    query_at = lax.broadcasted_iota(jnp.int32, (3 * BLOCK, 2 * BLOCK), 1) % BLOCK
    in_band = (key_at >= query_at) & (key_at <= query_at + 2 * WINDOW)
    first_row_half = lax.broadcasted_iota(jnp.int32, (1, 2 * BLOCK), 1) < BLOCK
    start_at = -place * count
    end_at = start_at + count * lax.axis_size(SP)

    def one(i):
        start = pl.multiple_of(i * BLOCK, BLOCK)
        rows = pl.ds(start, BLOCK)
        here = key_at + (start - WINDOW)
        valid = in_band & (here >= start_at) & (here < end_at)
        table = tables(i + 1)
        band = pl.ds(start, 3 * BLOCK)
        for pair in range(HEADS // 2):
            group = pair // 2
            lanes = slice(pair * 128, pair * 128 + 128)
            q = (turn(proj_ref[rows, Q_AT + pair * 128 : Q_AT + pair * 128 + 128], table).astype(F32) * HEAD_DIM ** (-0.5)).astype(BF16)
            zero = jnp.zeros_like(q)
            both = jnp.concatenate(
                [jnp.where(first_half, q, zero), jnp.where(first_half, zero, q)], axis=0
            )
            scores = dot(keys[group, band, :], both, ((1,), (1,)))
            scores = jnp.where(valid, scores, -1e30)
            sink = jnp.where(first_row_half, sink_ref[2 * pair], sink_ref[2 * pair + 1])
            top = jnp.maximum(jnp.max(scores, axis=0, keepdims=True), sink)
            expo = jnp.exp(scores - top)
            total = jnp.sum(expo, axis=0, keepdims=True) + jnp.exp(sink - top)
            mine = values[group * HEAD_DIM : (group + 1) * HEAD_DIM, band]
            o = dot(mine, expo.astype(BF16)) / total
            turned = jnp.concatenate([o[:, 0:BLOCK], o[:, BLOCK:]], axis=0).T
            out_ref[rows, lanes] = turned.astype(BF16)
            log = top + jnp.log(total)
            log_ref[2 * pair : 2 * pair + 1, rows] = log[:, 0:BLOCK]
            log_ref[2 * pair + 1 : 2 * pair + 2, rows] = log[:, BLOCK:]

    return own_keys, edge_keys, one


LINKS = ("z+", "z-", "y+", "y-")
WIDTH_A = 1920
WIDTH_B = 1280


def ring(kind, link_axis, other_at, length, total, cut):
    out = []
    for sign in (1, -1):
        previous = None
        for step in range(length // 2):
            last = step == length // 2 - 1
            cols = (0, total)
            if last:
                cols = (0, cut) if sign == 1 else (cut, total)
            name = (kind, link_axis, other_at, sign, step)
            out.append(dict(
                name=name, kind=kind, axis=link_axis, sign=sign,
                along=-sign * step, other=other_at, cols=cols, after=previous,
            ))
            previous = name
    return out


def transfers(length_z, length_y):
    sends = []
    for kind, first, length, second, length2, total, cut in (
        ("A", "z", length_z, "y", length_y, WIDTH_A, 1024),
        ("B", "y", length_y, "z", length_z, WIDTH_B, 640),
    ):
        sends += ring(kind, first, 0, length, total, cut)
        for offset in range(-(length // 2) + 1, length // 2 + 1):
            sends += ring(kind, second, offset, length2, total, cut)
    for s in sends:
        length, first = (length_z, "z") if s["kind"] == "A" else (length_y, "y")
        s["needs"] = []
        if s["after"] is not None:
            s["needs"] = [s["after"]]
        elif s["axis"] != first and s["other"] != 0:
            d = s["other"]
            if abs(d) == length // 2:
                s["needs"] = [(s["kind"], first, 0, sign, length // 2 - 1) for sign in (1, -1)]
            else:
                s["needs"] = [(s["kind"], first, 0, -1 if d > 0 else 1, abs(d) - 1)]
    return sends


def arrival_order(sends):
    import heapq

    rate, hop = 46.6e3, 1.9
    free = dict.fromkeys(LINKS, 0.0)
    left = {s["name"]: len(s["needs"]) for s in sends}
    followers = {}
    for s in sends:
        for need in s["needs"]:
            followers.setdefault(need, []).append(s)
    heap, order, first = [], [], []

    def start(s, now):
        link = s["axis"] + ("+" if s["sign"] == 1 else "-")
        size = 32 * 2 * (s["cols"][1] - s["cols"][0])
        free[link] = max(free[link], now) + size / rate
        heapq.heappush(heap, (free[link] + hop, len(order), str(s["name"]), s["name"]))

    def rank(s):
        return (s["axis"] != ("z" if s["kind"] == "A" else "y"), s["kind"] != "A")

    for s in sorted((s for s in sends if not s["needs"]), key=rank):
        first.append(s)
        start(s, 0.0)
    end = 0.0
    while heap:
        now, _, _, name = heapq.heappop(heap)
        ready = []
        for s in sorted(followers.get(name, []), key=rank):
            left[s["name"]] -= 1
            if left[s["name"]] == 0:
                ready.append(s)
                start(s, now)
        order.append((name, ready))
        end = now
    return first, order, end


def gather_kernel(
    lengths, tok_ref, gain_ref, step_ref, value_ref, inflow_ref, readout_ref, key_ref, vector_ref,
    gate_ref, query_ref, state_ref, window_ref,
    a_ref, b_ref, normed, before, after, held, send_sem, recv_sem, core_send, core_recv, edge_sem,
    own_sem,
):
    length_z, length_y = lengths
    z, y, c = (lax.axis_index(a) for a in SP)
    other = 1 - c
    mesh_id = pl.DeviceIdType.MESH

    def wrap(value, length):
        return lax.rem(value + length, length)

    steps = {"z": (SP[0], z, length_z), "y": (SP[1], y, length_y)}

    def towards(axis, sign):
        name, at, length = steps[axis]
        return {name: wrap(at + sign, length)}

    flat = (z * length_y + y) * 2 + c
    count = length_z * length_y * 2

    def device_at(index):
        index = wrap(index, count)
        return {
            SP[0]: index // (2 * length_y),
            SP[1]: lax.rem(index // 2, length_y),
            SP[2]: lax.rem(index, 2),
        }

    peers = [{SP[2]: other}] + [towards(a, s) for a in ("z", "y") for s in (1, -1)]
    peers += [device_at(flat + 1), device_at(flat - 1)]
    barrier = pltpu.get_barrier_semaphore()
    for peer in peers:
        pl.semaphore_signal(barrier, inc=1, device_id=peer, device_id_type=mesh_id)

    count_rows = tok_ref.shape[0]
    half = query_ref.shape[1] // 2
    moves = []
    for array, refs in (
        (a_ref, (value_ref, inflow_ref, readout_ref, key_ref, vector_ref, gate_ref, query_ref)),
        (b_ref, (state_ref, window_ref, query_ref)),
    ):
        column = 0
        for ref in refs:
            width = ref.shape[1]
            src = ref
            if ref is query_ref:
                src = ref.at[:, pl.ds(0 if array is a_ref else half, half)]
                width = half
            moves.append((src, array.at[z, y, c, :, pl.ds(column, width)]))
            column += width
    moves.append((tok_ref, held))
    moves = [pltpu.make_async_copy(*move, own_sem.at[i]) for i, move in enumerate(moves)]
    for move in moves:
        move.start()
    step = step_ref[...].astype(F32)
    rows, cols = step.shape
    step = jnp.concatenate([step, jnp.zeros((rows, 128 - cols), F32)], axis=1)
    step = jnp.concatenate([step, jnp.zeros((128 - rows, 128), F32)], axis=0)
    a_ref[z, y, c, :, WIDTH_A - 128 : WIDTH_A] = step.T[0:cols, :].astype(BF16)
    for move in moves[:-1]:
        move.wait()
    pl.semaphore_wait(barrier, len(peers))

    sends = transfers(length_z, length_y)
    number = {s["name"]: i for i, s in enumerate(sends)}
    by_name = {s["name"]: s for s in sends}

    def block(s, shift):
        along = s["along"] - shift * s["sign"]
        dz, dy = (along, s["other"]) if s["axis"] == "z" else (s["other"], along)
        ref = a_ref if s["kind"] == "A" else b_ref
        cols = pl.ds(s["cols"][0], s["cols"][1] - s["cols"][0])
        return ref.at[wrap(z + dz, length_z), wrap(y + dy, length_y), c, :, cols]

    def copy_of(s, shift):
        i = number[s["name"]]
        ref = block(s, shift)
        return pltpu.make_async_remote_copy(
            src_ref=ref, dst_ref=ref, send_sem=send_sem.at[i], recv_sem=recv_sem.at[i],
            device_id=towards(s["axis"], s["sign"]), device_id_type=mesh_id,
        )

    edge_copies = []
    for k, (index, dst) in enumerate(((flat - 1, after), (flat + 1, before))):
        edge_copies.append(pltpu.make_async_remote_copy(
            src_ref=tok_ref.at[pl.ds(k * (count_rows - HALO), HALO)], dst_ref=dst,
            send_sem=edge_sem.at[k, 0], recv_sem=edge_sem.at[k, 1],
            device_id=device_at(index), device_id_type=mesh_id,
        ))

    gain = gain_ref[...].astype(F32)

    def norm(value):
        wide = value.astype(F32)
        scale = lax.rsqrt(jnp.mean(wide * wide, axis=1, keepdims=True) + EPS)
        return wide * scale * gain

    def norm_block(i, carry):
        rows = pl.ds(pl.multiple_of(i * BLOCK, BLOCK), BLOCK)
        normed[rows, :] = norm(held[rows, :]).astype(BF16)
        return carry

    first, order, _ = arrival_order(sends)
    started = []
    for s in first:
        copy = copy_of(s, 0)
        copy.start()
        started.append(copy)
    for copy in edge_copies:
        copy.start()
    moves[-1].wait()
    lax.fori_loop(0, count_rows // BLOCK, norm_block, 0)

    waiting = {}
    for kind, first_axis, length, second in (("A", "z", length_z, "y"), ("B", "y", length_y, "z")):
        for offset in range(-(length // 2) + 1, length // 2 + 1):
            names = [s["name"] for s in sends
                     if s["kind"] == kind and s["axis"] == second and s["other"] == offset]
            waiting[(kind, offset)] = set(names)
    keys = list(waiting)

    def core_copy(key):
        kind, offset = key
        i = keys.index(key)
        if kind == "A":
            src = a_ref.at[wrap(z + offset, length_z), :, c]
        else:
            src = b_ref.at[:, wrap(y + offset, length_y), c]
        return src, i

    def send_core(key):
        src, i = core_copy(key)
        copy = pltpu.make_async_remote_copy(
            src_ref=src, dst_ref=src, send_sem=core_send.at[i], recv_sem=core_recv.at[i],
            device_id={SP[2]: other}, device_id_type=mesh_id,
        )
        copy.start()
        started.append(copy)

    def wait_core(key):
        kind, offset = key
        i = keys.index(key)
        if kind == "A":
            dst = a_ref.at[wrap(z + offset, length_z), :, other]
        else:
            dst = b_ref.at[:, wrap(y + offset, length_y), other]
        pltpu.make_async_remote_copy(
            src_ref=dst, dst_ref=dst, send_sem=core_send.at[i], recv_sem=core_recv.at[i],
            device_id={SP[2]: other}, device_id_type=mesh_id,
        ).wait_recv()

    for name, ready in order:
        copy_of(by_name[name], 1).wait_recv()
        for s in ready:
            copy = copy_of(s, 0)
            copy.start()
            started.append(copy)
        for key in keys:
            if name in waiting[key]:
                waiting[key].remove(name)
                if not waiting[key]:
                    send_core(key)
    for copy in started:
        copy.wait_send()
    for key in keys:
        wait_core(key)
    for copy in edge_copies:
        copy.wait()
    normed[count_rows : count_rows + HALO, :] = jnp.where(flat > 0, norm(before[...]), 0.0).astype(BF16)
    normed[count_rows + HALO : count_rows + 2 * HALO, :] = jnp.where(
        flat < count - 1, norm(after[...]), 0.0
    ).astype(BF16)


def gather(length_z, length_y, tokens, gain, step, *shards):
    sends = transfers(length_z, length_y)
    groups = length_z + length_y
    vmem = pl.BlockSpec(memory_space=pltpu.VMEM)
    hbm = pl.BlockSpec(memory_space=pl.ANY)
    dma = pltpu.SemaphoreType.DMA
    lead = (length_z, length_y, 2, 32)
    rows, width = tokens.shape
    edge = pltpu.VMEM((HALO, width), BF16)
    a, b, normed = pl.pallas_call(
        functools.partial(gather_kernel, (length_z, length_y)),
        in_specs=[hbm, vmem, vmem] + [hbm] * len(shards),
        out_specs=[vmem] * 3,
        out_shape=[
            jax.ShapeDtypeStruct((*lead, WIDTH_A), BF16),
            jax.ShapeDtypeStruct((*lead, WIDTH_B), BF16),
            jax.ShapeDtypeStruct((rows + 2 * HALO, width), BF16),
        ],
        scratch_shapes=[
            edge, edge, pltpu.VMEM((rows, width), BF16),
            dma((len(sends),)), dma((len(sends),)), dma((groups,)), dma((groups,)), dma((2, 2)),
            dma((len(shards) + 2,)),
        ],
        compiler_params=pltpu.CompilerParams(
            collective_id=2, has_side_effects=True, vmem_limit_bytes=28 << 20
        ),
        cost_estimate=pl.CostEstimate(flops=1 << 24, bytes_accessed=24 << 20, transcendentals=0),
        name="gather",
    )(tokens, gain, step, *shards)
    return a.reshape(-1, WIDTH_A), b.reshape(-1, WIDTH_B), normed


def exchange_kernel(
    rows, msg_ref, proj_ref, freq_ref, sink_ref, out_ref, window_ref, log_ref,
    kv_before_ref, kv_after_ref, keys, values, by_row, by_col, part, turned, by_y, summed, by_z, back, arrived, nxt, final, carry,
    part_sem, y_sem, z_sem, back_sem, final_sem, kv_sem,
):
    z, y, c = (lax.axis_index(a) for a in SP)
    length_z, length_y = lax.axis_size(SP[0]), lax.axis_size(SP[1])
    forward = c == 0
    other = 1 - c
    order_z = jnp.where(forward, z, length_z - 1 - z)
    mesh_id = pl.DeviceIdType.MESH
    peers = [{SP[2]: other}]
    peers += [{SP[1]: lax.rem(y + k, length_y)} for k in range(1, length_y)]
    peers += [{SP[0]: lax.rem(z + k, length_z)} for k in range(1, length_z)]
    flat = (z * length_y + y) * 2 + c
    count = length_z * length_y * 2

    def device_at(index):
        index = lax.rem(index + count, count)
        return {
            SP[0]: index // (2 * length_y),
            SP[1]: lax.rem(index // 2, length_y),
            SP[2]: lax.rem(index, 2),
        }

    peers += [device_at(flat + 1), device_at(flat - 1)]
    barrier = pltpu.get_barrier_semaphore()
    for peer in peers:
        pl.semaphore_signal(barrier, inc=1, device_id=peer, device_id_type=mesh_id)
    pl.semaphore_wait(barrier, len(peers))

    def send(src, dst, sems, peer):
        copy = pltpu.make_async_remote_copy(
            src_ref=src, dst_ref=dst, send_sem=sems.at[0], recv_sem=sems.at[1],
            device_id=peer, device_id_type=mesh_id,
        )
        copy.start()
        return copy

    def state_of(ref, *at):
        return ref[(*at, slice(0, STATE), slice(None))].astype(F32)

    def decay_of(ref, *at):
        tail = ref[(*at, slice(STATE, MSG), slice(None))].astype(F32)
        return tail[0:1] + tail[1:2] + tail[2:3]

    def put(ref, state, decay, *at):
        ref[(*at, slice(0, STATE), slice(None))] = state.astype(BF16)
        hi, mid, lo = (p.astype(F32) for p in split_bf16(decay, 3))
        which = lax.broadcasted_iota(jnp.int32, (MSG - STATE, 128), 0)
        tail = jnp.where(which == 0, hi, jnp.where(which == 1, mid, lo))
        ref[(*at, slice(STATE, MSG), slice(None))] = tail.astype(BF16)

    pairs = msg_ref.shape[1]
    copy = send(msg_ref.at[other], part, part_sem, {SP[2]: other})
    kv_cols = pl.ds(KV_AT, kv_before_ref.shape[1])
    kv_copies = [
        send(
            proj_ref.at[pl.ds(rows - WINDOW, WINDOW), kv_cols], kv_before_ref, kv_sem.at[0],
            device_at(flat + 1),
        ),
        send(proj_ref.at[pl.ds(0, WINDOW), kv_cols], kv_after_ref, kv_sem.at[1], device_at(flat - 1)),
    ]
    own_keys, edge_keys, attend = attention(
        rows, proj_ref, kv_before_ref, kv_after_ref, freq_ref, sink_ref,
        window_ref, log_ref, keys, values, by_row, by_col,
    )

    def attend_blocks(first, last):
        def one(i, carry):
            attend(i)
            return carry

        lax.fori_loop(first, last, one, 0)

    blocks = rows // BLOCK
    own_keys()
    copy.wait()
    for j in range(pairs):
        decay = decay_of(part, j)
        put(
            turned,
            jnp.exp(decay) * state_of(msg_ref, c, j) + state_of(part, j),
            decay + decay_of(msg_ref, c, j),
            j,
        )
    copies = []
    for k in range(1, length_y):
        to = lax.rem(y + k, length_y)
        copies.append(send(turned.at[to], by_y.at[k], y_sem.at[k], {SP[1]: to}))
    by_y[0] = turned[y]
    attend_blocks(1, 2)
    for copy in copies:
        copy.wait()
    before = []
    state = jnp.zeros((STATE, 128), F32)
    decay = jnp.zeros((1, 128), F32)
    for q in range(length_y):
        before.append((state, decay))
        slot = jnp.where(forward, lax.rem(y - q + length_y, length_y), lax.rem(y + 1 + q, length_y))
        step = decay_of(by_y, slot)
        state = jnp.exp(step) * state + state_of(by_y, slot)
        decay = decay + step
    put(summed, state, decay)
    for k in range(1, length_z):
        to = lax.rem(z + k, length_z)

        @pl.when((z + k >= length_z) == (c == 1))
        def _():
            send(summed, by_z.at[k], z_sem.at[k], {SP[0]: to})

    carry[...] = jnp.zeros_like(carry)
    attend_blocks(2, blocks - 1)
    for distance in reversed(range(1, length_z)):
        slot = jnp.where(forward, distance, length_z - distance)

        @pl.when(order_z >= distance)
        def _():
            pltpu.make_async_remote_copy(
                src_ref=summed, dst_ref=by_z.at[slot], send_sem=z_sem.at[slot, 0],
                recv_sem=z_sem.at[slot, 1], device_id={SP[0]: z}, device_id_type=mesh_id,
            ).wait_recv()
            carry[...] = jnp.exp(decay_of(by_z, slot)) * carry[...] + state_of(by_z, slot)

    for k in range(1, length_z):
        to = lax.rem(z + k, length_z)

        @pl.when((z + k >= length_z) == (c == 1))
        def _():
            pltpu.make_async_remote_copy(
                src_ref=summed, dst_ref=by_z.at[k], send_sem=z_sem.at[k, 0],
                recv_sem=z_sem.at[k, 1], device_id={SP[0]: to}, device_id_type=mesh_id,
            ).wait_send()

    incoming = carry[...]
    for q in range(length_y):
        to = jnp.where(forward, q, length_y - 1 - q)
        state, decay = before[q]
        back[to] = (jnp.exp(decay) * incoming + state).astype(BF16)
    copies = []
    for k in range(1, length_y):
        to = lax.rem(y + k, length_y)
        copies.append(send(back.at[to], arrived.at[k], back_sem.at[k], {SP[1]: to}))
    arrived[0] = back[y]
    for copy in kv_copies:
        copy.wait()
    edge_keys()
    attend(0)
    for copy in copies:
        copy.wait()
    for j in range(pairs):
        state = arrived[lax.rem(y - j + length_y, length_y)]
        out_ref[c, j] = state
        nxt[j] = (
            jnp.exp(decay_of(msg_ref, c, j)) * state.astype(F32) + state_of(msg_ref, c, j)
        ).astype(BF16)
    copy = send(nxt, final, final_sem, {SP[2]: other})
    attend(blocks - 1)
    copy.wait()
    out_ref[other] = final[...]


def exchange(message, proj, rows, freqs, sinks, length_z, length_y):
    pairs = message.shape[1]
    channels = HEADS * HEAD_DIM
    tile = (STATE, 128)
    full = (MSG, 128)
    dma = pltpu.SemaphoreType.DMA
    vmem = pl.BlockSpec(memory_space=pltpu.VMEM)
    return pl.pallas_call(
        functools.partial(exchange_kernel, rows),
        in_specs=[vmem, vmem, vmem, pl.BlockSpec(memory_space=pltpu.SMEM)],
        out_specs=[vmem] * 3,
        out_shape=[
            jax.ShapeDtypeStruct((2, pairs, *tile), BF16),
            jax.ShapeDtypeStruct((rows, channels), BF16),
            jax.ShapeDtypeStruct((HEADS, rows), F32),
        ],
        scratch_shapes=[
            pltpu.VMEM((WINDOW, 256), BF16),
            pltpu.VMEM((WINDOW, 256), BF16),
            pltpu.VMEM((2, rows + 2 * BLOCK, 128), BF16),
            pltpu.VMEM((128, rows + 2 * BLOCK), BF16),
            pltpu.VMEM((2, (rows + 2 * WINDOW) // GRID_W, 128), F32),
            pltpu.VMEM((2, GRID_W, 128), F32),
            pltpu.VMEM((pairs, *full), BF16),
            pltpu.VMEM((pairs, *full), BF16),
            pltpu.VMEM((length_y, *full), BF16),
            pltpu.VMEM(full, BF16),
            pltpu.VMEM((length_z, *full), BF16),
            pltpu.VMEM((length_y, *tile), BF16),
            pltpu.VMEM((length_y, *tile), BF16),
            pltpu.VMEM((pairs, *tile), BF16),
            pltpu.VMEM((pairs, *tile), BF16),
            pltpu.VMEM(tile, F32),
            dma((2,)), dma((length_y, 2)), dma((length_z, 2)), dma((length_y, 2)), dma((2,)),
            dma((2, 2)),
        ],
        compiler_params=pltpu.CompilerParams(
            collective_id=1, has_side_effects=True, vmem_limit_bytes=16 << 20
        ),
        cost_estimate=pl.CostEstimate(
            flops=4 * rows * 3 * BLOCK * channels, bytes_accessed=8 << 20, transcendentals=0
        ),
        name="exchange",
    )(message, proj, freqs, sinks)


def finish_kernel(
    window_ref, w_ref, conv_ref, col_ref, row_ref, piece_ref, etot_ref, in_ref, proj_ref, gain_ref,
    out_ref, *refs
):
    state_ref, held, far_out, far_in, near_out, near_in, far_sem, near_sem = refs
    n = lax.axis_size("tp")
    me = lax.axis_index("tp")
    mesh_id = pl.DeviceIdType.MESH
    sides = (1, -1)
    count, channels = state_ref.shape
    mix = mixer(
        conv_ref, col_ref, row_ref, piece_ref, etot_ref, in_ref, proj_ref, gain_ref, state_ref, held
    )
    width = w_ref.shape[0] // n
    half = width // 2
    chunk = far_out.shape[2]
    chunks = count // chunk

    def at(step):
        return lax.rem(me + step + n, n)

    barrier = pltpu.get_barrier_semaphore()
    for side in sides:
        pl.semaphore_signal(barrier, inc=1, device_id={"tp": at(side)}, device_id_type=mesh_id)
    pl.semaphore_wait(barrier, 2)

    def terms(rows, to):
        outs = pl.ds(pl.multiple_of(to * width, width), width)
        return dot(state_ref[rows, :], w_ref[outs, 0:channels], ((1,), (1,))) + dot(
            window_ref[rows, :], w_ref[outs, channels : 2 * channels], ((1,), (1,))
        )

    def far_copy(i, k):
        return pltpu.make_async_remote_copy(
            src_ref=far_out.at[k, i], dst_ref=far_in.at[k, i], send_sem=far_sem.at[k, i, 0],
            recv_sem=far_sem.at[k, i, 1], device_id={"tp": at(sides[k])}, device_id_type=mesh_id,
        )

    def near_copy(i, k):
        return pltpu.make_async_remote_copy(
            src_ref=near_out.at[k, i], dst_ref=near_in.at[k, i], send_sem=near_sem.at[k, i, 0],
            recv_sem=near_sem.at[k, i, 1], device_id={"tp": at(sides[k])}, device_id_type=mesh_id,
        )

    def send_far(i, carry):
        rows = pl.ds(pl.multiple_of(i * chunk, chunk), chunk)
        mix(i)
        value = terms(rows, at(2)).astype(BF16)
        for k in range(2):
            far_out[k, i] = value[:, k * half : (k + 1) * half]
            far_copy(i, k).start()
        return carry

    lax.fori_loop(0, chunks, send_far, 0)

    def send_near(i, carry):
        rows = pl.ds(pl.multiple_of(i * chunk, chunk), chunk)
        for k in range(2):
            value = terms(rows, at(sides[k])).astype(BF16).astype(F32)
            lanes = slice(k * half, (k + 1) * half)
            far_copy(i, k).wait_recv()
            near_out[k, i] = value.astype(BF16)
            near_out[k, i, :, lanes] = (value[:, lanes] + far_in[k, i].astype(F32)).astype(BF16)
            near_copy(i, k).start()
        return carry

    lax.fori_loop(0, chunks, send_near, 0)

    def collect(i, carry):
        rows = pl.ds(pl.multiple_of(i * chunk, chunk), chunk)
        value = terms(rows, me).astype(BF16).astype(F32)
        for k in range(2):
            near_copy(i, k).wait_recv()
            value = value + near_in[k, i].astype(F32)
        out_ref[rows, :] = value.astype(BF16)
        for k in range(2):
            far_copy(i, k).wait_send()
            near_copy(i, k).wait_send()
        return carry

    lax.fori_loop(0, chunks, collect, 0)


def finish(window, weights, mixed_from, n):
    count, channels = window.shape
    width = weights.shape[0] // n
    chunk = BLOCK
    chunks = count // chunk
    vmem = pl.BlockSpec(memory_space=pltpu.VMEM)
    dma = pltpu.SemaphoreType.DMA
    return pl.pallas_call(
        finish_kernel,
        in_specs=[vmem] * (2 + len(mixed_from)),
        out_specs=vmem,
        out_shape=jax.ShapeDtypeStruct((count, width), BF16),
        scratch_shapes=[
            pltpu.VMEM((count, channels), BF16),
            pltpu.VMEM((chunks, STATE, 2 * channels), BF16),
            pltpu.VMEM((2, chunks, chunk, width // 2), BF16),
            pltpu.VMEM((2, chunks, chunk, width // 2), BF16),
            pltpu.VMEM((2, chunks, chunk, width), BF16),
            pltpu.VMEM((2, chunks, chunk, width), BF16),
            dma((2, chunks, 2)), dma((2, chunks, 2)),
        ],
        compiler_params=pltpu.CompilerParams(
            collective_id=3, has_side_effects=True, vmem_limit_bytes=28 << 20
        ),
        cost_estimate=pl.CostEstimate(
            flops=4 * count * channels * width * n, bytes_accessed=8 << 20, transcendentals=0
        ),
        name="finish",
    )(window, weights, *mixed_from)


def flatten_rows(weight):
    return weight.reshape(weight.shape[0], -1)


def shards(
    tokens, input_gain, gate_weight, value_weight, inflow_weight, readout_weight, step_weight,
    conv_values, conv_inflow, conv_readout, log_rate, group_gain, query_weight, key_weight,
    vector_weight, sink_logit, state_out, window_out,
):
    count = tokens.shape[0]
    length_z, length_y = lax.axis_size(SP[0]), lax.axis_size(SP[1])
    quarter = HEAD_DIM // 4
    freqs = ROPE_BASE ** (-(jnp.arange(128) % quarter).astype(F32) / quarter)
    freqs = jnp.broadcast_to(freqs, (8, 128))
    step_turned = step_weight.transpose(1, 2, 0).reshape(2 * HEADS, -1)
    a, b, normed = gather(
        length_z, length_y, tokens, input_gain[None], step_turned, value_weight,
        flatten_rows(inflow_weight), flatten_rows(readout_weight), key_weight, vector_weight,
        gate_weight, query_weight, state_out.T, window_out.T,
    )
    proj, step_raw = project(normed, count, a, b)
    taps = (conv_values, flatten_rows(conv_inflow), flatten_rows(conv_readout))
    rate = log_rate.transpose(0, 2, 1).reshape(2 * HEADS, count)
    conv, col, row, piece, etot, message = conv_state(proj, taps, step_raw, rate)
    incoming, window, logs = exchange(
        message, proj, count, freqs, sink_logit, length_z, length_y
    )
    mixed = finish(
        window, b, (conv, col, row, piece, etot, incoming, proj, group_gain[None]),
        lax.axis_size("tp"),
    )
    return mixed, logs.T


def solution(mesh):
    torus = Mesh(mesh.devices.reshape(8, 4, 2, mesh.shape["tp"]), (*SP, "tp"))
    return jax.shard_map(
        shards,
        mesh=torus,
        in_specs=(
            P(SP, None), P(), P(SP, "tp"), P(SP, "tp"), P(SP, "tp", None), P(SP, "tp", None),
            P(SP, None, "tp"), P(None, "tp"), P(None, "tp", None), P(None, "tp", None),
            P(None, SP, "tp"), P("tp"), P(SP, "tp"), P(SP, "tp"), P(SP, "tp"), P("tp"),
            P("tp", SP), P("tp", SP),
        ),
        out_specs=(P(SP, "tp"), P(SP, "tp")),
        check_vma=False,
    )
```

```python
import functools

import jax
import jax.numpy as jnp
import numpy as np
from jax import lax
from jax.experimental import pallas as pl
from jax.experimental.pallas import tpu as pltpu
from jax.sharding import Mesh
from jax.sharding import PartitionSpec as P

HEAD_DIM = 64
STATE = 128
HEADS = 8
BLOCK = 128
WINDOW = 128
GRID_W = 64
HALO = 16
SP = ("sp_0", "sp_1", "sp_2")
EPS = 1e-06
ROPE_BASE = 10000.0
F32 = jnp.float32
BF16 = jnp.bfloat16
MSG = STATE + 16
KV_AT = 768
GATE_AT = 1024
Q_AT = 1536


def dot(a, b, dims=((1,), (0,)), precision=None):
    return lax.dot_general(
        a, b, (dims, ((), ())), preferred_element_type=F32, precision=precision
    )


def split_bf16(value, parts):
    pieces = []
    for _ in range(parts):
        piece = value.astype(BF16)
        pieces.append(piece)
        value = value - piece.astype(F32)
    return pieces


def spread(value, spread_matrix, parts):
    pieces = [p.astype(F32) for p in split_bf16(value, parts)]
    joined = jnp.concatenate(pieces, axis=1).astype(BF16)
    matrix = jnp.concatenate([spread_matrix] * parts, axis=0)
    return dot(joined, matrix)


def as_row(ref):
    wide = ref[...].astype(F32)
    return jnp.concatenate([wide[i : i + 1, :] for i in range(wide.shape[0])], axis=1)


def spread_matrix():
    shape = (2 * HEADS, 2 * HEADS * HEAD_DIM)
    rows = lax.broadcasted_iota(jnp.int32, shape, 0)
    first = lax.broadcasted_iota(jnp.int32, shape, 1) - rows * HEAD_DIM
    return jnp.where((first >= 0) & (first < HEAD_DIM), 1.0, 0.0).astype(BF16)


def conv_state(
    cin_ref, taps_x_ref, taps_b_ref, taps_c_ref, step_ref, rate_ref,
    conv_ref, col_ref, row_ref, piece_ref, etot_ref, msg_ref, win, near,
):
    count = cin_ref.shape[0] - 2 * HALO
    blocks = count // BLOCK
    channels = HEADS * HEAD_DIM
    spread_m = spread_matrix()
    taps = jnp.concatenate([t[...].astype(F32) for t in (taps_x_ref, taps_b_ref, taps_c_ref)], axis=1)
    lane16 = lax.broadcasted_iota(jnp.int32, (BLOCK, 2 * HEADS), 1)
    forward16 = lane16 < HEADS
    tri = (
        lax.broadcasted_iota(jnp.int32, (BLOCK, BLOCK), 0)
        >= lax.broadcasted_iota(jnp.int32, (BLOCK, BLOCK), 1)
    ).astype(F32)
    win[pl.ds(0, HALO), :] = cin_ref[pl.ds(count, HALO), :].astype(F32)
    win[pl.ds(HALO + count, HALO), :] = cin_ref[pl.ds(count + HALO, HALO), :].astype(F32)

    def fill(i, carry):
        start = pl.multiple_of(i * BLOCK, BLOCK)
        win[pl.ds(HALO + start, BLOCK), :] = cin_ref[pl.ds(start, BLOCK), :].astype(F32)
        return carry

    lax.fori_loop(0, blocks, fill, 0)

    def one(i, total):
        start = pl.multiple_of(i * BLOCK, BLOCK)
        rows = pl.ds(start, BLOCK)
        near[...] = win[pl.ds(start, BLOCK + 2 * HALO), :]
        acc = near[HALO - 2 : HALO - 2 + BLOCK, :] * taps[0:1, :]
        for tap in range(1, 5):
            first = HALO - 2 + tap
            acc = acc + near[first : first + BLOCK, :] * taps[tap : tap + 1, :]
        conv = (acc * jax.nn.sigmoid(acc)).astype(BF16)
        conv_ref[rows, :] = conv
        raw = step_ref[rows, 0 : 2 * HEADS]
        step = jnp.maximum(raw, 0.0) + jnp.log1p(jnp.exp(-jnp.abs(raw)))
        rate = jnp.concatenate([rate_ref[:, rows], jnp.zeros((BLOCK - 2 * HEADS, BLOCK), F32)], axis=0)
        decay = -jnp.exp(rate.T[:, 0 : 2 * HEADS]) * step
        cum = dot(tri, decay, precision=lax.Precision.HIGHEST)
        tot = cum[BLOCK - 1 : BLOCK, :]
        col = jnp.where(forward16, cum, cum - decay)
        col_ref[rows, 0 : 2 * HEADS] = col
        col_ref[rows, 2 * HEADS : 4 * HEADS] = jnp.broadcast_to(tot, (BLOCK, 2 * HEADS))
        both = jnp.concatenate([col, step, jnp.zeros((BLOCK, 128 - 4 * HEADS), F32)], axis=1)
        row_ref[i] = both.T[0 : 4 * HEADS, :]
        weight = jnp.exp(jnp.where(forward16, tot - col, col)) * step
        wide = spread(weight, spread_m, 2)
        xs = conv[:, 0:channels].astype(F32)
        scaled = (jnp.concatenate([xs, xs], axis=1) * wide).astype(BF16)
        inflow = conv[:, channels : channels + STATE]
        piece_ref[i] = dot(inflow, scaled, ((0,), (0,)))
        etot_ref[i] = spread(jnp.exp(jnp.broadcast_to(tot, (8, 2 * HEADS))), spread_m, 3)
        return total + tot

    total = lax.fori_loop(0, blocks, one, jnp.zeros((1, 2 * HEADS), F32))
    forward = piece_ref[0, :, 0:channels]
    backward = piece_ref[blocks - 1, :, channels : 2 * channels]
    for i in range(1, blocks):
        forward = etot_ref[i, 0:1, 0:channels] * forward + piece_ref[i, :, 0:channels]
        k = blocks - 1 - i
        backward = (
            etot_ref[k, 0:1, channels : 2 * channels] * backward
            + piece_ref[k, :, channels : 2 * channels]
        )
    spread_total = spread(jnp.broadcast_to(total, (16, 2 * HEADS)), spread_m, 3)
    hi, mid, lo = split_bf16(spread_total, 3)
    which = lax.broadcasted_iota(jnp.int32, (16, 2 * channels), 0)
    tail = jnp.where(
        which == 0, hi.astype(F32), jnp.where(which == 1, mid.astype(F32), lo.astype(F32))
    ).astype(BF16)
    for e, state in enumerate((forward, backward)):
        for pair in range(channels // 128):
            lanes = slice(pair * 128, pair * 128 + 128)
            msg_ref[e, pair, 0:STATE, :] = state[:, lanes].astype(BF16)
            msg_ref[e, pair, STATE:MSG, :] = tail[:, e * channels + pair * 128 : e * channels + pair * 128 + 128]


def mixer(conv_ref, col_ref, row_ref, piece_ref, etot_ref, in_ref, gate_ref, gain_ref, out_ref, held):
    count = conv_ref.shape[0]
    blocks = count // BLOCK
    channels = HEADS * HEAD_DIM
    spread_m = spread_matrix()
    gain = as_row(gain_ref)
    for e in range(2):
        state = jnp.concatenate(
            [in_ref[e, p].astype(F32) for p in range(channels // 128)], axis=1
        )
        lanes = slice(e * channels, (e + 1) * channels)
        for i in range(blocks) if e == 0 else reversed(range(blocks)):
            held[i, :, lanes] = state.astype(BF16)
            state = etot_ref[i, 0:1, lanes] * state + piece_ref[i, :, lanes]
    row_at = lax.broadcasted_iota(jnp.int32, (BLOCK, BLOCK), 0)
    col_at = lax.broadcasted_iota(jnp.int32, (BLOCK, BLOCK), 1)
    lower = row_at >= col_at
    diagonal = row_at == col_at
    first_half = col_at < HEAD_DIM
    forward16 = lax.broadcasted_iota(jnp.int32, (BLOCK, 2 * HEADS), 1) < HEADS

    def one(i):
        rows = pl.ds(pl.multiple_of(i * BLOCK, BLOCK), BLOCK)
        inflow = conv_ref[rows, channels : channels + STATE]
        readout = conv_ref[rows, channels + STATE : channels + 2 * STATE]
        inner = dot(readout, inflow, ((1,), (1,)))
        col = col_ref[rows, 0 : 2 * HEADS]
        tot = col_ref[rows, 2 * HEADS : 4 * HEADS]
        reach = spread(jnp.exp(jnp.where(forward16, col, tot - col)), spread_m, 2)
        far = dot(readout, held[i]) * reach
        parts = []
        for pair in range(HEADS // 2):
            weights = []
            for h in (2 * pair, 2 * pair + 1):
                b = HEADS + h
                arg = jnp.where(
                    lower,
                    col[:, h : h + 1] - row_ref[i, h : h + 1, :],
                    row_ref[i, b : b + 1, :] - col[:, b : b + 1],
                )
                step_f = row_ref[i, 2 * HEADS + h : 2 * HEADS + h + 1, :]
                step_b = row_ref[i, 2 * HEADS + b : 2 * HEADS + b + 1, :]
                step = jnp.where(lower, step_f, step_b) + jnp.where(diagonal, step_b, 0.0)
                weights.append((inner * jnp.exp(arg) * step).astype(BF16))
            xs = conv_ref[rows, pair * 128 : pair * 128 + 128]
            zero = jnp.zeros_like(xs)
            stacked = jnp.concatenate(
                [jnp.where(first_half, xs, zero), jnp.where(first_half, zero, xs)], axis=0
            )
            parts.append(dot(jnp.concatenate(weights, axis=1), stacked))
        y = jnp.concatenate(parts, axis=1) + far[:, 0:channels] + far[:, channels:]
        gate = gate_ref[rows, :].astype(F32)
        y = y * (gate * jax.nn.sigmoid(gate))
        y = y * lax.rsqrt(jnp.mean(y * y, axis=1, keepdims=True) + EPS)
        out_ref[rows, :] = (y * gain).astype(BF16)

    return one


def attention(
    count, q_ref, kv_ref, before_ref, after_ref, freq_ref, sink_ref,
    out_ref, log_ref, keys, values, by_row, by_col,
):
    blocks = count // BLOCK
    place = lax.axis_index(SP)
    lane = lax.broadcasted_iota(jnp.int32, (BLOCK, 128), 1)
    low_quarter = lane % 32 < 16
    first_half = lane < HEAD_DIM
    row_lane = (lane % HEAD_DIM < 32)[0:GRID_W]

    grid_rows = by_row.shape[1]
    first_row = place * (count // GRID_W) - WINDOW // GRID_W
    sign = jnp.where(low_quarter, -1.0, 1.0)
    for ref, first, length in ((by_row, first_row, grid_rows), (by_col, 0, GRID_W)):
        at = lax.broadcasted_iota(jnp.int32, (length, 128), 0) + first
        angle = at.astype(F32) * freq_ref[0:1, :]
        ref[0] = jnp.cos(angle)
        ref[1] = jnp.sin(angle) * sign[0:length]

    def tables(slot):
        out = []
        for kind in range(2):
            parts = []
            for r in range(BLOCK // GRID_W):
                row = by_row[kind, pl.ds(slot * (BLOCK // GRID_W) + r, 1), :]
                parts.append(jnp.where(row_lane, row, by_col[kind]))
            out.append(jnp.concatenate(parts, axis=0))
        return out

    def turn(value, table):
        wide = value.astype(F32)
        other = jnp.where(low_quarter, pltpu.roll(wide, 112, 1), pltpu.roll(wide, 16, 1))
        return (wide * table[0] + other * table[1]).astype(BF16)

    def store(raw, slot):
        rows = pl.ds(pl.multiple_of(slot * BLOCK, BLOCK), BLOCK)
        key = turn(raw[:, 0:128], tables(slot)).astype(F32)
        swapped = pltpu.roll(key, 64, 1)
        keys[0, rows, :] = jnp.where(first_half, key, swapped).astype(BF16)
        keys[1, rows, :] = jnp.where(first_half, swapped, key).astype(BF16)
        values[:, rows] = raw[:, 128:256].astype(F32).T.astype(BF16)

    def own_keys():
        def fill(i, carry):
            rows = pl.ds(pl.multiple_of(i * BLOCK, BLOCK), BLOCK)
            store(kv_ref[rows, :], i + 1)
            return carry

        lax.fori_loop(0, blocks, fill, 0)

    def edge_keys():
        store(before_ref[...], 0)
        store(after_ref[...], blocks + 1)

    key_at = lax.broadcasted_iota(jnp.int32, (3 * BLOCK, 2 * BLOCK), 0)
    query_at = lax.broadcasted_iota(jnp.int32, (3 * BLOCK, 2 * BLOCK), 1) % BLOCK
    in_band = (key_at >= query_at) & (key_at <= query_at + 2 * WINDOW)
    first_row_half = lax.broadcasted_iota(jnp.int32, (1, 2 * BLOCK), 1) < BLOCK
    start_at = -place * count
    end_at = start_at + count * lax.axis_size(SP)

    def one(i):
        start = pl.multiple_of(i * BLOCK, BLOCK)
        rows = pl.ds(start, BLOCK)
        here = key_at + (start - WINDOW)
        valid = in_band & (here >= start_at) & (here < end_at)
        table = tables(i + 1)
        band = pl.ds(start, 3 * BLOCK)
        for pair in range(HEADS // 2):
            group = pair // 2
            lanes = slice(pair * 128, pair * 128 + 128)
            q = (turn(q_ref[rows, lanes], table).astype(F32) * HEAD_DIM ** (-0.5)).astype(BF16)
            zero = jnp.zeros_like(q)
            both = jnp.concatenate(
                [jnp.where(first_half, q, zero), jnp.where(first_half, zero, q)], axis=0
            )
            scores = dot(keys[group, band, :], both, ((1,), (1,)))
            scores = jnp.where(valid, scores, -1e30)
            sink = jnp.where(first_row_half, sink_ref[2 * pair], sink_ref[2 * pair + 1])
            top = jnp.maximum(jnp.max(scores, axis=0, keepdims=True), sink)
            expo = jnp.exp(scores - top)
            total = jnp.sum(expo, axis=0, keepdims=True) + jnp.exp(sink - top)
            mine = values[group * HEAD_DIM : (group + 1) * HEAD_DIM, band]
            o = dot(mine, expo.astype(BF16)) / total
            turned = jnp.concatenate([o[:, 0:BLOCK], o[:, BLOCK:]], axis=0).T
            out_ref[rows, lanes] = turned.astype(BF16)
            log = top + jnp.log(total)
            log_ref[2 * pair : 2 * pair + 1, rows] = log[:, 0:BLOCK]
            log_ref[2 * pair + 1 : 2 * pair + 2, rows] = log[:, BLOCK:]

    return own_keys, edge_keys, one


LINKS = ("z+", "z-", "y+", "y-")
WIDTH_A = 1920
WIDTH_B = 1280


def ring(kind, link_axis, other_at, length, total, cut):
    out = []
    for sign in (1, -1):
        previous = None
        for step in range(length // 2):
            last = step == length // 2 - 1
            cols = (0, total)
            if last:
                cols = (0, cut) if sign == 1 else (cut, total)
            name = (kind, link_axis, other_at, sign, step)
            out.append(dict(
                name=name, kind=kind, axis=link_axis, sign=sign,
                along=-sign * step, other=other_at, cols=cols, after=previous,
            ))
            previous = name
    return out


def transfers(length_z, length_y):
    sends = []
    for kind, first, length, second, length2, total, cut in (
        ("A", "z", length_z, "y", length_y, WIDTH_A, 1024),
        ("B", "y", length_y, "z", length_z, WIDTH_B, 640),
    ):
        sends += ring(kind, first, 0, length, total, cut)
        for offset in range(-(length // 2) + 1, length // 2 + 1):
            sends += ring(kind, second, offset, length2, total, cut)
    for s in sends:
        length, first = (length_z, "z") if s["kind"] == "A" else (length_y, "y")
        s["needs"] = []
        if s["after"] is not None:
            s["needs"] = [s["after"]]
        elif s["axis"] != first and s["other"] != 0:
            d = s["other"]
            if abs(d) == length // 2:
                s["needs"] = [(s["kind"], first, 0, sign, length // 2 - 1) for sign in (1, -1)]
            else:
                s["needs"] = [(s["kind"], first, 0, -1 if d > 0 else 1, abs(d) - 1)]
    return sends


def arrival_order(sends):
    import heapq

    rate, hop = 46.6e3, 1.9
    free = dict.fromkeys(LINKS, 0.0)
    left = {s["name"]: len(s["needs"]) for s in sends}
    followers = {}
    for s in sends:
        for need in s["needs"]:
            followers.setdefault(need, []).append(s)
    heap, order, first = [], [], []

    def start(s, now):
        link = s["axis"] + ("+" if s["sign"] == 1 else "-")
        size = 32 * 2 * (s["cols"][1] - s["cols"][0])
        free[link] = max(free[link], now) + size / rate
        heapq.heappush(heap, (free[link] + hop, len(order), str(s["name"]), s["name"]))

    def rank(s):
        return (s["axis"] != ("z" if s["kind"] == "A" else "y"), s["kind"] != "A")

    for s in sorted((s for s in sends if not s["needs"]), key=rank):
        first.append(s)
        start(s, 0.0)
    end = 0.0
    while heap:
        now, _, _, name = heapq.heappop(heap)
        ready = []
        for s in sorted(followers.get(name, []), key=rank):
            left[s["name"]] -= 1
            if left[s["name"]] == 0:
                ready.append(s)
                start(s, now)
        order.append((name, ready))
        end = now
    return first, order, end


def gather(
    lengths, small_copies, enter, tok_ref, gain_ref, step_ref, value_ref, inflow_ref, readout_ref, key_ref, vector_ref,
    gate_ref, query_ref, state_ref, window_ref,
    a_ref, b_ref, normed, before, after, held, send_sem, recv_sem, core_send, core_recv, edge_sem,
    own_sem,
):
    length_z, length_y = lengths
    z, y, c = (lax.axis_index(a) for a in SP)
    other = 1 - c
    mesh_id = pl.DeviceIdType.MESH

    def wrap(value, length):
        return lax.rem(value + length, length)

    steps = {"z": (SP[0], z, length_z), "y": (SP[1], y, length_y)}

    def towards(axis, sign):
        name, at, length = steps[axis]
        return {name: wrap(at + sign, length)}

    flat = (z * length_y + y) * 2 + c
    count = length_z * length_y * 2

    def device_at(index):
        index = wrap(index, count)
        return {
            SP[0]: index // (2 * length_y),
            SP[1]: lax.rem(index // 2, length_y),
            SP[2]: lax.rem(index, 2),
        }

    count_rows = tok_ref.shape[0]
    half = query_ref.shape[1] // 2
    moves = []
    for array, refs in (
        (a_ref, (value_ref, inflow_ref, readout_ref, key_ref, vector_ref, gate_ref, query_ref)),
        (b_ref, (state_ref, window_ref, query_ref)),
    ):
        column = 0
        for ref in refs:
            width = ref.shape[1]
            src = ref
            if ref is query_ref:
                src = ref.at[:, pl.ds(0 if array is a_ref else half, half)]
                width = half
            moves.append((src, array.at[z, y, c, :, pl.ds(column, width)]))
            column += width
    moves.append((tok_ref, held))
    moves = [pltpu.make_async_copy(*move, own_sem.at[i]) for i, move in enumerate(moves)]
    for move in moves:
        move.start()
    small_copies()
    step = step_ref[...].astype(F32)
    rows, cols = step.shape
    step = jnp.concatenate([step, jnp.zeros((rows, 128 - cols), F32)], axis=1)
    step = jnp.concatenate([step, jnp.zeros((128 - rows, 128), F32)], axis=0)
    a_ref[z, y, c, :, WIDTH_A - 128 : WIDTH_A] = step.T[0:cols, :].astype(BF16)
    for move in moves[:-1]:
        move.wait()
    enter()

    sends = transfers(length_z, length_y)
    number = {s["name"]: i for i, s in enumerate(sends)}
    by_name = {s["name"]: s for s in sends}

    def block(s, shift):
        along = s["along"] - shift * s["sign"]
        dz, dy = (along, s["other"]) if s["axis"] == "z" else (s["other"], along)
        ref = a_ref if s["kind"] == "A" else b_ref
        cols = pl.ds(s["cols"][0], s["cols"][1] - s["cols"][0])
        return ref.at[wrap(z + dz, length_z), wrap(y + dy, length_y), c, :, cols]

    def copy_of(s, shift):
        i = number[s["name"]]
        ref = block(s, shift)
        return pltpu.make_async_remote_copy(
            src_ref=ref, dst_ref=ref, send_sem=send_sem.at[i], recv_sem=recv_sem.at[i],
            device_id=towards(s["axis"], s["sign"]), device_id_type=mesh_id,
        )

    edge_copies = []
    for k, (index, dst) in enumerate(((flat - 1, after), (flat + 1, before))):
        edge_copies.append(pltpu.make_async_remote_copy(
            src_ref=tok_ref.at[pl.ds(k * (count_rows - HALO), HALO)], dst_ref=dst,
            send_sem=edge_sem.at[k, 0], recv_sem=edge_sem.at[k, 1],
            device_id=device_at(index), device_id_type=mesh_id,
        ))

    gain = as_row(gain_ref)

    def norm(value):
        wide = value.astype(F32)
        scale = lax.rsqrt(jnp.mean(wide * wide, axis=1, keepdims=True) + EPS)
        return wide * scale * gain

    def norm_block(i, carry):
        rows = pl.ds(pl.multiple_of(i * BLOCK, BLOCK), BLOCK)
        normed[rows, :] = norm(held[rows, :]).astype(BF16)
        return carry

    first, order, _ = arrival_order(sends)
    started = []
    for s in first:
        copy = copy_of(s, 0)
        copy.start()
        started.append(copy)
    for copy in edge_copies:
        copy.start()
    moves[-1].wait()
    lax.fori_loop(0, count_rows // BLOCK, norm_block, 0)

    waiting = {}
    for kind, first_axis, length, second in (("A", "z", length_z, "y"), ("B", "y", length_y, "z")):
        for offset in range(-(length // 2) + 1, length // 2 + 1):
            names = [s["name"] for s in sends
                     if s["kind"] == kind and s["axis"] == second and s["other"] == offset]
            waiting[(kind, offset)] = set(names)
    keys = list(waiting)

    def core_copy(key):
        kind, offset = key
        i = keys.index(key)
        if kind == "A":
            src = a_ref.at[wrap(z + offset, length_z), :, c]
        else:
            src = b_ref.at[:, wrap(y + offset, length_y), c]
        return src, i

    def send_core(key):
        src, i = core_copy(key)
        copy = pltpu.make_async_remote_copy(
            src_ref=src, dst_ref=src, send_sem=core_send.at[i], recv_sem=core_recv.at[i],
            device_id={SP[2]: other}, device_id_type=mesh_id,
        )
        copy.start()
        started.append(copy)

    def wait_core(key):
        kind, offset = key
        i = keys.index(key)
        if kind == "A":
            dst = a_ref.at[wrap(z + offset, length_z), :, other]
        else:
            dst = b_ref.at[:, wrap(y + offset, length_y), other]
        pltpu.make_async_remote_copy(
            src_ref=dst, dst_ref=dst, send_sem=core_send.at[i], recv_sem=core_recv.at[i],
            device_id={SP[2]: other}, device_id_type=mesh_id,
        ).wait_recv()

    for name, ready in order:
        copy_of(by_name[name], 1).wait_recv()
        for s in ready:
            copy = copy_of(s, 0)
            copy.start()
            started.append(copy)
        for key in keys:
            if name in waiting[key]:
                waiting[key].remove(name)
                if not waiting[key]:
                    send_core(key)
    for copy in started:
        copy.wait_send()
    for key in keys:
        wait_core(key)
    for copy in edge_copies:
        copy.wait()
    normed[count_rows : count_rows + HALO, :] = jnp.where(flat > 0, norm(before[...]), 0.0).astype(BF16)
    normed[count_rows + HALO : count_rows + 2 * HALO, :] = jnp.where(
        flat < count - 1, norm(after[...]), 0.0
    ).astype(BF16)


def middle(
    normed, a_ref, b_ref, taps_x_ref, taps_b_ref, taps_c_ref, rate_ref, freq_ref, sink_ref,
    out_ref, window_ref, log_ref, gate_ref, conv_ref, col_ref, row_ref, piece_ref, etot_ref,
    cin_ref, kv_ref, q_ref, step_ref, win, near, msg_ref,
    kv_before_ref, kv_after_ref, keys, values, by_row, by_col, part, turned, by_y, summed, by_z,
    back, arrived, nxt, final, carry,
    part_sem, y_sem, z_sem, back_sem, final_sem, kv_sem,
):
    rows = kv_ref.shape[0]
    z, y, c = (lax.axis_index(a) for a in SP)
    length_z, length_y = lax.axis_size(SP[0]), lax.axis_size(SP[1])
    forward = c == 0
    other = 1 - c
    order_z = jnp.where(forward, z, length_z - 1 - z)
    mesh_id = pl.DeviceIdType.MESH
    flat = (z * length_y + y) * 2 + c
    count = length_z * length_y * 2

    def device_at(index):
        index = lax.rem(index + count, count)
        return {
            SP[0]: index // (2 * length_y),
            SP[1]: lax.rem(index // 2, length_y),
            SP[2]: lax.rem(index, 2),
        }

    def project(dst, count, tiles, source, first):
        tile = 256

        def column(j, carry_over):
            cols = pl.ds(pl.multiple_of(j * tile, tile), tile)
            from_cols = pl.ds(pl.multiple_of(first + j * tile, 128), tile)
            dst[:, cols] = dot(normed[0:count, :], source[:, from_cols]).astype(BF16)
            return carry_over

        lax.fori_loop(0, tiles, column, 0)

    project(kv_ref, rows, 1, a_ref, KV_AT)

    def send(src, dst, sems, peer):
        copy = pltpu.make_async_remote_copy(
            src_ref=src, dst_ref=dst, send_sem=sems.at[0], recv_sem=sems.at[1],
            device_id=peer, device_id_type=mesh_id,
        )
        copy.start()
        return copy

    def state_of(ref, *at):
        return ref[(*at, slice(0, STATE), slice(None))].astype(F32)

    def decay_of(ref, *at):
        tail = ref[(*at, slice(STATE, MSG), slice(None))].astype(F32)
        return tail[0:1] + tail[1:2] + tail[2:3]

    def put(ref, state, decay, *at):
        ref[(*at, slice(0, STATE), slice(None))] = state.astype(BF16)
        hi, mid, lo = (p.astype(F32) for p in split_bf16(decay, 3))
        which = lax.broadcasted_iota(jnp.int32, (MSG - STATE, 128), 0)
        tail = jnp.where(which == 0, hi, jnp.where(which == 1, mid, lo))
        ref[(*at, slice(STATE, MSG), slice(None))] = tail.astype(BF16)

    pairs = msg_ref.shape[1]
    kv_copies = [
        send(
            kv_ref.at[pl.ds(rows - WINDOW, WINDOW)], kv_before_ref, kv_sem.at[0],
            device_at(flat + 1),
        ),
        send(kv_ref.at[pl.ds(0, WINDOW)], kv_after_ref, kv_sem.at[1], device_at(flat - 1)),
    ]
    project(cin_ref, rows + 2 * HALO, 3, a_ref, 0)
    step_ref[...] = dot(normed[0:rows, :], a_ref[:, WIDTH_A - 128 : WIDTH_A])
    conv_state(
        cin_ref, taps_x_ref, taps_b_ref, taps_c_ref, step_ref, rate_ref,
        conv_ref, col_ref, row_ref, piece_ref, etot_ref, msg_ref, win, near,
    )
    copy = send(msg_ref.at[other], part, part_sem, {SP[2]: other})
    own_keys, edge_keys, attend = attention(
        rows, q_ref, kv_ref, kv_before_ref, kv_after_ref, freq_ref, sink_ref,
        window_ref, log_ref, keys, values, by_row, by_col,
    )

    def attend_blocks(first, last):
        def one(i, carry):
            attend(i)
            return carry

        lax.fori_loop(first, last, one, 0)

    blocks = rows // BLOCK
    own_keys()
    copy.wait()
    for j in range(pairs):
        decay = decay_of(part, j)
        put(
            turned,
            jnp.exp(decay) * state_of(msg_ref, c, j) + state_of(part, j),
            decay + decay_of(msg_ref, c, j),
            j,
        )
    copies = []
    for k in range(1, length_y):
        to = lax.rem(y + k, length_y)
        copies.append(send(turned.at[to], by_y.at[k], y_sem.at[k], {SP[1]: to}))
    by_y[0] = turned[y]
    project(q_ref.at[:, pl.ds(0, 256)], rows, 1, a_ref, WIDTH_A - 384)
    project(q_ref.at[:, pl.ds(256, 256)], rows, 1, b_ref, WIDTH_B - 256)
    for copy in copies:
        copy.wait()
    before = []
    state = jnp.zeros((STATE, 128), F32)
    decay = jnp.zeros((1, 128), F32)
    for q in range(length_y):
        before.append((state, decay))
        slot = jnp.where(forward, lax.rem(y - q + length_y, length_y), lax.rem(y + 1 + q, length_y))
        step = decay_of(by_y, slot)
        state = jnp.exp(step) * state + state_of(by_y, slot)
        decay = decay + step
    put(summed, state, decay)
    for k in range(1, length_z):
        to = lax.rem(z + k, length_z)

        @pl.when((z + k >= length_z) == (c == 1))
        def _():
            send(summed, by_z.at[k], z_sem.at[k], {SP[0]: to})

    carry[...] = jnp.zeros_like(carry)
    attend_blocks(1, blocks - 1)
    for distance in reversed(range(1, length_z)):
        slot = jnp.where(forward, distance, length_z - distance)

        @pl.when(order_z >= distance)
        def _():
            pltpu.make_async_remote_copy(
                src_ref=summed, dst_ref=by_z.at[slot], send_sem=z_sem.at[slot, 0],
                recv_sem=z_sem.at[slot, 1], device_id={SP[0]: z}, device_id_type=mesh_id,
            ).wait_recv()
            carry[...] = jnp.exp(decay_of(by_z, slot)) * carry[...] + state_of(by_z, slot)

    for k in range(1, length_z):
        to = lax.rem(z + k, length_z)

        @pl.when((z + k >= length_z) == (c == 1))
        def _():
            pltpu.make_async_remote_copy(
                src_ref=summed, dst_ref=by_z.at[k], send_sem=z_sem.at[k, 0],
                recv_sem=z_sem.at[k, 1], device_id={SP[0]: to}, device_id_type=mesh_id,
            ).wait_send()

    incoming = carry[...]
    for q in range(length_y):
        to = jnp.where(forward, q, length_y - 1 - q)
        state, decay = before[q]
        back[to] = (jnp.exp(decay) * incoming + state).astype(BF16)
    copies = []
    for k in range(1, length_y):
        to = lax.rem(y + k, length_y)
        copies.append(send(back.at[to], arrived.at[k], back_sem.at[k], {SP[1]: to}))
    arrived[0] = back[y]
    for copy in kv_copies:
        copy.wait()
    edge_keys()
    attend(0)
    for copy in copies:
        copy.wait()
    for j in range(pairs):
        state = arrived[lax.rem(y - j + length_y, length_y)]
        out_ref[c, j] = state
        nxt[j] = (
            jnp.exp(decay_of(msg_ref, c, j)) * state.astype(F32) + state_of(msg_ref, c, j)
        ).astype(BF16)
    copy = send(nxt, final, final_sem, {SP[2]: other})
    attend(blocks - 1)
    project(gate_ref, rows, 2, a_ref, GATE_AT)
    copy.wait()
    out_ref[other] = final[...]


def finish(
    window_ref, w_ref, conv_ref, col_ref, row_ref, piece_ref, etot_ref, in_ref, gate_ref, gain_ref,
    out_ref, *refs
):
    state_ref, held, far_out, far_in, near_out, near_in, far_sem, near_sem = refs
    n = lax.axis_size("tp")
    me = lax.axis_index("tp")
    mesh_id = pl.DeviceIdType.MESH
    sides = (1, -1)
    count, channels = state_ref.shape
    mix = mixer(
        conv_ref, col_ref, row_ref, piece_ref, etot_ref, in_ref, gate_ref, gain_ref, state_ref, held
    )
    width = w_ref.shape[0] // n
    half = width // 2
    chunk = far_out.shape[2]
    chunks = count // chunk

    def at(step):
        return lax.rem(me + step + n, n)

    def terms(rows, to):
        outs = pl.ds(pl.multiple_of(to * width, width), width)
        return dot(state_ref[rows, :], w_ref[outs, 0:channels], ((1,), (1,))) + dot(
            window_ref[rows, :], w_ref[outs, channels : 2 * channels], ((1,), (1,))
        )

    def far_copy(i, k):
        return pltpu.make_async_remote_copy(
            src_ref=far_out.at[k, i], dst_ref=far_in.at[k, i], send_sem=far_sem.at[k, i, 0],
            recv_sem=far_sem.at[k, i, 1], device_id={"tp": at(sides[k])}, device_id_type=mesh_id,
        )

    def near_copy(i, k):
        return pltpu.make_async_remote_copy(
            src_ref=near_out.at[k, i], dst_ref=near_in.at[k, i], send_sem=near_sem.at[k, i, 0],
            recv_sem=near_sem.at[k, i, 1], device_id={"tp": at(sides[k])}, device_id_type=mesh_id,
        )

    def send_far(i, carry):
        rows = pl.ds(pl.multiple_of(i * chunk, chunk), chunk)
        value = terms(rows, at(2)).astype(BF16)
        for k in range(2):
            far_out[k, i] = value[:, k * half : (k + 1) * half]
            far_copy(i, k).start()

        @pl.when(i + 1 < chunks)
        def _():
            mix(i + 1)

        return carry

    mix(0)
    lax.fori_loop(0, chunks, send_far, 0)

    def send_near(i, carry):
        rows = pl.ds(pl.multiple_of(i * chunk, chunk), chunk)
        for k in range(2):
            value = terms(rows, at(sides[k])).astype(BF16).astype(F32)
            lanes = slice(k * half, (k + 1) * half)
            far_copy(i, k).wait_recv()
            near_out[k, i] = value.astype(BF16)
            near_out[k, i, :, lanes] = (value[:, lanes] + far_in[k, i].astype(F32)).astype(BF16)
            near_copy(i, k).start()
        return carry

    lax.fori_loop(0, chunks, send_near, 0)

    def collect(i, carry):
        rows = pl.ds(pl.multiple_of(i * chunk, chunk), chunk)
        value = terms(rows, me).astype(BF16).astype(F32)
        for k in range(2):
            near_copy(i, k).wait_recv()
            value = value + near_in[k, i].astype(F32)
        out_ref[rows, :] = value.astype(BF16)
        for k in range(2):
            far_copy(i, k).wait_send()
            near_copy(i, k).wait_send()
        return carry

    lax.fori_loop(0, chunks, collect, 0)


def layer_kernel(
    lengths, tok_ref, *refs
):
    length_z, length_y = lengths
    smalls_hbm, refs = refs[:8], refs[8:]
    shards, refs = refs[:9], refs[9:]
    sink_ref, mixed_ref, log_ref = refs[:3]
    smalls, refs = refs[3:11], refs[11:]
    small_sem, a_ref, b_ref, normed = refs[:4]
    gather_refs, refs = refs[4:13], refs[13:]
    incoming, window_ref, gate_ref = refs[:3]
    conv_refs, refs = refs[3:8], refs[8:]
    middle_refs, finish_refs = refs[:29], refs[29:]
    gain_ref, step_ref, taps_x, taps_b, taps_c, rate_ref, freq_ref, group_gain_ref = smalls
    z, y, c = (lax.axis_index(a) for a in SP)
    t = lax.axis_index("tp")
    n = lax.axis_size("tp")
    flat = (z * length_y + y) * 2 + c
    count = length_z * length_y * 2
    peers = [{SP[2]: 1 - c}]
    peers += [{SP[1]: lax.rem(y + k, length_y)} for k in range(1, length_y)]
    peers += [{SP[0]: lax.rem(z + k, length_z)} for k in range(1, length_z)]
    peers += [{"tp": lax.rem(t + k, n)} for k in (1, n - 1)]
    for shift in (1, count - 1):
        index = lax.rem(flat + shift, count)
        peers.append({
            SP[0]: index // (2 * length_y),
            SP[1]: lax.rem(index // 2, length_y),
            SP[2]: lax.rem(index, 2),
        })
    barrier = pltpu.get_barrier_semaphore()
    for peer in peers:
        pl.semaphore_signal(barrier, inc=1, device_id=peer, device_id_type=pl.DeviceIdType.MESH)
    copies = [
        pltpu.make_async_copy(src, dst, small_sem.at[i])
        for i, (src, dst) in enumerate(zip(smalls_hbm, smalls))
    ]
    for copy in copies:
        copy.start()

    def small_copies():
        for copy in copies:
            copy.wait()

    def enter():
        pl.semaphore_wait(barrier, len(peers))

    gather(
        lengths, small_copies, enter, tok_ref, gain_ref, step_ref, *shards,
        a_ref, b_ref, normed, *gather_refs,
    )
    flat_a = a_ref.reshape(length_z * length_y * 64, WIDTH_A)
    flat_b = b_ref.reshape(length_z * length_y * 64, WIDTH_B)
    middle(
        normed, flat_a, flat_b, taps_x, taps_b, taps_c, rate_ref, freq_ref, sink_ref,
        incoming, window_ref, log_ref, gate_ref, *conv_refs, *middle_refs,
    )
    finish(
        window_ref, flat_b, *conv_refs, incoming, gate_ref, group_gain_ref, mixed_ref, *finish_refs
    )


def layer(length_z, length_y, n, tokens, smalls, shards, sinks):
    rows, model = tokens.shape
    channels = HEADS * HEAD_DIM
    width = channels + 2 * STATE
    blocks = rows // BLOCK
    pairs = channels // 128
    tile = (STATE, 128)
    full = (MSG, 128)
    lead = (length_z, length_y, 2, 32)
    sends = len(transfers(length_z, length_y))
    groups = length_z + length_y
    part = model // n
    dma = pltpu.SemaphoreType.DMA
    vmem = pltpu.VMEM
    hbm = pl.BlockSpec(memory_space=pl.ANY)
    scratch = [
        *(vmem(s.shape, s.dtype) for s in smalls),
        dma((len(smalls),)),
        vmem((*lead, WIDTH_A), BF16),
        vmem((*lead, WIDTH_B), BF16),
        vmem((rows + 2 * HALO, model), BF16),
        vmem((HALO, model), BF16), vmem((HALO, model), BF16), vmem((rows, model), BF16),
        dma((sends,)), dma((sends,)), dma((groups,)), dma((groups,)), dma((2, 2)),
        dma((len(shards) + 2,)),
        vmem((2, pairs, *tile), BF16),
        vmem((rows, channels), BF16),
        vmem((rows, channels), BF16),
        vmem((rows, width), BF16),
        vmem((rows, 4 * HEADS), F32),
        vmem((blocks, 4 * HEADS, BLOCK), F32),
        vmem((blocks, STATE, 2 * channels), F32),
        vmem((blocks, 8, 2 * channels), F32),
        vmem((rows + 2 * HALO, width), BF16),
        vmem((rows, 256), BF16),
        vmem((rows, channels), BF16),
        vmem((rows, 128), F32),
        vmem((rows + 2 * HALO, width), F32),
        vmem((BLOCK + 2 * HALO, width), F32),
        vmem((2, pairs, *full), BF16),
        vmem((WINDOW, 256), BF16),
        vmem((WINDOW, 256), BF16),
        vmem((2, rows + 2 * BLOCK, 128), BF16),
        vmem((128, rows + 2 * BLOCK), BF16),
        vmem((2, (rows + 2 * WINDOW) // GRID_W, 128), F32),
        vmem((2, GRID_W, 128), F32),
        vmem((pairs, *full), BF16),
        vmem((pairs, *full), BF16),
        vmem((length_y, *full), BF16),
        vmem(full, BF16),
        vmem((length_z, *full), BF16),
        vmem((length_y, *tile), BF16),
        vmem((length_y, *tile), BF16),
        vmem((pairs, *tile), BF16),
        vmem((pairs, *tile), BF16),
        vmem(tile, F32),
        dma((2,)), dma((length_y, 2)), dma((length_z, 2)), dma((length_y, 2)), dma((2,)),
        dma((2, 2)),
        vmem((rows, channels), BF16),
        vmem((blocks, STATE, 2 * channels), BF16),
        vmem((2, blocks, BLOCK, part // 2), BF16),
        vmem((2, blocks, BLOCK, part // 2), BF16),
        vmem((2, blocks, BLOCK, part), BF16),
        vmem((2, blocks, BLOCK, part), BF16),
        dma((2, blocks, 2)), dma((2, blocks, 2)),
    ]
    return pl.pallas_call(
        functools.partial(layer_kernel, (length_z, length_y)),
        in_specs=[hbm] * (1 + len(smalls) + len(shards)) + [pl.BlockSpec(memory_space=pltpu.SMEM)],
        out_specs=[pl.BlockSpec(memory_space=pltpu.VMEM)] * 2,
        out_shape=[
            jax.ShapeDtypeStruct((rows, part), BF16),
            jax.ShapeDtypeStruct((HEADS, rows), F32),
        ],
        scratch_shapes=scratch,
        compiler_params=pltpu.CompilerParams(
            collective_id=1, has_side_effects=True, vmem_limit_bytes=65_800_000
        ),
        cost_estimate=pl.CostEstimate(flops=1 << 33, bytes_accessed=24 << 20, transcendentals=0),
        name="layer",
    )(tokens, *smalls, *shards, sinks)


def flatten_rows(weight):
    return weight.reshape(weight.shape[0], -1)


def shards(
    tokens, input_gain, gate_weight, value_weight, inflow_weight, readout_weight, step_weight,
    conv_values, conv_inflow, conv_readout, log_rate, group_gain, query_weight, key_weight,
    vector_weight, sink_logit, state_out, window_out,
):
    count = tokens.shape[0]
    length_z, length_y = lax.axis_size(SP[0]), lax.axis_size(SP[1])
    quarter = HEAD_DIM // 4
    powers = (np.arange(128) % quarter).astype(np.float32) / np.float32(quarter)
    freqs = np.broadcast_to(np.float32(ROPE_BASE) ** -powers, (8, 128)).astype(np.float32)
    freqs = jnp.asarray(freqs)
    smalls = (
        input_gain.reshape(-1, 128),
        step_weight.transpose(1, 2, 0).reshape(2 * HEADS, -1),
        conv_values, flatten_rows(conv_inflow), flatten_rows(conv_readout),
        log_rate.transpose(0, 2, 1).reshape(2 * HEADS, count),
        freqs,
        group_gain.reshape(-1, 128),
    )
    shards_here = (
        value_weight, flatten_rows(inflow_weight), flatten_rows(readout_weight), key_weight,
        vector_weight, gate_weight, query_weight, state_out.T, window_out.T,
    )
    mixed, logs = layer(
        length_z, length_y, lax.axis_size("tp"), tokens, smalls, shards_here, sink_logit
    )
    return mixed, logs.T


def solution(mesh):
    torus = Mesh(mesh.devices.reshape(8, 4, 2, mesh.shape["tp"]), (*SP, "tp"))
    return jax.shard_map(
        shards,
        mesh=torus,
        in_specs=(
            P(SP, None), P(), P(SP, "tp"), P(SP, "tp"), P(SP, "tp", None), P(SP, "tp", None),
            P(SP, None, "tp"), P(None, "tp"), P(None, "tp", None), P(None, "tp", None),
            P(None, SP, "tp"), P("tp"), P(SP, "tp"), P(SP, "tp"), P(SP, "tp"), P("tp"),
            P("tp", SP), P("tp", SP),
        ),
        out_specs=(P(SP, "tp"), P(SP, "tp")),
        check_vma=False,
    )
```

```python
import functools
import heapq

import jax
import jax.numpy as jnp
import numpy as np
from jax import lax
from jax.experimental import pallas as pl
from jax.experimental.pallas import tpu as pltpu
from jax.sharding import Mesh
from jax.sharding import PartitionSpec as P

HEAD_DIM = 64
STATE = 128
HEADS = 8
BLOCK = 128
WINDOW = 128
GRID_W = 64
HALO = 16
SP = ("sp_0", "sp_1", "sp_2")
EPS = 1e-06
ROPE_BASE = 10000.0
F32 = jnp.float32
BF16 = jnp.bfloat16
MSG = STATE + 16
KV_AT = 768
Q_AT = 1024
OUT_AT = 512


def dot(a, b, dims=((1,), (0,)), precision=None):
    return lax.dot_general(
        a, b, (dims, ((), ())), preferred_element_type=F32, precision=precision
    )


def split_bf16(value, parts):
    pieces = []
    for _ in range(parts):
        piece = value.astype(BF16)
        pieces.append(piece)
        value = value - piece.astype(F32)
    return pieces


def spread(value, spread_matrix, parts):
    pieces = [p.astype(F32) for p in split_bf16(value, parts)]
    joined = jnp.concatenate(pieces, axis=1).astype(BF16)
    matrix = jnp.concatenate([spread_matrix] * parts, axis=0)
    return dot(joined, matrix)


def as_row(ref):
    wide = ref[...].astype(F32)
    return jnp.concatenate([wide[i : i + 1, :] for i in range(wide.shape[0])], axis=1)


def spread_matrix():
    shape = (2 * HEADS, 2 * HEADS * HEAD_DIM)
    rows = lax.broadcasted_iota(jnp.int32, shape, 0)
    first = lax.broadcasted_iota(jnp.int32, shape, 1) - rows * HEAD_DIM
    return jnp.where((first >= 0) & (first < HEAD_DIM), 1.0, 0.0).astype(BF16)


def conv_state(
    service, cin_ref, taps_x_ref, taps_b_ref, taps_c_ref, step_ref, rate_ref,
    conv_ref, col_ref, row_ref, piece_ref, etot_ref, msg_ref, win, near,
):
    count = cin_ref.shape[0] - 2 * HALO
    blocks = count // BLOCK
    channels = HEADS * HEAD_DIM
    spread_m = spread_matrix()
    taps = jnp.concatenate([t[...].astype(F32) for t in (taps_x_ref, taps_b_ref, taps_c_ref)], axis=1)
    lane16 = lax.broadcasted_iota(jnp.int32, (BLOCK, 2 * HEADS), 1)
    forward16 = lane16 < HEADS
    tri = (
        lax.broadcasted_iota(jnp.int32, (BLOCK, BLOCK), 0)
        >= lax.broadcasted_iota(jnp.int32, (BLOCK, BLOCK), 1)
    ).astype(F32)
    win[pl.ds(0, HALO), :] = cin_ref[pl.ds(count, HALO), :].astype(F32)
    win[pl.ds(HALO + count, HALO), :] = cin_ref[pl.ds(count + HALO, HALO), :].astype(F32)

    def fill(i, carry):
        start = pl.multiple_of(i * BLOCK, BLOCK)
        win[pl.ds(HALO + start, BLOCK), :] = cin_ref[pl.ds(start, BLOCK), :].astype(F32)
        return carry

    lax.fori_loop(0, blocks, fill, 0)
    service(0.5)

    def one(i, total):
        start = pl.multiple_of(i * BLOCK, BLOCK)
        rows = pl.ds(start, BLOCK)
        near[...] = win[pl.ds(start, BLOCK + 2 * HALO), :]
        acc = near[HALO - 2 : HALO - 2 + BLOCK, :] * taps[0:1, :]
        for tap in range(1, 5):
            first = HALO - 2 + tap
            acc = acc + near[first : first + BLOCK, :] * taps[tap : tap + 1, :]
        conv = (acc * jax.nn.sigmoid(acc)).astype(BF16)
        conv_ref[rows, :] = conv
        raw = step_ref[rows, 0 : 2 * HEADS]
        step = jnp.maximum(raw, 0.0) + jnp.log1p(jnp.exp(-jnp.abs(raw)))
        rate = jnp.concatenate([rate_ref[:, rows], jnp.zeros((BLOCK - 2 * HEADS, BLOCK), F32)], axis=0)
        decay = -jnp.exp(rate.T[:, 0 : 2 * HEADS]) * step
        cum = dot(tri, decay, precision=lax.Precision.HIGHEST)
        tot = cum[BLOCK - 1 : BLOCK, :]
        col = jnp.where(forward16, cum, cum - decay)
        col_ref[rows, 0 : 2 * HEADS] = col
        col_ref[rows, 2 * HEADS : 4 * HEADS] = jnp.broadcast_to(tot, (BLOCK, 2 * HEADS))
        both = jnp.concatenate([col, step, jnp.zeros((BLOCK, 128 - 4 * HEADS), F32)], axis=1)
        row_ref[i] = both.T[0 : 4 * HEADS, :]
        weight = jnp.exp(jnp.where(forward16, tot - col, col)) * step
        wide = spread(weight, spread_m, 2)
        xs = conv[:, 0:channels].astype(F32)
        scaled = (jnp.concatenate([xs, xs], axis=1) * wide).astype(BF16)
        inflow = conv[:, channels : channels + STATE]
        piece_ref[i] = dot(inflow, scaled, ((0,), (0,)))
        etot_ref[i] = spread(jnp.exp(jnp.broadcast_to(tot, (8, 2 * HEADS))), spread_m, 3)
        return total + tot

    total = jnp.zeros((1, 2 * HEADS), F32)
    for i in range(0, blocks, 2):
        total = lax.fori_loop(i, i + 2, one, total)
        service(1.7)
    forward = piece_ref[0, :, 0:channels]
    backward = piece_ref[blocks - 1, :, channels : 2 * channels]
    for i in range(1, blocks):
        forward = etot_ref[i, 0:1, 0:channels] * forward + piece_ref[i, :, 0:channels]
        k = blocks - 1 - i
        backward = (
            etot_ref[k, 0:1, channels : 2 * channels] * backward
            + piece_ref[k, :, channels : 2 * channels]
        )
    spread_total = spread(jnp.broadcast_to(total, (16, 2 * HEADS)), spread_m, 3)
    hi, mid, lo = split_bf16(spread_total, 3)
    which = lax.broadcasted_iota(jnp.int32, (16, 2 * channels), 0)
    tail = jnp.where(
        which == 0, hi.astype(F32), jnp.where(which == 1, mid.astype(F32), lo.astype(F32))
    ).astype(BF16)
    for e, state in enumerate((forward, backward)):
        for pair in range(channels // 128):
            lanes = slice(pair * 128, pair * 128 + 128)
            msg_ref[e, pair, 0:STATE, :] = state[:, lanes].astype(BF16)
            msg_ref[e, pair, STATE:MSG, :] = tail[:, e * channels + pair * 128 : e * channels + pair * 128 + 128]


def mixer(conv_ref, col_ref, row_ref, piece_ref, etot_ref, in_ref, gate_ref, gain_ref, out_ref, held):
    count = conv_ref.shape[0]
    blocks = count // BLOCK
    channels = HEADS * HEAD_DIM
    spread_m = spread_matrix()
    gain = as_row(gain_ref)
    for e in range(2):
        state = jnp.concatenate(
            [in_ref[e, p].astype(F32) for p in range(channels // 128)], axis=1
        )
        lanes = slice(e * channels, (e + 1) * channels)
        for i in range(blocks) if e == 0 else reversed(range(blocks)):
            held[i, :, lanes] = state.astype(BF16)
            state = etot_ref[i, 0:1, lanes] * state + piece_ref[i, :, lanes]
    row_at = lax.broadcasted_iota(jnp.int32, (BLOCK, BLOCK), 0)
    col_at = lax.broadcasted_iota(jnp.int32, (BLOCK, BLOCK), 1)
    lower = row_at >= col_at
    diagonal = row_at == col_at
    first_half = col_at < HEAD_DIM
    forward16 = lax.broadcasted_iota(jnp.int32, (BLOCK, 2 * HEADS), 1) < HEADS

    def one(i):
        rows = pl.ds(pl.multiple_of(i * BLOCK, BLOCK), BLOCK)
        inflow = conv_ref[rows, channels : channels + STATE]
        readout = conv_ref[rows, channels + STATE : channels + 2 * STATE]
        inner = dot(readout, inflow, ((1,), (1,)))
        col = col_ref[rows, 0 : 2 * HEADS]
        tot = col_ref[rows, 2 * HEADS : 4 * HEADS]
        reach = spread(jnp.exp(jnp.where(forward16, col, tot - col)), spread_m, 2)
        far = dot(readout, held[i]) * reach
        parts = []
        for pair in range(HEADS // 2):
            weights = []
            for h in (2 * pair, 2 * pair + 1):
                b = HEADS + h
                arg = jnp.where(
                    lower,
                    col[:, h : h + 1] - row_ref[i, h : h + 1, :],
                    row_ref[i, b : b + 1, :] - col[:, b : b + 1],
                )
                step_f = row_ref[i, 2 * HEADS + h : 2 * HEADS + h + 1, :]
                step_b = row_ref[i, 2 * HEADS + b : 2 * HEADS + b + 1, :]
                step = jnp.where(lower, step_f, step_b) + jnp.where(diagonal, step_b, 0.0)
                weights.append((inner * jnp.exp(arg) * step).astype(BF16))
            xs = conv_ref[rows, pair * 128 : pair * 128 + 128]
            zero = jnp.zeros_like(xs)
            stacked = jnp.concatenate(
                [jnp.where(first_half, xs, zero), jnp.where(first_half, zero, xs)], axis=0
            )
            parts.append(dot(jnp.concatenate(weights, axis=1), stacked))
        y = jnp.concatenate(parts, axis=1) + far[:, 0:channels] + far[:, channels:]
        gate = gate_ref[rows, :].astype(F32)
        y = y * (gate * jax.nn.sigmoid(gate))
        y = y * lax.rsqrt(jnp.mean(y * y, axis=1, keepdims=True) + EPS)
        out_ref[rows, :] = (y * gain).astype(BF16)

    return one


def attention(
    count, q_ref, kv_ref, before_ref, after_ref, freq_ref, sink_ref,
    out_ref, log_ref, keys, values, by_row, by_col,
):
    blocks = count // BLOCK
    place = lax.axis_index(SP)
    lane = lax.broadcasted_iota(jnp.int32, (BLOCK, 128), 1)
    low_quarter = lane % 32 < 16
    first_half = lane < HEAD_DIM
    row_lane = (lane % HEAD_DIM < 32)[0:GRID_W]

    grid_rows = by_row.shape[1]
    first_row = place * (count // GRID_W) - WINDOW // GRID_W
    sign = jnp.where(low_quarter, -1.0, 1.0)
    for ref, first, length in ((by_row, first_row, grid_rows), (by_col, 0, GRID_W)):
        at = lax.broadcasted_iota(jnp.int32, (length, 128), 0) + first
        angle = at.astype(F32) * freq_ref[0:1, :]
        ref[0] = jnp.cos(angle)
        ref[1] = jnp.sin(angle) * sign[0:length]

    def tables(slot):
        out = []
        for kind in range(2):
            parts = []
            for r in range(BLOCK // GRID_W):
                row = by_row[kind, pl.ds(slot * (BLOCK // GRID_W) + r, 1), :]
                parts.append(jnp.where(row_lane, row, by_col[kind]))
            out.append(jnp.concatenate(parts, axis=0))
        return out

    def turn(value, table):
        wide = value.astype(F32)
        other = jnp.where(low_quarter, pltpu.roll(wide, 112, 1), pltpu.roll(wide, 16, 1))
        return (wide * table[0] + other * table[1]).astype(BF16)

    def store(raw, slot):
        rows = pl.ds(pl.multiple_of(slot * BLOCK, BLOCK), BLOCK)
        key = turn(raw[:, 0:128], tables(slot)).astype(F32)
        swapped = pltpu.roll(key, 64, 1)
        keys[0, rows, :] = jnp.where(first_half, key, swapped).astype(BF16)
        keys[1, rows, :] = jnp.where(first_half, swapped, key).astype(BF16)
        values[:, rows] = raw[:, 128:256].astype(F32).T.astype(BF16)

    def own_keys():
        def fill(i, carry):
            rows = pl.ds(pl.multiple_of(i * BLOCK, BLOCK), BLOCK)
            store(kv_ref[rows, :], i + 1)
            return carry

        lax.fori_loop(0, blocks, fill, 0)

    def edge_keys():
        store(before_ref[...], 0)
        store(after_ref[...], blocks + 1)

    key_at = lax.broadcasted_iota(jnp.int32, (3 * BLOCK, 2 * BLOCK), 0)
    query_at = lax.broadcasted_iota(jnp.int32, (3 * BLOCK, 2 * BLOCK), 1) % BLOCK
    in_band = (key_at >= query_at) & (key_at <= query_at + 2 * WINDOW)
    first_row_half = lax.broadcasted_iota(jnp.int32, (1, 2 * BLOCK), 1) < BLOCK
    start_at = -place * count
    end_at = start_at + count * lax.axis_size(SP)

    def one(i):
        start = pl.multiple_of(i * BLOCK, BLOCK)
        rows = pl.ds(start, BLOCK)
        here = key_at + (start - WINDOW)
        valid = in_band & (here >= start_at) & (here < end_at)
        table = tables(i + 1)
        band = pl.ds(start, 3 * BLOCK)
        for pair in range(HEADS // 2):
            group = pair // 2
            lanes = slice(pair * 128, pair * 128 + 128)
            q = (turn(q_ref[rows, lanes], table).astype(F32) * HEAD_DIM ** (-0.5)).astype(BF16)
            zero = jnp.zeros_like(q)
            both = jnp.concatenate(
                [jnp.where(first_half, q, zero), jnp.where(first_half, zero, q)], axis=0
            )
            scores = dot(keys[group, band, :], both, ((1,), (1,)))
            scores = jnp.where(valid, scores, -1e30)
            sink = jnp.where(first_row_half, sink_ref[2 * pair], sink_ref[2 * pair + 1])
            top = jnp.maximum(jnp.max(scores, axis=0, keepdims=True), sink)
            expo = jnp.exp(scores - top)
            total = jnp.sum(expo, axis=0, keepdims=True) + jnp.exp(sink - top)
            mine = values[group * HEAD_DIM : (group + 1) * HEAD_DIM, band]
            o = dot(mine, expo.astype(BF16)) / total
            turned = jnp.concatenate([o[:, 0:BLOCK], o[:, BLOCK:]], axis=0).T
            out_ref[rows, lanes] = turned.astype(BF16)
            log = top + jnp.log(total)
            log_ref[2 * pair : 2 * pair + 1, rows] = log[:, 0:BLOCK]
            log_ref[2 * pair + 1 : 2 * pair + 2, rows] = log[:, BLOCK:]

    return own_keys, edge_keys, one


LINKS = ("z+", "z-", "y+", "y-")
EARLY = 1664
LATE = 1536
ROUTES = (
    (("A", 0, 0, 1024, 512, "z"), ("B", 0, 1024, 640, 384, "y")),
    (("C", 1, 0, 896, 512, "z"), ("D", 1, 896, 640, 384, "y")),
)
RATE = 46.6e3
HOP = 1.9


def ring(route, axis, other, length):
    name, array, column, total, cut, _ = route
    out = []
    for sign in (1, -1):
        previous = None
        for step in range(length // 2):
            cols = (column, total)
            if step == length // 2 - 1:
                cols = (column, cut) if sign == 1 else (column + cut, total - cut)
            key = (name, axis, other, sign, step)
            out.append(dict(
                key=key, route=name, array=array, axis=axis, sign=sign, along=-sign * step,
                other=other, cols=cols, needs=[previous] if previous else [],
            ))
            previous = key
    return out


def transfers(routes, lengths):
    sends, groups = [], {}
    for route in routes:
        name, _, _, _, _, first = route
        second = "y" if first == "z" else "z"
        length = lengths[first]
        sends += ring(route, first, 0, length)
        for offset in range(-(length // 2) + 1, length // 2 + 1):
            one = ring(route, second, offset, lengths[second])
            needs = []
            if offset == length // 2:
                needs = [(name, first, 0, sign, length // 2 - 1) for sign in (1, -1)]
            elif offset:
                needs = [(name, first, 0, -1 if offset > 0 else 1, abs(offset) - 1)]
            for s in one:
                s["needs"] = s["needs"] or needs
            sends += one
            groups[(name, offset)] = {s["key"] for s in one}
    return sends, groups


class Flow:
    def __init__(self, number, lengths, arrays, sems):
        self.routes = ROUTES[number]
        self.lengths = lengths
        self.arrays = arrays
        self.send_sem, self.recv_sem, self.core_send, self.core_recv = sems
        self.at = dict(zip("zy", (lax.axis_index(SP[0]), lax.axis_index(SP[1]))))
        self.c = lax.axis_index(SP[2])
        self.sends, self.groups = transfers(self.routes, lengths)
        self.number = {s["key"]: i for i, s in enumerate(self.sends)}
        self.by_key = {s["key"]: s for s in self.sends}
        self.group_keys = list(self.groups)
        self.left = {s["key"]: len(s["needs"]) for s in self.sends}
        self.followers = {}
        for s in self.sends:
            for need in s["needs"]:
                self.followers.setdefault(need, []).append(s)
        self.first_axis = {route[0]: route[5] for route in self.routes}
        self.free = dict.fromkeys(LINKS, 0.0)
        self.heap = []
        self.clock = 0.0
        self.started = []

    def wrap(self, axis, shift):
        length = self.lengths[axis]
        return lax.rem(self.at[axis] + shift + length, length)

    def rank(self, s):
        return (s["axis"] != self.first_axis[s["route"]], s["route"])

    def copy_of(self, s, shift):
        along = s["along"] - shift * s["sign"]
        place = {s["axis"]: along, "y" if s["axis"] == "z" else "z": s["other"]}
        ref = self.arrays[s["array"]].at[
            self.wrap("z", place["z"]), self.wrap("y", place["y"]), self.c, :, pl.ds(*s["cols"])
        ]
        i = self.number[s["key"]]
        to = {SP["zy".index(s["axis"])]: self.wrap(s["axis"], s["sign"])}
        return pltpu.make_async_remote_copy(
            src_ref=ref, dst_ref=ref, send_sem=self.send_sem.at[i], recv_sem=self.recv_sem.at[i],
            device_id=to, device_id_type=pl.DeviceIdType.MESH,
        )

    def core_copy(self, key, c):
        name, offset = key
        i = self.group_keys.index(key)
        route = [r for r in self.routes if r[0] == name][0]
        ref = self.arrays[route[1]]
        cols = pl.ds(route[2], route[3])
        if route[5] == "z":
            ref = ref.at[self.wrap("z", offset), :, c, :, cols]
        else:
            ref = ref.at[:, self.wrap("y", offset), c, :, cols]
        return pltpu.make_async_remote_copy(
            src_ref=ref, dst_ref=ref, send_sem=self.core_send.at[i],
            recv_sem=self.core_recv.at[i], device_id={SP[2]: 1 - self.c},
            device_id_type=pl.DeviceIdType.MESH,
        )

    def launch(self, s):
        copy = self.copy_of(s, 0)
        copy.start()
        self.started.append(copy)
        link = s["axis"] + ("+" if s["sign"] == 1 else "-")
        self.free[link] = max(self.free[link], self.clock) + 64 * s["cols"][1] / RATE
        heapq.heappush(self.heap, (self.free[link] + HOP, len(self.started), s["key"]))

    def begin(self):
        for s in sorted((s for s in self.sends if not s["needs"]), key=self.rank):
            self.launch(s)

    def handle(self):
        _, _, key = heapq.heappop(self.heap)
        self.copy_of(self.by_key[key], 1).wait_recv()
        for s in sorted(self.followers.get(key, []), key=self.rank):
            self.left[s["key"]] -= 1
            if self.left[s["key"]] == 0:
                self.launch(s)
        for group, keys in self.groups.items():
            if key in keys:
                keys.remove(key)
                if not keys:
                    copy = self.core_copy(group, self.c)
                    copy.start()
                    self.started.append(copy)

    def service(self, passed):
        self.clock += passed
        while self.heap and self.heap[0][0] <= self.clock:
            self.handle()

    def drain(self):
        while self.heap:
            self.clock = max(self.clock, self.heap[0][0])
            self.handle()
        for group in self.group_keys:
            self.core_copy(group, 1 - self.c).wait_recv()

    def finish(self):
        for copy in self.started:
            copy.wait_send()


def gather(
    early, late, small_copies, enter, tok_ref, gain_ref, step_ref, value_ref, inflow_ref,
    readout_ref, key_ref, vector_ref, gate_ref, query_ref, state_ref, window_ref,
    normed, before, after, held, edge_sem, own_sem,
):
    z, y, c = (lax.axis_index(a) for a in SP)
    length_z, length_y = early.lengths["z"], early.lengths["y"]
    flat = (z * length_y + y) * 2 + c
    count = length_z * length_y * 2
    count_rows = tok_ref.shape[0]
    a_ref, b_ref = early.arrays

    def device_at(index):
        index = lax.rem(index + count, count)
        return {
            SP[0]: index // (2 * length_y),
            SP[1]: lax.rem(index // 2, length_y),
            SP[2]: lax.rem(index, 2),
        }

    moves = []
    for array, refs in (
        (a_ref, (value_ref, inflow_ref, readout_ref, key_ref, vector_ref, query_ref)),
        (b_ref, (gate_ref, state_ref, window_ref)),
    ):
        column = 0
        for ref in refs:
            width = ref.shape[1]
            moves.append((ref, array.at[z, y, c, :, pl.ds(column, width)]))
            column += width
    moves.append((tok_ref, held))
    moves = [pltpu.make_async_copy(*move, own_sem.at[i]) for i, move in enumerate(moves)]
    for move in moves:
        move.start()
    small_copies()
    step = step_ref[...].astype(F32)
    rows, cols = step.shape
    step = jnp.concatenate([step, jnp.zeros((rows, 128 - cols), F32)], axis=1)
    step = jnp.concatenate([step, jnp.zeros((128 - rows, 128), F32)], axis=0)
    a_ref[z, y, c, :, EARLY - 128 : EARLY] = step.T[0:cols, :].astype(BF16)
    for move in moves[:6]:
        move.wait()
    enter()
    edge_copies = []
    for k, (index, dst) in enumerate(((flat - 1, after), (flat + 1, before))):
        edge_copies.append(pltpu.make_async_remote_copy(
            src_ref=tok_ref.at[pl.ds(k * (count_rows - HALO), HALO)], dst_ref=dst,
            send_sem=edge_sem.at[k, 0], recv_sem=edge_sem.at[k, 1],
            device_id=device_at(index), device_id_type=pl.DeviceIdType.MESH,
        ))
    gain = as_row(gain_ref)

    def norm(value):
        wide = value.astype(F32)
        scale = lax.rsqrt(jnp.mean(wide * wide, axis=1, keepdims=True) + EPS)
        return wide * scale * gain

    def norm_blocks(first, last):
        def norm_block(i, carry):
            rows = pl.ds(pl.multiple_of(i * BLOCK, BLOCK), BLOCK)
            normed[rows, :] = norm(held[rows, :]).astype(BF16)
            return carry

        lax.fori_loop(first, last, norm_block, 0)

    early.begin()
    for copy in edge_copies:
        copy.start()
    for move in moves[6:]:
        move.wait()
    blocks = count_rows // BLOCK
    norm_blocks(0, blocks // 2)
    early.service(4.5)
    norm_blocks(blocks // 2, blocks)
    early.service(2.0)
    for copy in edge_copies:
        copy.wait()
    normed[count_rows : count_rows + HALO, :] = jnp.where(flat > 0, norm(before[...]), 0.0).astype(BF16)
    normed[count_rows + HALO : count_rows + 2 * HALO, :] = jnp.where(
        flat < count - 1, norm(after[...]), 0.0
    ).astype(BF16)
    early.service(1.0)
    while sum(early.left.values()) > 0:
        early.clock = max(early.clock, early.heap[0][0])
        early.handle()
    late.clock = early.clock
    late.free = dict(early.free)
    late.begin()
    early.drain()
    late.service(max(early.clock - late.clock, 0.0))


def middle(
    late, normed, a_ref, b_ref, taps_x_ref, taps_b_ref, taps_c_ref, rate_ref, freq_ref, sink_ref,
    out_ref, window_ref, log_ref, gate_ref, conv_ref, col_ref, row_ref, piece_ref, etot_ref,
    cin_ref, kv_ref, q_ref, step_ref, win, near, msg_ref,
    kv_before_ref, kv_after_ref, keys, values, by_row, by_col, part, turned, by_y, summed, by_z,
    back, arrived, nxt, final, carry,
    part_sem, y_sem, z_sem, back_sem, final_sem, kv_sem,
):
    rows = kv_ref.shape[0]
    z, y, c = (lax.axis_index(a) for a in SP)
    length_z, length_y = lax.axis_size(SP[0]), lax.axis_size(SP[1])
    forward = c == 0
    other = 1 - c
    order_z = jnp.where(forward, z, length_z - 1 - z)
    mesh_id = pl.DeviceIdType.MESH
    flat = (z * length_y + y) * 2 + c
    count = length_z * length_y * 2

    def device_at(index):
        index = lax.rem(index + count, count)
        return {
            SP[0]: index // (2 * length_y),
            SP[1]: lax.rem(index // 2, length_y),
            SP[2]: lax.rem(index, 2),
        }

    def project(dst, count, tiles, source, first):
        tile = 256

        def column(j, carry_over):
            cols = pl.ds(pl.multiple_of(j * tile, tile), tile)
            from_cols = pl.ds(pl.multiple_of(first + j * tile, 128), tile)
            dst[:, cols] = dot(normed[0:count, :], source[:, from_cols]).astype(BF16)
            return carry_over

        lax.fori_loop(0, tiles, column, 0)

    project(kv_ref, rows, 1, a_ref, KV_AT)
    late.service(1.1)

    def send(src, dst, sems, peer):
        copy = pltpu.make_async_remote_copy(
            src_ref=src, dst_ref=dst, send_sem=sems.at[0], recv_sem=sems.at[1],
            device_id=peer, device_id_type=mesh_id,
        )
        copy.start()
        return copy

    def state_of(ref, *at):
        return ref[(*at, slice(0, STATE), slice(None))].astype(F32)

    def decay_of(ref, *at):
        tail = ref[(*at, slice(STATE, MSG), slice(None))].astype(F32)
        return tail[0:1] + tail[1:2] + tail[2:3]

    def put(ref, state, decay, *at):
        ref[(*at, slice(0, STATE), slice(None))] = state.astype(BF16)
        hi, mid, lo = (p.astype(F32) for p in split_bf16(decay, 3))
        which = lax.broadcasted_iota(jnp.int32, (MSG - STATE, 128), 0)
        tail = jnp.where(which == 0, hi, jnp.where(which == 1, mid, lo))
        ref[(*at, slice(STATE, MSG), slice(None))] = tail.astype(BF16)

    pairs = msg_ref.shape[1]
    kv_copies = [
        send(
            kv_ref.at[pl.ds(rows - WINDOW, WINDOW)], kv_before_ref, kv_sem.at[0],
            device_at(flat + 1),
        ),
        send(kv_ref.at[pl.ds(0, WINDOW)], kv_after_ref, kv_sem.at[1], device_at(flat - 1)),
    ]
    project(cin_ref.at[:, pl.ds(0, 256)], rows + 2 * HALO, 1, a_ref, 0)
    late.service(1.1)
    project(cin_ref.at[:, pl.ds(256, 512)], rows + 2 * HALO, 2, a_ref, 256)
    step_ref[...] = dot(normed[0:rows, :], a_ref[:, EARLY - 128 : EARLY])
    late.service(2.8)
    conv_state(
        late.service,
        cin_ref, taps_x_ref, taps_b_ref, taps_c_ref, step_ref, rate_ref,
        conv_ref, col_ref, row_ref, piece_ref, etot_ref, msg_ref, win, near,
    )
    copy = send(msg_ref.at[other], part, part_sem, {SP[2]: other})
    own_keys, edge_keys, attend = attention(
        rows, q_ref, kv_ref, kv_before_ref, kv_after_ref, freq_ref, sink_ref,
        window_ref, log_ref, keys, values, by_row, by_col,
    )

    blocks = rows // BLOCK
    own_keys()
    late.service(1.2)
    copy.wait()
    for j in range(pairs):
        decay = decay_of(part, j)
        put(
            turned,
            jnp.exp(decay) * state_of(msg_ref, c, j) + state_of(part, j),
            decay + decay_of(msg_ref, c, j),
            j,
        )
    copies = []
    for k in range(1, length_y):
        to = lax.rem(y + k, length_y)
        copies.append(send(turned.at[to], by_y.at[k], y_sem.at[k], {SP[1]: to}))
    by_y[0] = turned[y]
    project(q_ref, rows, 2, a_ref, Q_AT)
    late.service(2.4)
    for copy in copies:
        copy.wait()
    before = []
    state = jnp.zeros((STATE, 128), F32)
    decay = jnp.zeros((1, 128), F32)
    for q in range(length_y):
        before.append((state, decay))
        slot = jnp.where(forward, lax.rem(y - q + length_y, length_y), lax.rem(y + 1 + q, length_y))
        step = decay_of(by_y, slot)
        state = jnp.exp(step) * state + state_of(by_y, slot)
        decay = decay + step
    put(summed, state, decay)
    for k in range(1, length_z):
        to = lax.rem(z + k, length_z)

        @pl.when((z + k >= length_z) == (c == 1))
        def _():
            send(summed, by_z.at[k], z_sem.at[k], {SP[0]: to})

    carry[...] = jnp.zeros_like(carry)
    for i in range(1, blocks - 1):
        attend(i)
        late.service(1.9)
    for distance in reversed(range(1, length_z)):
        slot = jnp.where(forward, distance, length_z - distance)

        @pl.when(order_z >= distance)
        def _():
            pltpu.make_async_remote_copy(
                src_ref=summed, dst_ref=by_z.at[slot], send_sem=z_sem.at[slot, 0],
                recv_sem=z_sem.at[slot, 1], device_id={SP[0]: z}, device_id_type=mesh_id,
            ).wait_recv()
            carry[...] = jnp.exp(decay_of(by_z, slot)) * carry[...] + state_of(by_z, slot)

    for k in range(1, length_z):
        to = lax.rem(z + k, length_z)

        @pl.when((z + k >= length_z) == (c == 1))
        def _():
            pltpu.make_async_remote_copy(
                src_ref=summed, dst_ref=by_z.at[k], send_sem=z_sem.at[k, 0],
                recv_sem=z_sem.at[k, 1], device_id={SP[0]: to}, device_id_type=mesh_id,
            ).wait_send()

    incoming = carry[...]
    for q in range(length_y):
        to = jnp.where(forward, q, length_y - 1 - q)
        state, decay = before[q]
        back[to] = (jnp.exp(decay) * incoming + state).astype(BF16)
    copies = []
    for k in range(1, length_y):
        to = lax.rem(y + k, length_y)
        copies.append(send(back.at[to], arrived.at[k], back_sem.at[k], {SP[1]: to}))
    arrived[0] = back[y]
    for copy in kv_copies:
        copy.wait()
    edge_keys()
    attend(0)
    late.service(2.2)
    for copy in copies:
        copy.wait()
    for j in range(pairs):
        state = arrived[lax.rem(y - j + length_y, length_y)]
        out_ref[c, j] = state
        nxt[j] = (
            jnp.exp(decay_of(msg_ref, c, j)) * state.astype(F32) + state_of(msg_ref, c, j)
        ).astype(BF16)
    copy = send(nxt, final, final_sem, {SP[2]: other})
    attend(blocks - 1)
    late.service(2.0)
    late.drain()
    project(gate_ref, rows, 2, b_ref, 0)
    copy.wait()
    out_ref[other] = final[...]


def finish(
    window_ref, w_ref, conv_ref, col_ref, row_ref, piece_ref, etot_ref, in_ref, gate_ref, gain_ref,
    out_ref, *refs
):
    state_ref, held, far_out, far_in, near_out, near_in, far_sem, near_sem = refs
    n = lax.axis_size("tp")
    me = lax.axis_index("tp")
    mesh_id = pl.DeviceIdType.MESH
    sides = (1, -1)
    count, channels = state_ref.shape
    mix = mixer(
        conv_ref, col_ref, row_ref, piece_ref, etot_ref, in_ref, gate_ref, gain_ref, state_ref, held
    )
    width = w_ref.shape[0] // n
    half = width // 2
    chunk = far_out.shape[2]
    chunks = count // chunk

    def at(step):
        return lax.rem(me + step + n, n)

    def terms(rows, to):
        outs = pl.ds(pl.multiple_of(to * width, width), width)
        return dot(state_ref[rows, :], w_ref[outs, OUT_AT : OUT_AT + channels], ((1,), (1,))) + dot(
            window_ref[rows, :], w_ref[outs, OUT_AT + channels : OUT_AT + 2 * channels], ((1,), (1,))
        )

    def far_copy(i, k):
        return pltpu.make_async_remote_copy(
            src_ref=far_out.at[k, i], dst_ref=far_in.at[k, i], send_sem=far_sem.at[k, i, 0],
            recv_sem=far_sem.at[k, i, 1], device_id={"tp": at(sides[k])}, device_id_type=mesh_id,
        )

    def near_copy(i, k):
        return pltpu.make_async_remote_copy(
            src_ref=near_out.at[k, i], dst_ref=near_in.at[k, i], send_sem=near_sem.at[k, i, 0],
            recv_sem=near_sem.at[k, i, 1], device_id={"tp": at(sides[k])}, device_id_type=mesh_id,
        )

    def send_far(i, carry):
        rows = pl.ds(pl.multiple_of(i * chunk, chunk), chunk)
        value = terms(rows, at(2)).astype(BF16)
        for k in range(2):
            far_out[k, i] = value[:, k * half : (k + 1) * half]
            far_copy(i, k).start()

        @pl.when(i + 1 < chunks)
        def _():
            mix(i + 1)

        return carry

    mix(0)
    lax.fori_loop(0, chunks, send_far, 0)

    def send_near(i, carry):
        rows = pl.ds(pl.multiple_of(i * chunk, chunk), chunk)
        for k in range(2):
            value = terms(rows, at(sides[k])).astype(BF16).astype(F32)
            lanes = slice(k * half, (k + 1) * half)
            far_copy(i, k).wait_recv()
            near_out[k, i] = value.astype(BF16)
            near_out[k, i, :, lanes] = (value[:, lanes] + far_in[k, i].astype(F32)).astype(BF16)
            near_copy(i, k).start()
        return carry

    lax.fori_loop(0, chunks, send_near, 0)

    def collect(i, carry):
        rows = pl.ds(pl.multiple_of(i * chunk, chunk), chunk)
        value = terms(rows, me).astype(BF16).astype(F32)
        for k in range(2):
            near_copy(i, k).wait_recv()
            value = value + near_in[k, i].astype(F32)
        out_ref[rows, :] = value.astype(BF16)
        for k in range(2):
            far_copy(i, k).wait_send()
            near_copy(i, k).wait_send()
        return carry

    lax.fori_loop(0, chunks, collect, 0)


def layer_kernel(
    lengths, tok_ref, *refs
):
    length_z, length_y = lengths
    smalls_hbm, refs = refs[:8], refs[8:]
    shards, refs = refs[:9], refs[9:]
    sink_ref, mixed_ref, log_ref = refs[:3]
    smalls, refs = refs[3:11], refs[11:]
    small_sem, a_ref, b_ref, normed = refs[:4]
    gather_refs, refs = refs[4:9], refs[9:]
    flow_sems, refs = (refs[0:4], refs[4:8]), refs[8:]
    incoming, window_ref, gate_ref = refs[:3]
    conv_refs, refs = refs[3:8], refs[8:]
    middle_refs, finish_refs = refs[:29], refs[29:]
    gain_ref, step_ref, taps_x, taps_b, taps_c, rate_ref, freq_ref, group_gain_ref = smalls
    z, y, c = (lax.axis_index(a) for a in SP)
    t = lax.axis_index("tp")
    n = lax.axis_size("tp")
    flat = (z * length_y + y) * 2 + c
    count = length_z * length_y * 2
    peers = [{SP[2]: 1 - c}]
    peers += [{SP[1]: lax.rem(y + k, length_y)} for k in range(1, length_y)]
    peers += [{SP[0]: lax.rem(z + k, length_z)} for k in range(1, length_z)]
    peers += [{"tp": lax.rem(t + k, n)} for k in (1, n - 1)]
    for shift in (1, count - 1):
        index = lax.rem(flat + shift, count)
        peers.append({
            SP[0]: index // (2 * length_y),
            SP[1]: lax.rem(index // 2, length_y),
            SP[2]: lax.rem(index, 2),
        })
    barrier = pltpu.get_barrier_semaphore()
    for peer in peers:
        pl.semaphore_signal(barrier, inc=1, device_id=peer, device_id_type=pl.DeviceIdType.MESH)
    copies = [
        pltpu.make_async_copy(src, dst, small_sem.at[i])
        for i, (src, dst) in enumerate(zip(smalls_hbm, smalls))
    ]
    for copy in copies:
        copy.start()

    def small_copies():
        for copy in copies:
            copy.wait()

    def enter():
        pl.semaphore_wait(barrier, len(peers))

    early, late = (
        Flow(i, {"z": length_z, "y": length_y}, (a_ref, b_ref), flow_sems[i]) for i in range(2)
    )
    gather(
        early, late, small_copies, enter, tok_ref, gain_ref, step_ref, *shards,
        normed, *gather_refs,
    )
    flat_a = a_ref.reshape(length_z * length_y * 64, EARLY)
    flat_b = b_ref.reshape(length_z * length_y * 64, LATE)
    middle(
        late, normed, flat_a, flat_b, taps_x, taps_b, taps_c, rate_ref, freq_ref, sink_ref,
        incoming, window_ref, log_ref, gate_ref, *conv_refs, *middle_refs,
    )
    finish(
        window_ref, flat_b, *conv_refs, incoming, gate_ref, group_gain_ref, mixed_ref, *finish_refs
    )
    early.finish()
    late.finish()


def layer(length_z, length_y, n, tokens, smalls, shards, sinks):
    rows, model = tokens.shape
    channels = HEADS * HEAD_DIM
    width = channels + 2 * STATE
    blocks = rows // BLOCK
    pairs = channels // 128
    tile = (STATE, 128)
    full = (MSG, 128)
    lead = (length_z, length_y, 2, 32)
    flows = [transfers(routes, {"z": length_z, "y": length_y}) for routes in ROUTES]
    part = model // n
    dma = pltpu.SemaphoreType.DMA
    vmem = pltpu.VMEM
    hbm = pl.BlockSpec(memory_space=pl.ANY)
    scratch = [
        *(vmem(s.shape, s.dtype) for s in smalls),
        dma((len(smalls),)),
        vmem((*lead, EARLY), BF16),
        vmem((*lead, LATE), BF16),
        vmem((rows + 2 * HALO, model), BF16),
        vmem((HALO, model), BF16), vmem((HALO, model), BF16), vmem((rows, model), BF16),
        dma((2, 2)), dma((len(shards) + 1,)),
        *(dma((len(part),)) for sends, groups in flows for part in (sends, sends, groups, groups)),
        vmem((2, pairs, *tile), BF16),
        vmem((rows, channels), BF16),
        vmem((rows, channels), BF16),
        vmem((rows, width), BF16),
        vmem((rows, 4 * HEADS), F32),
        vmem((blocks, 4 * HEADS, BLOCK), F32),
        vmem((blocks, STATE, 2 * channels), F32),
        vmem((blocks, 8, 2 * channels), F32),
        vmem((rows + 2 * HALO, width), BF16),
        vmem((rows, 256), BF16),
        vmem((rows, channels), BF16),
        vmem((rows, 128), F32),
        vmem((rows + 2 * HALO, width), F32),
        vmem((BLOCK + 2 * HALO, width), F32),
        vmem((2, pairs, *full), BF16),
        vmem((WINDOW, 256), BF16),
        vmem((WINDOW, 256), BF16),
        vmem((2, rows + 2 * BLOCK, 128), BF16),
        vmem((128, rows + 2 * BLOCK), BF16),
        vmem((2, (rows + 2 * WINDOW) // GRID_W, 128), F32),
        vmem((2, GRID_W, 128), F32),
        vmem((pairs, *full), BF16),
        vmem((pairs, *full), BF16),
        vmem((length_y, *full), BF16),
        vmem(full, BF16),
        vmem((length_z, *full), BF16),
        vmem((length_y, *tile), BF16),
        vmem((length_y, *tile), BF16),
        vmem((pairs, *tile), BF16),
        vmem((pairs, *tile), BF16),
        vmem(tile, F32),
        dma((2,)), dma((length_y, 2)), dma((length_z, 2)), dma((length_y, 2)), dma((2,)),
        dma((2, 2)),
        vmem((rows, channels), BF16),
        vmem((blocks, STATE, 2 * channels), BF16),
        vmem((2, blocks, BLOCK, part // 2), BF16),
        vmem((2, blocks, BLOCK, part // 2), BF16),
        vmem((2, blocks, BLOCK, part), BF16),
        vmem((2, blocks, BLOCK, part), BF16),
        dma((2, blocks, 2)), dma((2, blocks, 2)),
    ]
    return pl.pallas_call(
        functools.partial(layer_kernel, (length_z, length_y)),
        in_specs=[hbm] * (1 + len(smalls) + len(shards)) + [pl.BlockSpec(memory_space=pltpu.SMEM)],
        out_specs=[pl.BlockSpec(memory_space=pltpu.VMEM)] * 2,
        out_shape=[
            jax.ShapeDtypeStruct((rows, part), BF16),
            jax.ShapeDtypeStruct((HEADS, rows), F32),
        ],
        scratch_shapes=scratch,
        compiler_params=pltpu.CompilerParams(
            collective_id=1, has_side_effects=True, vmem_limit_bytes=65_800_000
        ),
        cost_estimate=pl.CostEstimate(flops=1 << 33, bytes_accessed=24 << 20, transcendentals=0),
        name="layer",
    )(tokens, *smalls, *shards, sinks)


def flatten_rows(weight):
    return weight.reshape(weight.shape[0], -1)


def shards(
    tokens, input_gain, gate_weight, value_weight, inflow_weight, readout_weight, step_weight,
    conv_values, conv_inflow, conv_readout, log_rate, group_gain, query_weight, key_weight,
    vector_weight, sink_logit, state_out, window_out,
):
    count = tokens.shape[0]
    length_z, length_y = lax.axis_size(SP[0]), lax.axis_size(SP[1])
    quarter = HEAD_DIM // 4
    powers = (np.arange(128) % quarter).astype(np.float32) / np.float32(quarter)
    freqs = np.broadcast_to(np.float32(ROPE_BASE) ** -powers, (8, 128)).astype(np.float32)
    freqs = jnp.asarray(freqs)
    smalls = (
        input_gain.reshape(-1, 128),
        step_weight.transpose(1, 2, 0).reshape(2 * HEADS, -1),
        conv_values, flatten_rows(conv_inflow), flatten_rows(conv_readout),
        log_rate.transpose(0, 2, 1).reshape(2 * HEADS, count),
        freqs,
        group_gain.reshape(-1, 128),
    )
    shards_here = (
        value_weight, flatten_rows(inflow_weight), flatten_rows(readout_weight), key_weight,
        vector_weight, gate_weight, query_weight, state_out.T, window_out.T,
    )
    mixed, logs = layer(
        length_z, length_y, lax.axis_size("tp"), tokens, smalls, shards_here, sink_logit
    )
    return mixed, logs.T


def solution(mesh):
    torus = Mesh(mesh.devices.reshape(8, 4, 2, mesh.shape["tp"]), (*SP, "tp"))
    return jax.shard_map(
        shards,
        mesh=torus,
        in_specs=(
            P(SP, None), P(), P(SP, "tp"), P(SP, "tp"), P(SP, "tp", None), P(SP, "tp", None),
            P(SP, None, "tp"), P(None, "tp"), P(None, "tp", None), P(None, "tp", None),
            P(None, SP, "tp"), P("tp"), P(SP, "tp"), P(SP, "tp"), P(SP, "tp"), P("tp"),
            P("tp", SP), P("tp", SP),
        ),
        out_specs=(P(SP, "tp"), P(SP, "tp")),
        check_vma=False,
    )
```

```python
import functools
import heapq

import jax
import jax.numpy as jnp
import numpy as np
from jax import lax
from jax.experimental import pallas as pl
from jax.experimental.pallas import tpu as pltpu
from jax.sharding import Mesh
from jax.sharding import PartitionSpec as P

HEAD_DIM = 64
STATE = 128
HEADS = 8
BLOCK = 128
WINDOW = 128
GRID_W = 64
HALO = 16
SP = ("sp_0", "sp_1", "sp_2")
EPS = 1e-06
ROPE_BASE = 10000.0
F32 = jnp.float32
BF16 = jnp.bfloat16
MSG = STATE + 16
KV_AT = 768
Q_AT = 1024
OUT_AT = 512


def dot(a, b, dims=((1,), (0,)), precision=None):
    return lax.dot_general(
        a, b, (dims, ((), ())), preferred_element_type=F32, precision=precision
    )


def split_bf16(value, parts):
    pieces = []
    for _ in range(parts):
        piece = value.astype(BF16)
        pieces.append(piece)
        value = value - piece.astype(F32)
    return pieces


def spread(value, spread_matrix, parts):
    pieces = [p.astype(F32) for p in split_bf16(value, parts)]
    joined = jnp.concatenate(pieces, axis=1).astype(BF16)
    matrix = jnp.concatenate([spread_matrix] * parts, axis=0)
    return dot(joined, matrix)


def as_row(ref):
    wide = ref[...].astype(F32)
    return jnp.concatenate([wide[i : i + 1, :] for i in range(wide.shape[0])], axis=1)


def spread_matrix():
    shape = (2 * HEADS, 2 * HEADS * HEAD_DIM)
    rows = lax.broadcasted_iota(jnp.int32, shape, 0)
    first = lax.broadcasted_iota(jnp.int32, shape, 1) - rows * HEAD_DIM
    return jnp.where((first >= 0) & (first < HEAD_DIM), 1.0, 0.0).astype(BF16)


def conv_state(
    traffic_service, cin_ref, taps_x_ref, taps_b_ref, taps_c_ref, step_ref, rate_ref,
    conv_ref, col_ref, row_ref, piece_ref, etot_ref, msg_ref, win,
):
    count = cin_ref.shape[0] - 2 * HALO
    blocks = count // BLOCK
    channels = HEADS * HEAD_DIM
    spread_m = spread_matrix()
    taps = jnp.concatenate([t[...].astype(F32) for t in (taps_x_ref, taps_b_ref, taps_c_ref)], axis=1)
    lane16 = lax.broadcasted_iota(jnp.int32, (BLOCK, 2 * HEADS), 1)
    forward16 = lane16 < HEADS
    tri = (
        lax.broadcasted_iota(jnp.int32, (BLOCK, BLOCK), 0)
        >= lax.broadcasted_iota(jnp.int32, (BLOCK, BLOCK), 1)
    ).astype(F32)
    win[pl.ds(0, HALO), :] = cin_ref[pl.ds(count, HALO), :].astype(F32)
    win[pl.ds(HALO + count, HALO), :] = cin_ref[pl.ds(count + HALO, HALO), :].astype(F32)

    def fill(i, carry):
        start = pl.multiple_of(i * BLOCK, BLOCK)
        win[pl.ds(HALO + start, BLOCK), :] = cin_ref[pl.ds(start, BLOCK), :].astype(F32)
        return carry

    lax.fori_loop(0, blocks, fill, 0)
    traffic_service(0.5)

    def some(which):
        spans = [slice(i * BLOCK, (i + 1) * BLOCK) for i in which]
        steps, decays, convs = [], [], []
        for rows in spans:
            raw = step_ref[rows, 0 : 2 * HEADS]
            steps.append(jnp.maximum(raw, 0.0) + jnp.log1p(jnp.exp(-jnp.abs(raw))))
            rate = jnp.concatenate(
                [rate_ref[:, rows], jnp.zeros((BLOCK - 2 * HEADS, BLOCK), F32)], axis=0
            )
            decays.append(-jnp.exp(rate.T[:, 0 : 2 * HEADS]) * steps[-1])
        cums = [dot(tri, decay, precision=lax.Precision.HIGHEST) for decay in decays]
        tots = [cum[BLOCK - 1 : BLOCK, :] for cum in cums]
        cols = [jnp.where(forward16, cum, cum - decay) for cum, decay in zip(cums, decays)]
        weights = [
            jnp.exp(jnp.where(forward16, tot - col, col)) * step
            for tot, col, step in zip(tots, cols, steps)
        ]
        wides = [spread(weight, spread_m, 2) for weight in weights]
        etots = [spread(jnp.exp(jnp.broadcast_to(tot, (8, 2 * HEADS))), spread_m, 3) for tot in tots]
        rests = jnp.zeros((BLOCK, 128 - 4 * HEADS), F32)
        turned = [jnp.concatenate([col, step, rests], axis=1).T for col, step in zip(cols, steps)]
        for rows in spans:
            acc = 0.0
            for tap in range(5):
                first = rows.start + HALO - 2 + tap
                acc = acc + win[first : first + BLOCK, :] * taps[tap : tap + 1, :]
            convs.append((acc * jax.nn.sigmoid(acc)).astype(BF16))
        pieces = []
        for conv, wide in zip(convs, wides):
            xs = conv[:, 0:channels].astype(F32)
            scaled = (jnp.concatenate([xs, xs], axis=1) * wide).astype(BF16)
            pieces.append(dot(conv[:, channels : channels + STATE], scaled, ((0,), (0,))))
        for n, (i, rows) in enumerate(zip(which, spans)):
            conv_ref[rows, :] = convs[n]
            col_ref[rows, 0 : 2 * HEADS] = cols[n]
            col_ref[rows, 2 * HEADS : 4 * HEADS] = jnp.broadcast_to(tots[n], (BLOCK, 2 * HEADS))
            row_ref[i] = turned[n][0 : 4 * HEADS, :]
            piece_ref[i] = pieces[n]
            etot_ref[i] = etots[n]
        return sum(tots)

    total = jnp.zeros((1, 2 * HEADS), F32)
    for i in range(0, blocks, 2):
        total = total + some((i, i + 1))
        traffic_service(1.6)
    forward = piece_ref[0, :, 0:channels]
    backward = piece_ref[blocks - 1, :, channels : 2 * channels]
    for i in range(1, blocks):
        forward = etot_ref[i, 0:1, 0:channels] * forward + piece_ref[i, :, 0:channels]
        k = blocks - 1 - i
        backward = (
            etot_ref[k, 0:1, channels : 2 * channels] * backward
            + piece_ref[k, :, channels : 2 * channels]
        )
    spread_total = spread(jnp.broadcast_to(total, (16, 2 * HEADS)), spread_m, 3)
    hi, mid, lo = split_bf16(spread_total, 3)
    which = lax.broadcasted_iota(jnp.int32, (16, 2 * channels), 0)
    tail = jnp.where(
        which == 0, hi.astype(F32), jnp.where(which == 1, mid.astype(F32), lo.astype(F32))
    ).astype(BF16)
    for e, state in enumerate((forward, backward)):
        for pair in range(channels // 128):
            lanes = slice(pair * 128, pair * 128 + 128)
            msg_ref[e, pair, 0:STATE, :] = state[:, lanes].astype(BF16)
            msg_ref[e, pair, STATE:MSG, :] = tail[:, e * channels + pair * 128 : e * channels + pair * 128 + 128]


def mixer(conv_ref, col_ref, row_ref, piece_ref, etot_ref, in_ref, gate_ref, gain_ref, out_ref, held):
    count = conv_ref.shape[0]
    blocks = count // BLOCK
    channels = HEADS * HEAD_DIM
    spread_m = spread_matrix()
    gain = as_row(gain_ref)
    for e in range(2):
        state = jnp.concatenate(
            [in_ref[e, p].astype(F32) for p in range(channels // 128)], axis=1
        )
        lanes = slice(e * channels, (e + 1) * channels)
        for i in range(blocks) if e == 0 else reversed(range(blocks)):
            held[i, :, lanes] = state.astype(BF16)
            state = etot_ref[i, 0:1, lanes] * state + piece_ref[i, :, lanes]
    row_at = lax.broadcasted_iota(jnp.int32, (BLOCK, BLOCK), 0)
    col_at = lax.broadcasted_iota(jnp.int32, (BLOCK, BLOCK), 1)
    lower = row_at >= col_at
    diagonal = row_at == col_at
    first_half = col_at < HEAD_DIM
    forward16 = lax.broadcasted_iota(jnp.int32, (BLOCK, 2 * HEADS), 1) < HEADS

    def one(i):
        rows = pl.ds(pl.multiple_of(i * BLOCK, BLOCK), BLOCK)
        inflow = conv_ref[rows, channels : channels + STATE]
        readout = conv_ref[rows, channels + STATE : channels + 2 * STATE]
        inner = dot(readout, inflow, ((1,), (1,)))
        col = col_ref[rows, 0 : 2 * HEADS]
        tot = col_ref[rows, 2 * HEADS : 4 * HEADS]
        reach = spread(jnp.exp(jnp.where(forward16, col, tot - col)), spread_m, 2)
        far = dot(readout, held[i]) * reach
        parts = []
        for pair in range(HEADS // 2):
            weights = []
            for h in (2 * pair, 2 * pair + 1):
                b = HEADS + h
                arg = jnp.where(
                    lower,
                    col[:, h : h + 1] - row_ref[i, h : h + 1, :],
                    row_ref[i, b : b + 1, :] - col[:, b : b + 1],
                )
                step_f = row_ref[i, 2 * HEADS + h : 2 * HEADS + h + 1, :]
                step_b = row_ref[i, 2 * HEADS + b : 2 * HEADS + b + 1, :]
                step = jnp.where(lower, step_f, step_b) + jnp.where(diagonal, step_b, 0.0)
                weights.append((inner * jnp.exp(arg) * step).astype(BF16))
            xs = conv_ref[rows, pair * 128 : pair * 128 + 128]
            zero = jnp.zeros_like(xs)
            stacked = jnp.concatenate(
                [jnp.where(first_half, xs, zero), jnp.where(first_half, zero, xs)], axis=0
            )
            parts.append(dot(jnp.concatenate(weights, axis=1), stacked))
        y = jnp.concatenate(parts, axis=1) + far[:, 0:channels] + far[:, channels:]
        gate = gate_ref[rows, :].astype(F32)
        y = y * (gate * jax.nn.sigmoid(gate))
        y = y * lax.rsqrt(jnp.mean(y * y, axis=1, keepdims=True) + EPS)
        out_ref[rows, :] = (y * gain).astype(BF16)

    return one


def attention(
    count, q_ref, kv_ref, before_ref, after_ref, freq_ref, sink_ref,
    out_ref, log_ref, keys, values, by_row, by_col,
):
    blocks = count // BLOCK
    place = lax.axis_index(SP)
    lane = lax.broadcasted_iota(jnp.int32, (BLOCK, 128), 1)
    low_quarter = lane % 32 < 16
    first_half = lane < HEAD_DIM
    row_lane = (lane % HEAD_DIM < 32)[0:GRID_W]

    grid_rows = by_row.shape[1]
    first_row = place * (count // GRID_W) - WINDOW // GRID_W
    sign = jnp.where(low_quarter, -1.0, 1.0)
    for ref, first, length in ((by_row, first_row, grid_rows), (by_col, 0, GRID_W)):
        at = lax.broadcasted_iota(jnp.int32, (length, 128), 0) + first
        angle = at.astype(F32) * freq_ref[0:1, :]
        ref[0] = jnp.cos(angle)
        ref[1] = jnp.sin(angle) * sign[0:length]

    def tables(slot):
        out = []
        for kind in range(2):
            parts = []
            for r in range(BLOCK // GRID_W):
                row = by_row[kind, pl.ds(slot * (BLOCK // GRID_W) + r, 1), :]
                parts.append(jnp.where(row_lane, row, by_col[kind]))
            out.append(jnp.concatenate(parts, axis=0))
        return out

    def turn(value, table):
        wide = value.astype(F32)
        other = jnp.where(low_quarter, pltpu.roll(wide, 112, 1), pltpu.roll(wide, 16, 1))
        return (wide * table[0] + other * table[1]).astype(BF16)

    def store(raw, slot):
        rows = pl.ds(pl.multiple_of(slot * BLOCK, BLOCK), BLOCK)
        key = turn(raw[:, 0:128], tables(slot)).astype(F32)
        swapped = pltpu.roll(key, 64, 1)
        keys[0, rows, :] = jnp.where(first_half, key, swapped).astype(BF16)
        keys[1, rows, :] = jnp.where(first_half, swapped, key).astype(BF16)
        values[:, rows] = raw[:, 128:256].astype(F32).T.astype(BF16)

    def own_keys():
        def fill(i, carry):
            rows = pl.ds(pl.multiple_of(i * BLOCK, BLOCK), BLOCK)
            store(kv_ref[rows, :], i + 1)
            return carry

        lax.fori_loop(0, blocks, fill, 0)

    def edge_keys():
        store(before_ref[...], 0)
        store(after_ref[...], blocks + 1)

    key_at = lax.broadcasted_iota(jnp.int32, (3 * BLOCK, 2 * BLOCK), 0)
    query_at = lax.broadcasted_iota(jnp.int32, (3 * BLOCK, 2 * BLOCK), 1) % BLOCK
    in_band = (key_at >= query_at) & (key_at <= query_at + 2 * WINDOW)
    first_row_half = lax.broadcasted_iota(jnp.int32, (1, 2 * BLOCK), 1) < BLOCK
    start_at = -place * count
    end_at = start_at + count * lax.axis_size(SP)

    def one(i):
        start = pl.multiple_of(i * BLOCK, BLOCK)
        rows = pl.ds(start, BLOCK)
        here = key_at + (start - WINDOW)
        valid = in_band & (here >= start_at) & (here < end_at)
        table = tables(i + 1)
        band = pl.ds(start, 3 * BLOCK)
        qs = []
        for pair in range(HEADS // 2):
            lanes = slice(pair * 128, pair * 128 + 128)
            q = (turn(q_ref[rows, lanes], table).astype(F32) * HEAD_DIM ** (-0.5)).astype(BF16)
            zero = jnp.zeros_like(q)
            qs.append(jnp.concatenate(
                [jnp.where(first_half, q, zero), jnp.where(first_half, zero, q)], axis=0
            ))
        scores = [dot(keys[pair // 2, band, :], q, ((1,), (1,))) for pair, q in enumerate(qs)]
        outs = []
        for pair in range(HEADS // 2):
            group = pair // 2
            mine = jnp.where(valid, scores[pair], -1e30)
            sink = jnp.where(first_row_half, sink_ref[2 * pair], sink_ref[2 * pair + 1])
            top = jnp.maximum(jnp.max(mine, axis=0, keepdims=True), sink)
            expo = jnp.exp(mine - top)
            total = jnp.sum(expo, axis=0, keepdims=True) + jnp.exp(sink - top)
            value = values[group * HEAD_DIM : (group + 1) * HEAD_DIM, band]
            outs.append(dot(value, expo.astype(BF16)) / total)
            log = top + jnp.log(total)
            log_ref[2 * pair : 2 * pair + 1, rows] = log[:, 0:BLOCK]
            log_ref[2 * pair + 1 : 2 * pair + 2, rows] = log[:, BLOCK:]
        for pair, o in enumerate(outs):
            turned = jnp.concatenate([o[:, 0:BLOCK], o[:, BLOCK:]], axis=0).T
            out_ref[rows, pair * 128 : pair * 128 + 128] = turned.astype(BF16)

    return own_keys, edge_keys, one


LINKS = ("z+", "z-", "y+", "y-")
WIDTHS = (1152, 512, 1536)
ROUTES = (
    (("A", 0, 0, 640, 384, "z"), ("B", 0, 640, 512, 256, "y")),
    (("C", 1, 0, 256, 128, "z"), ("D", 1, 256, 256, 128, "y")),
    (("E", 2, 0, 896, 512, "z"), ("F", 2, 896, 640, 384, "y")),
)
BEGIN_AFTER = (50, 60)
RATE = 46.6e3
HOP = 1.9


def ring(route, axis, other, length):
    name, array, column, total, cut, _ = route
    out = []
    for sign in (1, -1):
        previous = None
        for step in range(length // 2):
            cols = (column, total)
            if step == length // 2 - 1:
                cols = (column, cut) if sign == 1 else (column + cut, total - cut)
            key = (name, axis, other, sign, step)
            out.append(dict(
                key=key, route=name, array=array, axis=axis, sign=sign, along=-sign * step,
                other=other, cols=cols, needs=[previous] if previous else [],
            ))
            previous = key
    return out


def transfers(routes, lengths):
    sends, groups = [], {}
    for route in routes:
        name, _, _, _, _, first = route
        second = "y" if first == "z" else "z"
        length = lengths[first]
        sends += ring(route, first, 0, length)
        for offset in range(-(length // 2) + 1, length // 2 + 1):
            one = ring(route, second, offset, lengths[second])
            needs = []
            if offset == length // 2:
                needs = [(name, first, 0, sign, length // 2 - 1) for sign in (1, -1)]
            elif offset:
                needs = [(name, first, 0, -1 if offset > 0 else 1, abs(offset) - 1)]
            for s in one:
                s["needs"] = s["needs"] or needs
            sends += one
            groups[(name, offset)] = {s["key"] for s in one}
    return sends, groups


class Flow:
    def __init__(self, number, lengths, arrays, sems, free):
        self.routes = ROUTES[number]
        self.lengths = lengths
        self.arrays = arrays
        self.send_sem, self.recv_sem, self.core_send, self.core_recv = sems
        self.free = free
        self.at = dict(zip("zy", (lax.axis_index(SP[0]), lax.axis_index(SP[1]))))
        self.c = lax.axis_index(SP[2])
        self.sends, self.groups = transfers(self.routes, lengths)
        self.number = {s["key"]: i for i, s in enumerate(self.sends)}
        self.by_key = {s["key"]: s for s in self.sends}
        self.group_keys = list(self.groups)
        self.left = {s["key"]: len(s["needs"]) for s in self.sends}
        self.followers = {}
        for s in self.sends:
            for need in s["needs"]:
                self.followers.setdefault(need, []).append(s)
        self.first_axis = {route[0]: route[5] for route in self.routes}
        self.heap = []
        self.clock = 0.0
        self.started = []
        self.launched = 0

    def wrap(self, axis, shift):
        length = self.lengths[axis]
        return lax.rem(self.at[axis] + shift + length, length)

    def rank(self, s):
        return (s["axis"] != self.first_axis[s["route"]], s["route"])

    def copy_of(self, s, shift):
        along = s["along"] - shift * s["sign"]
        place = {s["axis"]: along, "y" if s["axis"] == "z" else "z": s["other"]}
        ref = self.arrays[s["array"]].at[
            self.wrap("z", place["z"]), self.wrap("y", place["y"]), self.c, :, pl.ds(*s["cols"])
        ]
        i = self.number[s["key"]]
        to = {SP["zy".index(s["axis"])]: self.wrap(s["axis"], s["sign"])}
        return pltpu.make_async_remote_copy(
            src_ref=ref, dst_ref=ref, send_sem=self.send_sem.at[i], recv_sem=self.recv_sem.at[i],
            device_id=to, device_id_type=pl.DeviceIdType.MESH,
        )

    def core_copy(self, key, c):
        name, offset = key
        i = self.group_keys.index(key)
        route = [r for r in self.routes if r[0] == name][0]
        ref = self.arrays[route[1]]
        cols = pl.ds(route[2], route[3])
        if route[5] == "z":
            ref = ref.at[self.wrap("z", offset), :, c, :, cols]
        else:
            ref = ref.at[:, self.wrap("y", offset), c, :, cols]
        return pltpu.make_async_remote_copy(
            src_ref=ref, dst_ref=ref, send_sem=self.core_send.at[i],
            recv_sem=self.core_recv.at[i], device_id={SP[2]: 1 - self.c},
            device_id_type=pl.DeviceIdType.MESH,
        )

    def launch(self, s):
        copy = self.copy_of(s, 0)
        copy.start()
        self.started.append(copy)
        self.launched += 1
        link = s["axis"] + ("+" if s["sign"] == 1 else "-")
        self.free[link] = max(self.free[link], self.clock) + 64 * s["cols"][1] / RATE
        heapq.heappush(self.heap, (self.free[link] + HOP, len(self.started), s["key"]))

    def begin(self):
        for s in sorted((s for s in self.sends if not s["needs"]), key=self.rank):
            self.launch(s)

    def handle(self):
        _, _, key = heapq.heappop(self.heap)
        self.copy_of(self.by_key[key], 1).wait_recv()
        for s in sorted(self.followers.get(key, []), key=self.rank):
            self.left[s["key"]] -= 1
            if self.left[s["key"]] == 0:
                self.launch(s)
        for group, keys in self.groups.items():
            if key in keys:
                keys.remove(key)
                if not keys:
                    copy = self.core_copy(group, self.c)
                    copy.start()
                    self.started.append(copy)

    def wait_core(self):
        for group in self.group_keys:
            self.core_copy(group, 1 - self.c).wait_recv()


class Traffic:
    def __init__(self, lengths, arrays, sems):
        free = dict.fromkeys(LINKS, 0.0)
        self.flows = [Flow(i, lengths, arrays, s, free) for i, s in enumerate(sems)]
        self.lengths = lengths
        self.arrays = arrays
        self.clock = 0.0
        self.newest = 0

    def begin(self):
        self.flows[0].begin()

    def next_arrival(self):
        return min(((f.heap[0][0], i) for i, f in enumerate(self.flows) if f.heap), default=None)

    def handle(self, index, now):
        flow = self.flows[index]
        flow.clock = max(flow.clock, now)
        flow.handle()
        if index == self.newest and index + 1 < len(self.flows):
            if flow.launched >= BEGIN_AFTER[index]:
                self.newest += 1
                self.flows[self.newest].clock = flow.clock
                self.flows[self.newest].begin()

    def service(self, passed):
        self.clock += passed
        while (head := self.next_arrival()) and head[0] <= self.clock:
            self.handle(head[1], self.clock)

    def until(self, index):
        while self.newest < index or self.flows[index].heap:
            head = self.next_arrival()
            self.clock = max(self.clock, head[0])
            self.handle(head[1], self.clock)
        self.flows[index].wait_core()

    def finish(self):
        for flow in self.flows:
            for copy in flow.started:
                copy.wait_send()


def gather(
    traffic, small_copies, enter, tok_ref, gain_ref, step_ref, value_ref, inflow_ref,
    readout_ref, key_ref, vector_ref, gate_ref, query_ref, state_ref, window_ref,
    normed, before, after, held, edge_sem, own_sem,
):
    z, y, c = (lax.axis_index(a) for a in SP)
    length_z, length_y = traffic.lengths["z"], traffic.lengths["y"]
    flat = (z * length_y + y) * 2 + c
    count = length_z * length_y * 2
    count_rows = tok_ref.shape[0]
    a_ref, q_ref, b_ref = traffic.arrays

    def device_at(index):
        index = lax.rem(index + count, count)
        return {
            SP[0]: index // (2 * length_y),
            SP[1]: lax.rem(index // 2, length_y),
            SP[2]: lax.rem(index, 2),
        }

    moves = []
    for array, refs in (
        (a_ref, (value_ref, inflow_ref, readout_ref, key_ref, vector_ref)),
        (q_ref, (query_ref,)),
        (b_ref, (gate_ref, state_ref, window_ref)),
    ):
        column = 0
        for ref in refs:
            width = ref.shape[1]
            moves.append((ref, array.at[z, y, c, :, pl.ds(column, width)]))
            column += width
    moves.append((tok_ref, held))
    moves = [pltpu.make_async_copy(*move, own_sem.at[i]) for i, move in enumerate(moves)]
    for move in moves:
        move.start()
    small_copies()
    step = step_ref[...].astype(F32)
    rows, cols = step.shape
    step = jnp.concatenate([step, jnp.zeros((rows, 128 - cols), F32)], axis=1)
    step = jnp.concatenate([step, jnp.zeros((128 - rows, 128), F32)], axis=0)
    a_ref[z, y, c, :, WIDTHS[0] - 128 : WIDTHS[0]] = step.T[0:cols, :].astype(BF16)
    for move in moves[:5]:
        move.wait()
    enter()
    edge_copies = []
    for k, (index, dst) in enumerate(((flat - 1, after), (flat + 1, before))):
        edge_copies.append(pltpu.make_async_remote_copy(
            src_ref=tok_ref.at[pl.ds(k * (count_rows - HALO), HALO)], dst_ref=dst,
            send_sem=edge_sem.at[k, 0], recv_sem=edge_sem.at[k, 1],
            device_id=device_at(index), device_id_type=pl.DeviceIdType.MESH,
        ))
    gain = as_row(gain_ref)

    def norm(value):
        wide = value.astype(F32)
        scale = lax.rsqrt(jnp.mean(wide * wide, axis=1, keepdims=True) + EPS)
        return wide * scale * gain

    def norm_blocks(first, last):
        def norm_block(i, carry):
            rows = pl.ds(pl.multiple_of(i * BLOCK, BLOCK), BLOCK)
            normed[rows, :] = norm(held[rows, :]).astype(BF16)
            return carry

        lax.fori_loop(first, last, norm_block, 0)

    traffic.begin()
    for copy in edge_copies:
        copy.start()
    for move in moves[5:]:
        move.wait()
    blocks = count_rows // BLOCK
    traffic.service(1.0)
    for i in range(blocks):
        norm_blocks(i, i + 1)
        traffic.service(0.6)
    for copy in edge_copies:
        copy.wait()
    normed[count_rows : count_rows + HALO, :] = jnp.where(flat > 0, norm(before[...]), 0.0).astype(BF16)
    normed[count_rows + HALO : count_rows + 2 * HALO, :] = jnp.where(
        flat < count - 1, norm(after[...]), 0.0
    ).astype(BF16)
    traffic.service(0.3)
    traffic.until(0)
    traffic.service(1.5)


def middle(
    traffic, normed, a_ref, query_ref, b_ref, taps_x_ref, taps_b_ref, taps_c_ref, rate_ref, freq_ref, sink_ref,
    out_ref, window_ref, log_ref, gate_ref, conv_ref, col_ref, row_ref, piece_ref, etot_ref,
    cin_ref, kv_ref, q_ref, step_ref, win, near, msg_ref,
    kv_before_ref, kv_after_ref, keys, values, by_row, by_col, part, turned, by_y, summed, by_z,
    back, arrived, nxt, final, carry,
    part_sem, y_sem, z_sem, back_sem, final_sem, kv_sem,
):
    rows = kv_ref.shape[0]
    z, y, c = (lax.axis_index(a) for a in SP)
    length_z, length_y = lax.axis_size(SP[0]), lax.axis_size(SP[1])
    forward = c == 0
    other = 1 - c
    order_z = jnp.where(forward, z, length_z - 1 - z)
    mesh_id = pl.DeviceIdType.MESH
    flat = (z * length_y + y) * 2 + c
    count = length_z * length_y * 2

    def device_at(index):
        index = lax.rem(index + count, count)
        return {
            SP[0]: index // (2 * length_y),
            SP[1]: lax.rem(index // 2, length_y),
            SP[2]: lax.rem(index, 2),
        }

    def project(dst, count, tiles, source, first):
        tile = 256
        for j in range(tiles):
            cols = slice(first + j * tile, first + (j + 1) * tile)
            dst[:, j * tile : (j + 1) * tile] = dot(normed[0:count, :], source[:, cols]).astype(BF16)
            traffic.service(1.05)

    project(kv_ref, rows, 1, a_ref, KV_AT)

    def send(src, dst, sems, peer):
        copy = pltpu.make_async_remote_copy(
            src_ref=src, dst_ref=dst, send_sem=sems.at[0], recv_sem=sems.at[1],
            device_id=peer, device_id_type=mesh_id,
        )
        copy.start()
        return copy

    def state_of(ref, *at):
        return ref[(*at, slice(0, STATE), slice(None))].astype(F32)

    def decay_of(ref, *at):
        tail = ref[(*at, slice(STATE, MSG), slice(None))].astype(F32)
        return tail[0:1] + tail[1:2] + tail[2:3]

    def put(ref, state, decay, *at):
        ref[(*at, slice(0, STATE), slice(None))] = state.astype(BF16)
        hi, mid, lo = (p.astype(F32) for p in split_bf16(decay, 3))
        which = lax.broadcasted_iota(jnp.int32, (MSG - STATE, 128), 0)
        tail = jnp.where(which == 0, hi, jnp.where(which == 1, mid, lo))
        ref[(*at, slice(STATE, MSG), slice(None))] = tail.astype(BF16)

    pairs = msg_ref.shape[1]
    kv_copies = [
        send(
            kv_ref.at[pl.ds(rows - WINDOW, WINDOW)], kv_before_ref, kv_sem.at[0],
            device_at(flat + 1),
        ),
        send(kv_ref.at[pl.ds(0, WINDOW)], kv_after_ref, kv_sem.at[1], device_at(flat - 1)),
    ]
    project(cin_ref, rows + 2 * HALO, 3, a_ref, 0)
    step_ref[...] = dot(normed[0:rows, :], a_ref[:, WIDTHS[0] - 128 : WIDTHS[0]])
    traffic.service(0.6)
    conv_state(
        traffic.service,
        cin_ref, taps_x_ref, taps_b_ref, taps_c_ref, step_ref, rate_ref,
        conv_ref, col_ref, row_ref, piece_ref, etot_ref, msg_ref, win,
    )
    copy = send(msg_ref.at[other], part, part_sem, {SP[2]: other})
    own_keys, edge_keys, attend = attention(
        rows, q_ref, kv_ref, kv_before_ref, kv_after_ref, freq_ref, sink_ref,
        window_ref, log_ref, keys, values, by_row, by_col,
    )

    blocks = rows // BLOCK
    own_keys()
    traffic.service(1.2)
    copy.wait()
    for j in range(pairs):
        decay = decay_of(part, j)
        put(
            turned,
            jnp.exp(decay) * state_of(msg_ref, c, j) + state_of(part, j),
            decay + decay_of(msg_ref, c, j),
            j,
        )
    copies = []
    for k in range(1, length_y):
        to = lax.rem(y + k, length_y)
        copies.append(send(turned.at[to], by_y.at[k], y_sem.at[k], {SP[1]: to}))
    by_y[0] = turned[y]
    traffic.until(1)
    project(q_ref, rows, 2, query_ref, 0)
    attend(1)
    traffic.service(1.1)
    for copy in copies:
        copy.wait()
    before = []
    state = jnp.zeros((STATE, 128), F32)
    decay = jnp.zeros((1, 128), F32)
    for q in range(length_y):
        before.append((state, decay))
        slot = jnp.where(forward, lax.rem(y - q + length_y, length_y), lax.rem(y + 1 + q, length_y))
        step = decay_of(by_y, slot)
        state = jnp.exp(step) * state + state_of(by_y, slot)
        decay = decay + step
    put(summed, state, decay)
    for k in range(1, length_z):
        to = lax.rem(z + k, length_z)

        @pl.when((z + k >= length_z) == (c == 1))
        def _():
            send(summed, by_z.at[k], z_sem.at[k], {SP[0]: to})

    carry[...] = jnp.zeros_like(carry)
    for i in range(2, blocks - 1):
        attend(i)
        traffic.service(1.1)
    for distance in reversed(range(1, length_z)):
        slot = jnp.where(forward, distance, length_z - distance)

        @pl.when(order_z >= distance)
        def _():
            pltpu.make_async_remote_copy(
                src_ref=summed, dst_ref=by_z.at[slot], send_sem=z_sem.at[slot, 0],
                recv_sem=z_sem.at[slot, 1], device_id={SP[0]: z}, device_id_type=mesh_id,
            ).wait_recv()
            carry[...] = jnp.exp(decay_of(by_z, slot)) * carry[...] + state_of(by_z, slot)

    for k in range(1, length_z):
        to = lax.rem(z + k, length_z)

        @pl.when((z + k >= length_z) == (c == 1))
        def _():
            pltpu.make_async_remote_copy(
                src_ref=summed, dst_ref=by_z.at[k], send_sem=z_sem.at[k, 0],
                recv_sem=z_sem.at[k, 1], device_id={SP[0]: to}, device_id_type=mesh_id,
            ).wait_send()

    incoming = carry[...]
    for q in range(length_y):
        to = jnp.where(forward, q, length_y - 1 - q)
        state, decay = before[q]
        back[to] = (jnp.exp(decay) * incoming + state).astype(BF16)
    copies = []
    for k in range(1, length_y):
        to = lax.rem(y + k, length_y)
        copies.append(send(back.at[to], arrived.at[k], back_sem.at[k], {SP[1]: to}))
    arrived[0] = back[y]
    for copy in kv_copies:
        copy.wait()
    edge_keys()
    attend(0)
    traffic.service(1.3)
    for copy in copies:
        copy.wait()
    for j in range(pairs):
        state = arrived[lax.rem(y - j + length_y, length_y)]
        out_ref[c, j] = state
        nxt[j] = (
            jnp.exp(decay_of(msg_ref, c, j)) * state.astype(F32) + state_of(msg_ref, c, j)
        ).astype(BF16)
    copy = send(nxt, final, final_sem, {SP[2]: other})
    attend(blocks - 1)
    traffic.service(1.1)
    traffic.until(2)
    project(gate_ref, rows, 2, b_ref, 0)
    copy.wait()
    out_ref[other] = final[...]


def finish(
    window_ref, w_ref, conv_ref, col_ref, row_ref, piece_ref, etot_ref, in_ref, gate_ref, gain_ref,
    out_ref, *refs
):
    state_ref, held, far_out, far_in, near_out, near_in, far_sem, near_sem = refs
    n = lax.axis_size("tp")
    me = lax.axis_index("tp")
    mesh_id = pl.DeviceIdType.MESH
    sides = (1, -1)
    count, channels = state_ref.shape
    mix = mixer(
        conv_ref, col_ref, row_ref, piece_ref, etot_ref, in_ref, gate_ref, gain_ref, state_ref, held
    )
    width = w_ref.shape[0] // n
    half = width // 2
    chunk = far_out.shape[2]
    chunks = count // chunk

    def at(step):
        return lax.rem(me + step + n, n)

    def terms(rows, to):
        outs = pl.ds(pl.multiple_of(to * width, width), width)
        return dot(state_ref[rows, :], w_ref[outs, OUT_AT : OUT_AT + channels], ((1,), (1,))) + dot(
            window_ref[rows, :], w_ref[outs, OUT_AT + channels : OUT_AT + 2 * channels], ((1,), (1,))
        )

    def far_copy(i, k):
        return pltpu.make_async_remote_copy(
            src_ref=far_out.at[k, i], dst_ref=far_in.at[k, i], send_sem=far_sem.at[k, i, 0],
            recv_sem=far_sem.at[k, i, 1], device_id={"tp": at(sides[k])}, device_id_type=mesh_id,
        )

    def near_copy(i, k):
        return pltpu.make_async_remote_copy(
            src_ref=near_out.at[k, i], dst_ref=near_in.at[k, i], send_sem=near_sem.at[k, i, 0],
            recv_sem=near_sem.at[k, i, 1], device_id={"tp": at(sides[k])}, device_id_type=mesh_id,
        )

    def send_far(i, carry):
        rows = pl.ds(pl.multiple_of(i * chunk, chunk), chunk)
        value = terms(rows, at(2)).astype(BF16)
        for k in range(2):
            far_out[k, i] = value[:, k * half : (k + 1) * half]
            far_copy(i, k).start()

        @pl.when(i + 1 < chunks)
        def _():
            mix(i + 1)

        return carry

    mix(0)
    lax.fori_loop(0, chunks, send_far, 0)

    def send_near(i, carry):
        rows = pl.ds(pl.multiple_of(i * chunk, chunk), chunk)
        for k in range(2):
            value = terms(rows, at(sides[k])).astype(BF16).astype(F32)
            lanes = slice(k * half, (k + 1) * half)
            far_copy(i, k).wait_recv()
            near_out[k, i] = value.astype(BF16)
            near_out[k, i, :, lanes] = (value[:, lanes] + far_in[k, i].astype(F32)).astype(BF16)
            near_copy(i, k).start()
        return carry

    lax.fori_loop(0, chunks, send_near, 0)

    def collect(i, carry):
        rows = pl.ds(pl.multiple_of(i * chunk, chunk), chunk)
        value = terms(rows, me).astype(BF16).astype(F32)
        for k in range(2):
            near_copy(i, k).wait_recv()
            value = value + near_in[k, i].astype(F32)
        out_ref[rows, :] = value.astype(BF16)
        for k in range(2):
            far_copy(i, k).wait_send()
            near_copy(i, k).wait_send()
        return carry

    lax.fori_loop(0, chunks, collect, 0)


def layer_kernel(
    lengths, tok_ref, *refs
):
    length_z, length_y = lengths
    smalls_hbm, refs = refs[:8], refs[8:]
    shards, refs = refs[:9], refs[9:]
    sink_ref, mixed_ref, log_ref = refs[:3]
    smalls, refs = refs[3:11], refs[11:]
    small_sem, arrays, normed = refs[0], refs[1:4], refs[4]
    gather_refs, refs = refs[5:10], refs[10:]
    flow_sems, refs = (refs[0:4], refs[4:8], refs[8:12]), refs[12:]
    incoming, window_ref, gate_ref = refs[:3]
    conv_refs, refs = refs[3:8], refs[8:]
    middle_refs, finish_refs = refs[:29], refs[29:]
    gain_ref, step_ref, taps_x, taps_b, taps_c, rate_ref, freq_ref, group_gain_ref = smalls
    z, y, c = (lax.axis_index(a) for a in SP)
    t = lax.axis_index("tp")
    n = lax.axis_size("tp")
    flat = (z * length_y + y) * 2 + c
    count = length_z * length_y * 2
    peers = [{SP[2]: 1 - c}]
    peers += [{SP[1]: lax.rem(y + k, length_y)} for k in range(1, length_y)]
    peers += [{SP[0]: lax.rem(z + k, length_z)} for k in range(1, length_z)]
    peers += [{"tp": lax.rem(t + k, n)} for k in (1, n - 1)]
    for shift in (1, count - 1):
        index = lax.rem(flat + shift, count)
        peers.append({
            SP[0]: index // (2 * length_y),
            SP[1]: lax.rem(index // 2, length_y),
            SP[2]: lax.rem(index, 2),
        })
    barrier = pltpu.get_barrier_semaphore()
    for peer in peers:
        pl.semaphore_signal(barrier, inc=1, device_id=peer, device_id_type=pl.DeviceIdType.MESH)
    copies = [
        pltpu.make_async_copy(src, dst, small_sem.at[i])
        for i, (src, dst) in enumerate(zip(smalls_hbm, smalls))
    ]
    for copy in copies:
        copy.start()

    def small_copies():
        for copy in copies:
            copy.wait()

    def enter():
        pl.semaphore_wait(barrier, len(peers))

    traffic = Traffic({"z": length_z, "y": length_y}, arrays, flow_sems)
    gather(
        traffic, small_copies, enter, tok_ref, gain_ref, step_ref, *shards, normed, *gather_refs,
    )
    flat_refs = [
        ref.reshape(length_z * length_y * 64, width) for ref, width in zip(arrays, WIDTHS)
    ]
    middle(
        traffic, normed, *flat_refs, taps_x, taps_b, taps_c, rate_ref, freq_ref, sink_ref,
        incoming, window_ref, log_ref, gate_ref, *conv_refs, *middle_refs,
    )
    finish(
        window_ref, flat_refs[2], *conv_refs, incoming, gate_ref, group_gain_ref, mixed_ref, *finish_refs
    )
    traffic.finish()


def layer(length_z, length_y, n, tokens, smalls, shards, sinks):
    rows, model = tokens.shape
    channels = HEADS * HEAD_DIM
    width = channels + 2 * STATE
    blocks = rows // BLOCK
    pairs = channels // 128
    tile = (STATE, 128)
    full = (MSG, 128)
    lead = (length_z, length_y, 2, 32)
    flows = [transfers(routes, {"z": length_z, "y": length_y}) for routes in ROUTES]
    part = model // n
    dma = pltpu.SemaphoreType.DMA
    vmem = pltpu.VMEM
    hbm = pl.BlockSpec(memory_space=pl.ANY)
    scratch = [
        *(vmem(s.shape, s.dtype) for s in smalls),
        dma((len(smalls),)),
        *(vmem((*lead, w), BF16) for w in WIDTHS),
        vmem((rows + 2 * HALO, model), BF16),
        vmem((HALO, model), BF16), vmem((HALO, model), BF16), vmem((rows, model), BF16),
        dma((2, 2)), dma((len(shards) + 1,)),
        *(dma((len(part),)) for sends, groups in flows for part in (sends, sends, groups, groups)),
        vmem((2, pairs, *tile), BF16),
        vmem((rows, channels), BF16),
        vmem((rows, channels), BF16),
        vmem((rows, width), BF16),
        vmem((rows, 4 * HEADS), F32),
        vmem((blocks, 4 * HEADS, BLOCK), F32),
        vmem((blocks, STATE, 2 * channels), F32),
        vmem((blocks, 8, 2 * channels), F32),
        vmem((rows + 2 * HALO, width), BF16),
        vmem((rows, 256), BF16),
        vmem((rows, channels), BF16),
        vmem((rows, 128), F32),
        vmem((rows + 2 * HALO, width), F32),
        vmem((BLOCK + 2 * HALO, width), F32),
        vmem((2, pairs, *full), BF16),
        vmem((WINDOW, 256), BF16),
        vmem((WINDOW, 256), BF16),
        vmem((2, rows + 2 * BLOCK, 128), BF16),
        vmem((128, rows + 2 * BLOCK), BF16),
        vmem((2, (rows + 2 * WINDOW) // GRID_W, 128), F32),
        vmem((2, GRID_W, 128), F32),
        vmem((pairs, *full), BF16),
        vmem((pairs, *full), BF16),
        vmem((length_y, *full), BF16),
        vmem(full, BF16),
        vmem((length_z, *full), BF16),
        vmem((length_y, *tile), BF16),
        vmem((length_y, *tile), BF16),
        vmem((pairs, *tile), BF16),
        vmem((pairs, *tile), BF16),
        vmem(tile, F32),
        dma((2,)), dma((length_y, 2)), dma((length_z, 2)), dma((length_y, 2)), dma((2,)),
        dma((2, 2)),
        vmem((rows, channels), BF16),
        vmem((blocks, STATE, 2 * channels), BF16),
        vmem((2, blocks, BLOCK, part // 2), BF16),
        vmem((2, blocks, BLOCK, part // 2), BF16),
        vmem((2, blocks, BLOCK, part), BF16),
        vmem((2, blocks, BLOCK, part), BF16),
        dma((2, blocks, 2)), dma((2, blocks, 2)),
    ]
    return pl.pallas_call(
        functools.partial(layer_kernel, (length_z, length_y)),
        in_specs=[hbm] * (1 + len(smalls) + len(shards)) + [pl.BlockSpec(memory_space=pltpu.SMEM)],
        out_specs=[pl.BlockSpec(memory_space=pltpu.VMEM)] * 2,
        out_shape=[
            jax.ShapeDtypeStruct((rows, part), BF16),
            jax.ShapeDtypeStruct((HEADS, rows), F32),
        ],
        scratch_shapes=scratch,
        compiler_params=pltpu.CompilerParams(
            collective_id=1, has_side_effects=True, vmem_limit_bytes=65_800_000
        ),
        cost_estimate=pl.CostEstimate(flops=1 << 33, bytes_accessed=24 << 20, transcendentals=0),
        name="layer",
    )(tokens, *smalls, *shards, sinks)


def flatten_rows(weight):
    return weight.reshape(weight.shape[0], -1)


def shards(
    tokens, input_gain, gate_weight, value_weight, inflow_weight, readout_weight, step_weight,
    conv_values, conv_inflow, conv_readout, log_rate, group_gain, query_weight, key_weight,
    vector_weight, sink_logit, state_out, window_out,
):
    count = tokens.shape[0]
    length_z, length_y = lax.axis_size(SP[0]), lax.axis_size(SP[1])
    quarter = HEAD_DIM // 4
    powers = (np.arange(128) % quarter).astype(np.float32) / np.float32(quarter)
    freqs = np.broadcast_to(np.float32(ROPE_BASE) ** -powers, (8, 128)).astype(np.float32)
    freqs = jnp.asarray(freqs)
    smalls = (
        input_gain.reshape(-1, 128),
        step_weight.transpose(1, 2, 0).reshape(2 * HEADS, -1),
        conv_values, flatten_rows(conv_inflow), flatten_rows(conv_readout),
        log_rate.transpose(0, 2, 1).reshape(2 * HEADS, count),
        freqs,
        group_gain.reshape(-1, 128),
    )
    shards_here = (
        value_weight, flatten_rows(inflow_weight), flatten_rows(readout_weight), key_weight,
        vector_weight, gate_weight, query_weight, state_out.T, window_out.T,
    )
    mixed, logs = layer(
        length_z, length_y, lax.axis_size("tp"), tokens, smalls, shards_here, sink_logit
    )
    return mixed, logs.T


def solution(mesh):
    torus = Mesh(mesh.devices.reshape(8, 4, 2, mesh.shape["tp"]), (*SP, "tp"))
    return jax.shard_map(
        shards,
        mesh=torus,
        in_specs=(
            P(SP, None), P(), P(SP, "tp"), P(SP, "tp"), P(SP, "tp", None), P(SP, "tp", None),
            P(SP, None, "tp"), P(None, "tp"), P(None, "tp", None), P(None, "tp", None),
            P(None, SP, "tp"), P("tp"), P(SP, "tp"), P(SP, "tp"), P(SP, "tp"), P("tp"),
            P("tp", SP), P("tp", SP),
        ),
        out_specs=(P(SP, "tp"), P(SP, "tp")),
        check_vma=False,
    )
```

```python
import functools
import heapq

import jax
import jax.numpy as jnp
import numpy as np
from jax import lax
from jax.experimental import pallas as pl
from jax.experimental.pallas import tpu as pltpu
from jax.sharding import Mesh
from jax.sharding import PartitionSpec as P

HEAD_DIM = 64
STATE = 128
HEADS = 8
BLOCK = 128
WINDOW = 128
GRID_W = 64
HALO = 16
SP = ("sp_0", "sp_1", "sp_2")
EPS = 1e-06
ROPE_BASE = 10000.0
F32 = jnp.float32
BF16 = jnp.bfloat16
MSG = STATE + 16
KV_AT = 768
Q_AT = 1024
OUT_AT = 512


def dot(a, b, dims=((1,), (0,)), precision=None):
    return lax.dot_general(
        a, b, (dims, ((), ())), preferred_element_type=F32, precision=precision
    )


def split_bf16(value, parts):
    pieces = []
    for _ in range(parts):
        piece = value.astype(BF16)
        pieces.append(piece)
        value = value - piece.astype(F32)
    return pieces


def spread(value, spread_matrix, parts):
    pieces = [p.astype(F32) for p in split_bf16(value, parts)]
    joined = jnp.concatenate(pieces, axis=1).astype(BF16)
    matrix = jnp.concatenate([spread_matrix] * parts, axis=0)
    return dot(joined, matrix)


def as_row(ref):
    wide = ref[...].astype(F32)
    return jnp.concatenate([wide[i : i + 1, :] for i in range(wide.shape[0])], axis=1)


def spread_matrix():
    shape = (2 * HEADS, 2 * HEADS * HEAD_DIM)
    rows = lax.broadcasted_iota(jnp.int32, shape, 0)
    first = lax.broadcasted_iota(jnp.int32, shape, 1) - rows * HEAD_DIM
    return jnp.where((first >= 0) & (first < HEAD_DIM), 1.0, 0.0).astype(BF16)


def conv_state(
    traffic_service, cin_ref, taps_x_ref, taps_b_ref, taps_c_ref, step_ref, rate_ref,
    conv_ref, col_ref, row_ref, piece_ref, etot_ref, msg_ref, win,
):
    count = cin_ref.shape[0] - 2 * HALO
    blocks = count // BLOCK
    channels = HEADS * HEAD_DIM
    spread_m = spread_matrix()
    taps = jnp.concatenate([t[...].astype(F32) for t in (taps_x_ref, taps_b_ref, taps_c_ref)], axis=1)
    lane16 = lax.broadcasted_iota(jnp.int32, (BLOCK, 2 * HEADS), 1)
    forward16 = lane16 < HEADS
    tri = (
        lax.broadcasted_iota(jnp.int32, (BLOCK, BLOCK), 0)
        >= lax.broadcasted_iota(jnp.int32, (BLOCK, BLOCK), 1)
    ).astype(F32)
    win[pl.ds(0, HALO), :] = cin_ref[pl.ds(count, HALO), :].astype(F32)
    win[pl.ds(HALO + count, HALO), :] = cin_ref[pl.ds(count + HALO, HALO), :].astype(F32)

    def fill(i, carry):
        start = pl.multiple_of(i * BLOCK, BLOCK)
        win[pl.ds(HALO + start, BLOCK), :] = cin_ref[pl.ds(start, BLOCK), :].astype(F32)
        return carry

    lax.fori_loop(0, blocks, fill, 0)
    traffic_service(0.5)

    def some(which):
        spans = [slice(i * BLOCK, (i + 1) * BLOCK) for i in which]
        steps, decays, convs = [], [], []
        for rows in spans:
            raw = step_ref[rows, 0 : 2 * HEADS]
            steps.append(jnp.maximum(raw, 0.0) + jnp.log1p(jnp.exp(-jnp.abs(raw))))
            rate = jnp.concatenate(
                [rate_ref[:, rows], jnp.zeros((BLOCK - 2 * HEADS, BLOCK), F32)], axis=0
            )
            decays.append(-jnp.exp(rate.T[:, 0 : 2 * HEADS]) * steps[-1])
        cums = [dot(tri, decay, precision=lax.Precision.HIGHEST) for decay in decays]
        tots = [cum[BLOCK - 1 : BLOCK, :] for cum in cums]
        cols = [jnp.where(forward16, cum, cum - decay) for cum, decay in zip(cums, decays)]
        weights = [
            jnp.exp(jnp.where(forward16, tot - col, col)) * step
            for tot, col, step in zip(tots, cols, steps)
        ]
        wides = [spread(weight, spread_m, 2) for weight in weights]
        etots = [spread(jnp.exp(jnp.broadcast_to(tot, (8, 2 * HEADS))), spread_m, 3) for tot in tots]
        rests = jnp.zeros((BLOCK, 128 - 4 * HEADS), F32)
        turned = [jnp.concatenate([col, step, rests], axis=1).T for col, step in zip(cols, steps)]
        for rows in spans:
            acc = 0.0
            for tap in range(5):
                first = rows.start + HALO - 2 + tap
                acc = acc + win[first : first + BLOCK, :] * taps[tap : tap + 1, :]
            convs.append((acc * jax.nn.sigmoid(acc)).astype(BF16))
        pieces = []
        for conv, wide in zip(convs, wides):
            xs = conv[:, 0:channels].astype(F32)
            scaled = (jnp.concatenate([xs, xs], axis=1) * wide).astype(BF16)
            pieces.append(dot(conv[:, channels : channels + STATE], scaled, ((0,), (0,))))
        for n, (i, rows) in enumerate(zip(which, spans)):
            conv_ref[rows, :] = convs[n]
            col_ref[rows, 0 : 2 * HEADS] = cols[n]
            col_ref[rows, 2 * HEADS : 4 * HEADS] = jnp.broadcast_to(tots[n], (BLOCK, 2 * HEADS))
            row_ref[i] = turned[n][0 : 4 * HEADS, :]
            piece_ref[i] = pieces[n]
            etot_ref[i] = etots[n]
        return sum(tots)

    total = jnp.zeros((1, 2 * HEADS), F32)
    for i in range(0, blocks, 2):
        total = total + some((i, i + 1))
        traffic_service(1.6)
    forward = piece_ref[0, :, 0:channels]
    backward = piece_ref[blocks - 1, :, channels : 2 * channels]
    for i in range(1, blocks):
        forward = etot_ref[i, 0:1, 0:channels] * forward + piece_ref[i, :, 0:channels]
        k = blocks - 1 - i
        backward = (
            etot_ref[k, 0:1, channels : 2 * channels] * backward
            + piece_ref[k, :, channels : 2 * channels]
        )
    spread_total = spread(jnp.broadcast_to(total, (16, 2 * HEADS)), spread_m, 3)
    hi, mid, lo = split_bf16(spread_total, 3)
    which = lax.broadcasted_iota(jnp.int32, (16, 2 * channels), 0)
    tail = jnp.where(
        which == 0, hi.astype(F32), jnp.where(which == 1, mid.astype(F32), lo.astype(F32))
    ).astype(BF16)
    for e, state in enumerate((forward, backward)):
        for pair in range(channels // 128):
            lanes = slice(pair * 128, pair * 128 + 128)
            msg_ref[e, pair, 0:STATE, :] = state[:, lanes].astype(BF16)
            msg_ref[e, pair, STATE:MSG, :] = tail[:, e * channels + pair * 128 : e * channels + pair * 128 + 128]


def mixer(conv_ref, col_ref, row_ref, piece_ref, etot_ref, in_ref, gate_ref, gain_ref, out_ref, held):
    count = conv_ref.shape[0]
    blocks = count // BLOCK
    channels = HEADS * HEAD_DIM
    spread_m = spread_matrix()
    gain = as_row(gain_ref)
    for e in range(2):
        state = jnp.concatenate(
            [in_ref[e, p].astype(F32) for p in range(channels // 128)], axis=1
        )
        lanes = slice(e * channels, (e + 1) * channels)
        for i in range(blocks) if e == 0 else reversed(range(blocks)):
            held[i, :, lanes] = state.astype(BF16)
            state = etot_ref[i, 0:1, lanes] * state + piece_ref[i, :, lanes]
    row_at = lax.broadcasted_iota(jnp.int32, (BLOCK, BLOCK), 0)
    col_at = lax.broadcasted_iota(jnp.int32, (BLOCK, BLOCK), 1)
    lower = row_at >= col_at
    diagonal = row_at == col_at
    first_half = col_at < HEAD_DIM
    forward16 = lax.broadcasted_iota(jnp.int32, (BLOCK, 2 * HEADS), 1) < HEADS

    def one(i):
        rows = pl.ds(pl.multiple_of(i * BLOCK, BLOCK), BLOCK)
        inflow = conv_ref[rows, channels : channels + STATE]
        readout = conv_ref[rows, channels + STATE : channels + 2 * STATE]
        inner = dot(readout, inflow, ((1,), (1,)))
        col = col_ref[rows, 0 : 2 * HEADS]
        tot = col_ref[rows, 2 * HEADS : 4 * HEADS]
        reach = spread(jnp.exp(jnp.where(forward16, col, tot - col)), spread_m, 2)
        far = dot(readout, held[i]) * reach
        parts = []
        for pair in range(HEADS // 2):
            weights = []
            for h in (2 * pair, 2 * pair + 1):
                b = HEADS + h
                arg = jnp.where(
                    lower,
                    col[:, h : h + 1] - row_ref[i, h : h + 1, :],
                    row_ref[i, b : b + 1, :] - col[:, b : b + 1],
                )
                step_f = row_ref[i, 2 * HEADS + h : 2 * HEADS + h + 1, :]
                step_b = row_ref[i, 2 * HEADS + b : 2 * HEADS + b + 1, :]
                step = jnp.where(lower, step_f, step_b) + jnp.where(diagonal, step_b, 0.0)
                weights.append((inner * jnp.exp(arg) * step).astype(BF16))
            xs = conv_ref[rows, pair * 128 : pair * 128 + 128]
            zero = jnp.zeros_like(xs)
            stacked = jnp.concatenate(
                [jnp.where(first_half, xs, zero), jnp.where(first_half, zero, xs)], axis=0
            )
            parts.append(dot(jnp.concatenate(weights, axis=1), stacked))
        y = jnp.concatenate(parts, axis=1) + far[:, 0:channels] + far[:, channels:]
        gate = gate_ref[rows, :].astype(F32)
        y = y * (gate * jax.nn.sigmoid(gate))
        y = y * lax.rsqrt(jnp.mean(y * y, axis=1, keepdims=True) + EPS)
        out_ref[rows, :] = (y * gain).astype(BF16)

    return one


def attention(
    count, q_ref, kv_ref, before_ref, after_ref, freq_ref, sink_ref,
    out_ref, log_ref, keys, values, by_row, by_col,
):
    blocks = count // BLOCK
    place = lax.axis_index(SP)
    lane = lax.broadcasted_iota(jnp.int32, (BLOCK, 128), 1)
    low_quarter = lane % 32 < 16
    first_half = lane < HEAD_DIM
    row_lane = (lane % HEAD_DIM < 32)[0:GRID_W]

    grid_rows = by_row.shape[1]
    first_row = place * (count // GRID_W) - WINDOW // GRID_W
    sign = jnp.where(low_quarter, -1.0, 1.0)
    for ref, first, length in ((by_row, first_row, grid_rows), (by_col, 0, GRID_W)):
        at = lax.broadcasted_iota(jnp.int32, (length, 128), 0) + first
        angle = at.astype(F32) * freq_ref[0:1, :]
        ref[0] = jnp.cos(angle)
        ref[1] = jnp.sin(angle) * sign[0:length]

    def tables(slot):
        out = []
        for kind in range(2):
            parts = []
            for r in range(BLOCK // GRID_W):
                row = by_row[kind, pl.ds(slot * (BLOCK // GRID_W) + r, 1), :]
                parts.append(jnp.where(row_lane, row, by_col[kind]))
            out.append(jnp.concatenate(parts, axis=0))
        return out

    def turn(value, table):
        wide = value.astype(F32)
        other = jnp.where(low_quarter, pltpu.roll(wide, 112, 1), pltpu.roll(wide, 16, 1))
        return (wide * table[0] + other * table[1]).astype(BF16)

    def store(raw, slot):
        rows = pl.ds(pl.multiple_of(slot * BLOCK, BLOCK), BLOCK)
        key = turn(raw[:, 0:128], tables(slot)).astype(F32)
        swapped = pltpu.roll(key, 64, 1)
        keys[0, rows, :] = jnp.where(first_half, key, swapped).astype(BF16)
        keys[1, rows, :] = jnp.where(first_half, swapped, key).astype(BF16)
        values[:, rows] = raw[:, 128:256].astype(F32).T.astype(BF16)

    def own_keys():
        def fill(i, carry):
            rows = pl.ds(pl.multiple_of(i * BLOCK, BLOCK), BLOCK)
            store(kv_ref[rows, :], i + 1)
            return carry

        lax.fori_loop(0, blocks, fill, 0)

    def edge_keys():
        store(before_ref[...], 0)
        store(after_ref[...], blocks + 1)

    key_at = lax.broadcasted_iota(jnp.int32, (3 * BLOCK, 2 * BLOCK), 0)
    query_at = lax.broadcasted_iota(jnp.int32, (3 * BLOCK, 2 * BLOCK), 1) % BLOCK
    in_band = (key_at >= query_at) & (key_at <= query_at + 2 * WINDOW)
    first_row_half = lax.broadcasted_iota(jnp.int32, (1, 2 * BLOCK), 1) < BLOCK
    start_at = -place * count
    end_at = start_at + count * lax.axis_size(SP)

    def one(i):
        start = pl.multiple_of(i * BLOCK, BLOCK)
        rows = pl.ds(start, BLOCK)
        here = key_at + (start - WINDOW)
        valid = in_band & (here >= start_at) & (here < end_at)
        table = tables(i + 1)
        band = pl.ds(start, 3 * BLOCK)
        qs = []
        for pair in range(HEADS // 2):
            lanes = slice(pair * 128, pair * 128 + 128)
            q = (turn(q_ref[rows, lanes], table).astype(F32) * HEAD_DIM ** (-0.5)).astype(BF16)
            zero = jnp.zeros_like(q)
            qs.append(jnp.concatenate(
                [jnp.where(first_half, q, zero), jnp.where(first_half, zero, q)], axis=0
            ))
        scores = [dot(keys[pair // 2, band, :], q, ((1,), (1,))) for pair, q in enumerate(qs)]
        outs = []
        for pair in range(HEADS // 2):
            group = pair // 2
            mine = jnp.where(valid, scores[pair], -1e30)
            sink = jnp.where(first_row_half, sink_ref[2 * pair], sink_ref[2 * pair + 1])
            top = jnp.maximum(jnp.max(mine, axis=0, keepdims=True), sink)
            expo = jnp.exp(mine - top)
            total = jnp.sum(expo, axis=0, keepdims=True) + jnp.exp(sink - top)
            value = values[group * HEAD_DIM : (group + 1) * HEAD_DIM, band]
            outs.append(dot(value, expo.astype(BF16)) / total)
            log = top + jnp.log(total)
            log_ref[2 * pair : 2 * pair + 1, rows] = log[:, 0:BLOCK]
            log_ref[2 * pair + 1 : 2 * pair + 2, rows] = log[:, BLOCK:]
        for pair, o in enumerate(outs):
            turned = jnp.concatenate([o[:, 0:BLOCK], o[:, BLOCK:]], axis=0).T
            out_ref[rows, pair * 128 : pair * 128 + 128] = turned.astype(BF16)

    return own_keys, edge_keys, one


LINKS = ("z+", "z-", "y+", "y-")
WIDTHS = (1664, 1536)
ROUTES = (
    (("A", 0, 0, 1024, 512, "z"), ("B", 0, 1024, 640, 384, "y")),
    (("C", 1, 0, 896, 512, "z"), ("D", 1, 896, 640, 384, "y")),
)
BEGIN_AFTER = (76,)
RATE = 42.0e3
HOP = 2.6


def ring(route, axis, other, length):
    name, array, column, total, cut, _ = route
    out = []
    for sign in (1, -1):
        previous = None
        for step in range(length // 2):
            cols = (column, total)
            if step == length // 2 - 1:
                cols = (column, cut) if sign == 1 else (column + cut, total - cut)
            key = (name, axis, other, sign, step)
            out.append(dict(
                key=key, route=name, array=array, axis=axis, sign=sign, along=-sign * step,
                other=other, cols=cols, needs=[previous] if previous else [],
            ))
            previous = key
    return out


def transfers(routes, lengths):
    sends, groups = [], {}
    for route in routes:
        name, _, _, _, _, first = route
        second = "y" if first == "z" else "z"
        length = lengths[first]
        sends += ring(route, first, 0, length)
        for offset in range(-(length // 2) + 1, length // 2 + 1):
            one = ring(route, second, offset, lengths[second])
            needs = []
            if offset == length // 2:
                needs = [(name, first, 0, sign, length // 2 - 1) for sign in (1, -1)]
            elif offset:
                needs = [(name, first, 0, -1 if offset > 0 else 1, abs(offset) - 1)]
            for s in one:
                s["needs"] = s["needs"] or needs
            sends += one
            groups[(name, offset)] = {s["key"] for s in one}
    return sends, groups


class Flow:
    def __init__(self, number, lengths, arrays, sems, free):
        self.routes = ROUTES[number]
        self.lengths = lengths
        self.arrays = arrays
        self.send_sem, self.recv_sem, self.core_send, self.core_recv = sems
        self.free = free
        self.at = dict(zip("zy", (lax.axis_index(SP[0]), lax.axis_index(SP[1]))))
        self.c = lax.axis_index(SP[2])
        self.sends, self.groups = transfers(self.routes, lengths)
        self.number = {s["key"]: i for i, s in enumerate(self.sends)}
        self.by_key = {s["key"]: s for s in self.sends}
        self.group_keys = list(self.groups)
        self.left = {s["key"]: len(s["needs"]) for s in self.sends}
        self.followers = {}
        for s in self.sends:
            for need in s["needs"]:
                self.followers.setdefault(need, []).append(s)
        self.first_axis = {route[0]: route[5] for route in self.routes}
        self.heap = []
        self.clock = 0.0
        self.started = []
        self.launched = 0

    def wrap(self, axis, shift):
        length = self.lengths[axis]
        return lax.rem(self.at[axis] + shift + length, length)

    def rank(self, s):
        return (s["axis"] != self.first_axis[s["route"]], s["route"])

    def copy_of(self, s, shift):
        along = s["along"] - shift * s["sign"]
        place = {s["axis"]: along, "y" if s["axis"] == "z" else "z": s["other"]}
        ref = self.arrays[s["array"]].at[
            self.wrap("z", place["z"]), self.wrap("y", place["y"]), self.c, :, pl.ds(*s["cols"])
        ]
        i = self.number[s["key"]]
        to = {SP["zy".index(s["axis"])]: self.wrap(s["axis"], s["sign"])}
        return pltpu.make_async_remote_copy(
            src_ref=ref, dst_ref=ref, send_sem=self.send_sem.at[i], recv_sem=self.recv_sem.at[i],
            device_id=to, device_id_type=pl.DeviceIdType.MESH,
        )

    def core_copy(self, key, c):
        name, offset = key
        i = self.group_keys.index(key)
        route = [r for r in self.routes if r[0] == name][0]
        ref = self.arrays[route[1]]
        cols = pl.ds(route[2], route[3])
        if route[5] == "z":
            ref = ref.at[self.wrap("z", offset), :, c, :, cols]
        else:
            ref = ref.at[:, self.wrap("y", offset), c, :, cols]
        return pltpu.make_async_remote_copy(
            src_ref=ref, dst_ref=ref, send_sem=self.core_send.at[i],
            recv_sem=self.core_recv.at[i], device_id={SP[2]: 1 - self.c},
            device_id_type=pl.DeviceIdType.MESH,
        )

    def launch(self, s):
        copy = self.copy_of(s, 0)
        copy.start()
        self.started.append(copy)
        self.launched += 1
        link = s["axis"] + ("+" if s["sign"] == 1 else "-")
        self.free[link] = max(self.free[link], self.clock) + 64 * s["cols"][1] / RATE
        heapq.heappush(self.heap, (self.free[link] + HOP, len(self.started), s["key"]))

    def begin(self):
        for s in sorted((s for s in self.sends if not s["needs"]), key=self.rank):
            self.launch(s)

    def handle(self):
        _, _, key = heapq.heappop(self.heap)
        self.copy_of(self.by_key[key], 1).wait_recv()
        for s in sorted(self.followers.get(key, []), key=self.rank):
            self.left[s["key"]] -= 1
            if self.left[s["key"]] == 0:
                self.launch(s)
        for group, keys in self.groups.items():
            if key in keys:
                keys.remove(key)
                if not keys:
                    copy = self.core_copy(group, self.c)
                    copy.start()
                    self.started.append(copy)

    def wait_core(self):
        for group in self.group_keys:
            self.core_copy(group, 1 - self.c).wait_recv()


class Traffic:
    def __init__(self, lengths, arrays, sems):
        free = dict.fromkeys(LINKS, 0.0)
        self.flows = [Flow(i, lengths, arrays, s, free) for i, s in enumerate(sems)]
        self.lengths = lengths
        self.arrays = arrays
        self.clock = 0.0
        self.newest = 0

    def begin(self):
        self.flows[0].begin()

    def next_arrival(self):
        return min(((f.heap[0][0], i) for i, f in enumerate(self.flows) if f.heap), default=None)

    def handle(self, index, now):
        flow = self.flows[index]
        flow.clock = max(flow.clock, now)
        flow.handle()
        if index == self.newest and index + 1 < len(self.flows):
            if flow.launched >= BEGIN_AFTER[index]:
                self.newest += 1
                self.flows[self.newest].clock = flow.clock
                self.flows[self.newest].begin()

    def service(self, passed):
        self.clock += passed
        while (head := self.next_arrival()) and head[0] <= self.clock:
            self.handle(head[1], self.clock)

    def until(self, index):
        while self.newest < index or self.flows[index].heap:
            head = self.next_arrival()
            self.clock = max(self.clock, head[0])
            self.handle(head[1], self.clock)
        self.flows[index].wait_core()

    def finish(self):
        for flow in self.flows:
            for copy in flow.started:
                copy.wait_send()


def gather(
    traffic, small_copies, enter, tok_ref, gain_ref, step_ref, value_ref, inflow_ref,
    readout_ref, key_ref, vector_ref, gate_ref, query_ref, state_ref, window_ref,
    normed, before, after, held, edge_sem, own_sem,
):
    z, y, c = (lax.axis_index(a) for a in SP)
    length_z, length_y = traffic.lengths["z"], traffic.lengths["y"]
    flat = (z * length_y + y) * 2 + c
    count = length_z * length_y * 2
    count_rows = tok_ref.shape[0]
    a_ref, b_ref = traffic.arrays

    def device_at(index):
        index = lax.rem(index + count, count)
        return {
            SP[0]: index // (2 * length_y),
            SP[1]: lax.rem(index // 2, length_y),
            SP[2]: lax.rem(index, 2),
        }

    moves = []
    for array, refs in (
        (a_ref, (value_ref, inflow_ref, readout_ref, key_ref, vector_ref, query_ref)),
        (b_ref, (gate_ref, state_ref, window_ref)),
    ):
        column = 0
        for ref in refs:
            width = ref.shape[1]
            moves.append((ref, array.at[z, y, c, :, pl.ds(column, width)]))
            column += width
    moves.append((tok_ref, held))
    moves = [pltpu.make_async_copy(*move, own_sem.at[i]) for i, move in enumerate(moves)]
    for move in moves:
        move.start()
    small_copies()
    step = step_ref[...].astype(F32)
    rows, cols = step.shape
    step = jnp.concatenate([step, jnp.zeros((rows, 128 - cols), F32)], axis=1)
    step = jnp.concatenate([step, jnp.zeros((128 - rows, 128), F32)], axis=0)
    a_ref[z, y, c, :, WIDTHS[0] - 128 : WIDTHS[0]] = step.T[0:cols, :].astype(BF16)
    for move in moves[:6]:
        move.wait()
    enter()
    edge_copies = []
    for k, (index, dst) in enumerate(((flat - 1, after), (flat + 1, before))):
        edge_copies.append(pltpu.make_async_remote_copy(
            src_ref=tok_ref.at[pl.ds(k * (count_rows - HALO), HALO)], dst_ref=dst,
            send_sem=edge_sem.at[k, 0], recv_sem=edge_sem.at[k, 1],
            device_id=device_at(index), device_id_type=pl.DeviceIdType.MESH,
        ))
    gain = as_row(gain_ref)

    def norm(value):
        wide = value.astype(F32)
        scale = lax.rsqrt(jnp.mean(wide * wide, axis=1, keepdims=True) + EPS)
        return wide * scale * gain

    def norm_blocks(first, last):
        def norm_block(i, carry):
            rows = pl.ds(pl.multiple_of(i * BLOCK, BLOCK), BLOCK)
            normed[rows, :] = norm(held[rows, :]).astype(BF16)
            return carry

        lax.fori_loop(first, last, norm_block, 0)

    traffic.begin()
    for copy in edge_copies:
        copy.start()
    for move in moves[6:]:
        move.wait()
    blocks = count_rows // BLOCK
    traffic.service(1.0)
    for i in range(blocks):
        norm_blocks(i, i + 1)
        traffic.service(0.6)
    for copy in edge_copies:
        copy.wait()
    normed[count_rows : count_rows + HALO, :] = jnp.where(flat > 0, norm(before[...]), 0.0).astype(BF16)
    normed[count_rows + HALO : count_rows + 2 * HALO, :] = jnp.where(
        flat < count - 1, norm(after[...]), 0.0
    ).astype(BF16)
    traffic.service(0.3)
    traffic.until(0)
    traffic.service(0.5)


def middle(
    traffic, normed, a_ref, b_ref, taps_x_ref, taps_b_ref, taps_c_ref, rate_ref, freq_ref, sink_ref,
    out_ref, window_ref, log_ref, gate_ref, conv_ref, col_ref, row_ref, piece_ref, etot_ref,
    cin_ref, kv_ref, q_ref, step_ref, win, near, msg_ref,
    kv_before_ref, kv_after_ref, keys, values, by_row, by_col, part, turned, by_y, summed, by_z,
    back, arrived, nxt, final, carry,
    part_sem, y_sem, z_sem, back_sem, final_sem, kv_sem,
):
    rows = kv_ref.shape[0]
    z, y, c = (lax.axis_index(a) for a in SP)
    length_z, length_y = lax.axis_size(SP[0]), lax.axis_size(SP[1])
    forward = c == 0
    other = 1 - c
    order_z = jnp.where(forward, z, length_z - 1 - z)
    mesh_id = pl.DeviceIdType.MESH
    flat = (z * length_y + y) * 2 + c
    count = length_z * length_y * 2

    def device_at(index):
        index = lax.rem(index + count, count)
        return {
            SP[0]: index // (2 * length_y),
            SP[1]: lax.rem(index // 2, length_y),
            SP[2]: lax.rem(index, 2),
        }

    def project(dst, count, tiles, source, first):
        tile = 256
        for j in range(tiles):
            cols = slice(first + j * tile, first + (j + 1) * tile)
            dst[:, j * tile : (j + 1) * tile] = dot(normed[0:count, :], source[:, cols]).astype(BF16)
            traffic.service(1.05)

    project(kv_ref, rows, 1, a_ref, KV_AT)

    def send(src, dst, sems, peer):
        copy = pltpu.make_async_remote_copy(
            src_ref=src, dst_ref=dst, send_sem=sems.at[0], recv_sem=sems.at[1],
            device_id=peer, device_id_type=mesh_id,
        )
        copy.start()
        return copy

    def state_of(ref, *at):
        return ref[(*at, slice(0, STATE), slice(None))].astype(F32)

    def decay_of(ref, *at):
        tail = ref[(*at, slice(STATE, MSG), slice(None))].astype(F32)
        return tail[0:1] + tail[1:2] + tail[2:3]

    def put(ref, state, decay, *at):
        ref[(*at, slice(0, STATE), slice(None))] = state.astype(BF16)
        hi, mid, lo = (p.astype(F32) for p in split_bf16(decay, 3))
        which = lax.broadcasted_iota(jnp.int32, (MSG - STATE, 128), 0)
        tail = jnp.where(which == 0, hi, jnp.where(which == 1, mid, lo))
        ref[(*at, slice(STATE, MSG), slice(None))] = tail.astype(BF16)

    pairs = msg_ref.shape[1]
    kv_copies = [
        send(
            kv_ref.at[pl.ds(rows - WINDOW, WINDOW)], kv_before_ref, kv_sem.at[0],
            device_at(flat + 1),
        ),
        send(kv_ref.at[pl.ds(0, WINDOW)], kv_after_ref, kv_sem.at[1], device_at(flat - 1)),
    ]
    project(cin_ref, rows + 2 * HALO, 3, a_ref, 0)
    step_ref[...] = dot(normed[0:rows, :], a_ref[:, WIDTHS[0] - 128 : WIDTHS[0]])
    traffic.service(0.6)
    conv_state(
        traffic.service,
        cin_ref, taps_x_ref, taps_b_ref, taps_c_ref, step_ref, rate_ref,
        conv_ref, col_ref, row_ref, piece_ref, etot_ref, msg_ref, win,
    )
    copy = send(msg_ref.at[other], part, part_sem, {SP[2]: other})
    own_keys, edge_keys, attend = attention(
        rows, q_ref, kv_ref, kv_before_ref, kv_after_ref, freq_ref, sink_ref,
        window_ref, log_ref, keys, values, by_row, by_col,
    )

    blocks = rows // BLOCK
    own_keys()
    traffic.service(1.2)
    copy.wait()
    for j in range(pairs):
        decay = decay_of(part, j)
        put(
            turned,
            jnp.exp(decay) * state_of(msg_ref, c, j) + state_of(part, j),
            decay + decay_of(msg_ref, c, j),
            j,
        )
    copies = []
    for k in range(1, length_y):
        to = lax.rem(y + k, length_y)
        copies.append(send(turned.at[to], by_y.at[k], y_sem.at[k], {SP[1]: to}))
    by_y[0] = turned[y]
    project(q_ref, rows, 2, a_ref, Q_AT)
    attend(1)
    traffic.service(1.1)
    for copy in copies:
        copy.wait()
    before = []
    state = jnp.zeros((STATE, 128), F32)
    decay = jnp.zeros((1, 128), F32)
    for q in range(length_y):
        before.append((state, decay))
        slot = jnp.where(forward, lax.rem(y - q + length_y, length_y), lax.rem(y + 1 + q, length_y))
        step = decay_of(by_y, slot)
        state = jnp.exp(step) * state + state_of(by_y, slot)
        decay = decay + step
    put(summed, state, decay)
    for k in range(1, length_z):
        to = lax.rem(z + k, length_z)

        @pl.when((z + k >= length_z) == (c == 1))
        def _():
            send(summed, by_z.at[k], z_sem.at[k], {SP[0]: to})

    carry[...] = jnp.zeros_like(carry)
    for i in range(2, blocks - 1):
        attend(i)
        traffic.service(1.1)
    for distance in reversed(range(1, length_z)):
        slot = jnp.where(forward, distance, length_z - distance)

        @pl.when(order_z >= distance)
        def _():
            pltpu.make_async_remote_copy(
                src_ref=summed, dst_ref=by_z.at[slot], send_sem=z_sem.at[slot, 0],
                recv_sem=z_sem.at[slot, 1], device_id={SP[0]: z}, device_id_type=mesh_id,
            ).wait_recv()
            carry[...] = jnp.exp(decay_of(by_z, slot)) * carry[...] + state_of(by_z, slot)

    for k in range(1, length_z):
        to = lax.rem(z + k, length_z)

        @pl.when((z + k >= length_z) == (c == 1))
        def _():
            pltpu.make_async_remote_copy(
                src_ref=summed, dst_ref=by_z.at[k], send_sem=z_sem.at[k, 0],
                recv_sem=z_sem.at[k, 1], device_id={SP[0]: to}, device_id_type=mesh_id,
            ).wait_send()

    incoming = carry[...]
    for q in range(length_y):
        to = jnp.where(forward, q, length_y - 1 - q)
        state, decay = before[q]
        back[to] = (jnp.exp(decay) * incoming + state).astype(BF16)
    copies = []
    for k in range(1, length_y):
        to = lax.rem(y + k, length_y)
        copies.append(send(back.at[to], arrived.at[k], back_sem.at[k], {SP[1]: to}))
    arrived[0] = back[y]
    for copy in kv_copies:
        copy.wait()
    edge_keys()
    attend(0)
    traffic.service(1.3)
    for copy in copies:
        copy.wait()
    for j in range(pairs):
        state = arrived[lax.rem(y - j + length_y, length_y)]
        out_ref[c, j] = state
        nxt[j] = (
            jnp.exp(decay_of(msg_ref, c, j)) * state.astype(F32) + state_of(msg_ref, c, j)
        ).astype(BF16)
    copy = send(nxt, final, final_sem, {SP[2]: other})
    attend(blocks - 1)
    traffic.service(1.1)
    traffic.until(1)
    project(gate_ref, rows, 2, b_ref, 0)
    copy.wait()
    out_ref[other] = final[...]


def finish(
    window_ref, w_ref, conv_ref, col_ref, row_ref, piece_ref, etot_ref, in_ref, gate_ref, gain_ref,
    out_ref, *refs
):
    state_ref, held, far_out, far_in, near_out, near_in, far_sem, near_sem = refs
    n = lax.axis_size("tp")
    me = lax.axis_index("tp")
    mesh_id = pl.DeviceIdType.MESH
    sides = (1, -1)
    count, channels = state_ref.shape
    mix = mixer(
        conv_ref, col_ref, row_ref, piece_ref, etot_ref, in_ref, gate_ref, gain_ref, state_ref, held
    )
    width = w_ref.shape[0] // n
    half = width // 2
    chunk = far_out.shape[2]
    chunks = count // chunk

    def at(step):
        return lax.rem(me + step + n, n)

    def terms(rows, to):
        outs = pl.ds(pl.multiple_of(to * width, width), width)
        return dot(state_ref[rows, :], w_ref[outs, OUT_AT : OUT_AT + channels], ((1,), (1,))) + dot(
            window_ref[rows, :], w_ref[outs, OUT_AT + channels : OUT_AT + 2 * channels], ((1,), (1,))
        )

    def far_copy(i, k):
        return pltpu.make_async_remote_copy(
            src_ref=far_out.at[k, i], dst_ref=far_in.at[k, i], send_sem=far_sem.at[k, i, 0],
            recv_sem=far_sem.at[k, i, 1], device_id={"tp": at(sides[k])}, device_id_type=mesh_id,
        )

    def near_copy(i, k):
        return pltpu.make_async_remote_copy(
            src_ref=near_out.at[k, i], dst_ref=near_in.at[k, i], send_sem=near_sem.at[k, i, 0],
            recv_sem=near_sem.at[k, i, 1], device_id={"tp": at(sides[k])}, device_id_type=mesh_id,
        )

    def send_far(i, carry):
        rows = pl.ds(pl.multiple_of(i * chunk, chunk), chunk)
        value = terms(rows, at(2)).astype(BF16)
        for k in range(2):
            far_out[k, i] = value[:, k * half : (k + 1) * half]
            far_copy(i, k).start()

        @pl.when(i + 1 < chunks)
        def _():
            mix(i + 1)

        return carry

    mix(0)
    lax.fori_loop(0, chunks, send_far, 0)

    def send_near(i, carry):
        rows = pl.ds(pl.multiple_of(i * chunk, chunk), chunk)
        for k in range(2):
            value = terms(rows, at(sides[k])).astype(BF16).astype(F32)
            lanes = slice(k * half, (k + 1) * half)
            far_copy(i, k).wait_recv()
            near_out[k, i] = value.astype(BF16)
            near_out[k, i, :, lanes] = (value[:, lanes] + far_in[k, i].astype(F32)).astype(BF16)
            near_copy(i, k).start()
        return carry

    lax.fori_loop(0, chunks, send_near, 0)

    def collect(i, carry):
        rows = pl.ds(pl.multiple_of(i * chunk, chunk), chunk)
        value = terms(rows, me).astype(BF16).astype(F32)
        for k in range(2):
            near_copy(i, k).wait_recv()
            value = value + near_in[k, i].astype(F32)
        out_ref[rows, :] = value.astype(BF16)
        for k in range(2):
            far_copy(i, k).wait_send()
            near_copy(i, k).wait_send()
        return carry

    lax.fori_loop(0, chunks, collect, 0)


def layer_kernel(
    lengths, tok_ref, *refs
):
    length_z, length_y = lengths
    smalls_hbm, refs = refs[:8], refs[8:]
    shards, refs = refs[:9], refs[9:]
    sink_ref, mixed_ref, log_ref = refs[:3]
    smalls, refs = refs[3:11], refs[11:]
    small_sem, arrays, normed = refs[0], refs[1:3], refs[3]
    gather_refs, refs = refs[4:9], refs[9:]
    flow_sems, refs = (refs[0:4], refs[4:8]), refs[8:]
    incoming, window_ref, gate_ref = refs[:3]
    conv_refs, refs = refs[3:8], refs[8:]
    middle_refs, finish_refs = refs[:29], refs[29:]
    gain_ref, step_ref, taps_x, taps_b, taps_c, rate_ref, freq_ref, group_gain_ref = smalls
    z, y, c = (lax.axis_index(a) for a in SP)
    t = lax.axis_index("tp")
    n = lax.axis_size("tp")
    flat = (z * length_y + y) * 2 + c
    count = length_z * length_y * 2
    peers = [{SP[2]: 1 - c}]
    peers += [{SP[1]: lax.rem(y + k, length_y)} for k in range(1, length_y)]
    peers += [{SP[0]: lax.rem(z + k, length_z)} for k in range(1, length_z)]
    peers += [{"tp": lax.rem(t + k, n)} for k in (1, n - 1)]
    for shift in (1, count - 1):
        index = lax.rem(flat + shift, count)
        peers.append({
            SP[0]: index // (2 * length_y),
            SP[1]: lax.rem(index // 2, length_y),
            SP[2]: lax.rem(index, 2),
        })
    barrier = pltpu.get_barrier_semaphore()
    for peer in peers:
        pl.semaphore_signal(barrier, inc=1, device_id=peer, device_id_type=pl.DeviceIdType.MESH)
    copies = [
        pltpu.make_async_copy(src, dst, small_sem.at[i])
        for i, (src, dst) in enumerate(zip(smalls_hbm, smalls))
    ]
    for copy in copies:
        copy.start()

    def small_copies():
        for copy in copies:
            copy.wait()

    def enter():
        pl.semaphore_wait(barrier, len(peers))

    traffic = Traffic({"z": length_z, "y": length_y}, arrays, flow_sems)
    gather(
        traffic, small_copies, enter, tok_ref, gain_ref, step_ref, *shards, normed, *gather_refs,
    )
    flat_refs = [
        ref.reshape(length_z * length_y * 64, width) for ref, width in zip(arrays, WIDTHS)
    ]
    middle(
        traffic, normed, *flat_refs, taps_x, taps_b, taps_c, rate_ref, freq_ref, sink_ref,
        incoming, window_ref, log_ref, gate_ref, *conv_refs, *middle_refs,
    )
    finish(
        window_ref, flat_refs[1], *conv_refs, incoming, gate_ref, group_gain_ref, mixed_ref, *finish_refs
    )
    traffic.finish()


def layer(length_z, length_y, n, tokens, smalls, shards, sinks):
    rows, model = tokens.shape
    channels = HEADS * HEAD_DIM
    width = channels + 2 * STATE
    blocks = rows // BLOCK
    pairs = channels // 128
    tile = (STATE, 128)
    full = (MSG, 128)
    lead = (length_z, length_y, 2, 32)
    flows = [transfers(routes, {"z": length_z, "y": length_y}) for routes in ROUTES]
    part = model // n
    dma = pltpu.SemaphoreType.DMA
    vmem = pltpu.VMEM
    hbm = pl.BlockSpec(memory_space=pl.ANY)
    scratch = [
        *(vmem(s.shape, s.dtype) for s in smalls),
        dma((len(smalls),)),
        *(vmem((*lead, w), BF16) for w in WIDTHS),
        vmem((rows + 2 * HALO, model), BF16),
        vmem((HALO, model), BF16), vmem((HALO, model), BF16), vmem((rows, model), BF16),
        dma((2, 2)), dma((len(shards) + 1,)),
        *(dma((len(part),)) for sends, groups in flows for part in (sends, sends, groups, groups)),
        vmem((2, pairs, *tile), BF16),
        vmem((rows, channels), BF16),
        vmem((rows, channels), BF16),
        vmem((rows, width), BF16),
        vmem((rows, 4 * HEADS), F32),
        vmem((blocks, 4 * HEADS, BLOCK), F32),
        vmem((blocks, STATE, 2 * channels), F32),
        vmem((blocks, 8, 2 * channels), F32),
        vmem((rows + 2 * HALO, width), BF16),
        vmem((rows, 256), BF16),
        vmem((rows, channels), BF16),
        vmem((rows, 128), F32),
        vmem((rows + 2 * HALO, width), F32),
        vmem((BLOCK + 2 * HALO, width), F32),
        vmem((2, pairs, *full), BF16),
        vmem((WINDOW, 256), BF16),
        vmem((WINDOW, 256), BF16),
        vmem((2, rows + 2 * BLOCK, 128), BF16),
        vmem((128, rows + 2 * BLOCK), BF16),
        vmem((2, (rows + 2 * WINDOW) // GRID_W, 128), F32),
        vmem((2, GRID_W, 128), F32),
        vmem((pairs, *full), BF16),
        vmem((pairs, *full), BF16),
        vmem((length_y, *full), BF16),
        vmem(full, BF16),
        vmem((length_z, *full), BF16),
        vmem((length_y, *tile), BF16),
        vmem((length_y, *tile), BF16),
        vmem((pairs, *tile), BF16),
        vmem((pairs, *tile), BF16),
        vmem(tile, F32),
        dma((2,)), dma((length_y, 2)), dma((length_z, 2)), dma((length_y, 2)), dma((2,)),
        dma((2, 2)),
        vmem((rows, channels), BF16),
        vmem((blocks, STATE, 2 * channels), BF16),
        vmem((2, blocks, BLOCK, part // 2), BF16),
        vmem((2, blocks, BLOCK, part // 2), BF16),
        vmem((2, blocks, BLOCK, part), BF16),
        vmem((2, blocks, BLOCK, part), BF16),
        dma((2, blocks, 2)), dma((2, blocks, 2)),
    ]
    return pl.pallas_call(
        functools.partial(layer_kernel, (length_z, length_y)),
        in_specs=[hbm] * (1 + len(smalls) + len(shards)) + [pl.BlockSpec(memory_space=pltpu.SMEM)],
        out_specs=[pl.BlockSpec(memory_space=pltpu.VMEM)] * 2,
        out_shape=[
            jax.ShapeDtypeStruct((rows, part), BF16),
            jax.ShapeDtypeStruct((HEADS, rows), F32),
        ],
        scratch_shapes=scratch,
        compiler_params=pltpu.CompilerParams(
            collective_id=1, has_side_effects=True, vmem_limit_bytes=65_800_000
        ),
        cost_estimate=pl.CostEstimate(flops=1 << 33, bytes_accessed=24 << 20, transcendentals=0),
        name="layer",
    )(tokens, *smalls, *shards, sinks)


def flatten_rows(weight):
    return weight.reshape(weight.shape[0], -1)


def shards(
    tokens, input_gain, gate_weight, value_weight, inflow_weight, readout_weight, step_weight,
    conv_values, conv_inflow, conv_readout, log_rate, group_gain, query_weight, key_weight,
    vector_weight, sink_logit, state_out, window_out,
):
    count = tokens.shape[0]
    length_z, length_y = lax.axis_size(SP[0]), lax.axis_size(SP[1])
    quarter = HEAD_DIM // 4
    powers = (np.arange(128) % quarter).astype(np.float32) / np.float32(quarter)
    freqs = np.broadcast_to(np.float32(ROPE_BASE) ** -powers, (8, 128)).astype(np.float32)
    freqs = jnp.asarray(freqs)
    smalls = (
        input_gain.reshape(-1, 128),
        step_weight.transpose(1, 2, 0).reshape(2 * HEADS, -1),
        conv_values, flatten_rows(conv_inflow), flatten_rows(conv_readout),
        log_rate.transpose(0, 2, 1).reshape(2 * HEADS, count),
        freqs,
        group_gain.reshape(-1, 128),
    )
    shards_here = (
        value_weight, flatten_rows(inflow_weight), flatten_rows(readout_weight), key_weight,
        vector_weight, gate_weight, query_weight, state_out.T, window_out.T,
    )
    mixed, logs = layer(
        length_z, length_y, lax.axis_size("tp"), tokens, smalls, shards_here, sink_logit
    )
    return mixed, logs.T


def solution(mesh):
    torus = Mesh(mesh.devices.reshape(8, 4, 2, mesh.shape["tp"]), (*SP, "tp"))
    return jax.shard_map(
        shards,
        mesh=torus,
        in_specs=(
            P(SP, None), P(), P(SP, "tp"), P(SP, "tp"), P(SP, "tp", None), P(SP, "tp", None),
            P(SP, None, "tp"), P(None, "tp"), P(None, "tp", None), P(None, "tp", None),
            P(None, SP, "tp"), P("tp"), P(SP, "tp"), P(SP, "tp"), P(SP, "tp"), P("tp"),
            P("tp", SP), P("tp", SP),
        ),
        out_specs=(P(SP, "tp"), P(SP, "tp")),
        check_vma=False,
    )
```

```python
import functools
import heapq

import jax
import jax.numpy as jnp
import numpy as np
from jax import lax
from jax.experimental import pallas as pl
from jax.experimental.pallas import tpu as pltpu
from jax.sharding import Mesh
from jax.sharding import PartitionSpec as P

HEAD_DIM = 64
STATE = 128
HEADS = 8
BLOCK = 128
WINDOW = 128
GRID_W = 64
HALO = 16
SP = ("sp_0", "sp_1", "sp_2")
EPS = 1e-06
ROPE_BASE = 10000.0
F32 = jnp.float32
BF16 = jnp.bfloat16
MSG = STATE + 16
KV_AT = 768
Q_AT = 1024
OUT_AT = 512


def dot(a, b, dims=((1,), (0,)), precision=None):
    return lax.dot_general(
        a, b, (dims, ((), ())), preferred_element_type=F32, precision=precision
    )


def split_bf16(value, parts):
    pieces = []
    for _ in range(parts):
        piece = value.astype(BF16)
        pieces.append(piece)
        value = value - piece.astype(F32)
    return pieces


def spread(value, spread_matrix, parts):
    pieces = [p.astype(F32) for p in split_bf16(value, parts)]
    joined = jnp.concatenate(pieces, axis=1).astype(BF16)
    matrix = jnp.concatenate([spread_matrix] * parts, axis=0)
    return dot(joined, matrix)


def as_row(ref):
    wide = ref[...].astype(F32)
    return jnp.concatenate([wide[i : i + 1, :] for i in range(wide.shape[0])], axis=1)


def spread_matrix():
    shape = (2 * HEADS, 2 * HEADS * HEAD_DIM)
    rows = lax.broadcasted_iota(jnp.int32, shape, 0)
    first = lax.broadcasted_iota(jnp.int32, shape, 1) - rows * HEAD_DIM
    return jnp.where((first >= 0) & (first < HEAD_DIM), 1.0, 0.0).astype(BF16)


def conv_state(
    traffic_service, cin_ref, taps_x_ref, taps_b_ref, taps_c_ref, step_ref, rate_ref,
    conv_ref, col_ref, row_ref, piece_ref, etot_ref, msg_ref, win,
):
    count = cin_ref.shape[0] - 2 * HALO
    blocks = count // BLOCK
    channels = HEADS * HEAD_DIM
    spread_m = spread_matrix()
    taps = jnp.concatenate([t[...].astype(F32) for t in (taps_x_ref, taps_b_ref, taps_c_ref)], axis=1)
    lane16 = lax.broadcasted_iota(jnp.int32, (BLOCK, 2 * HEADS), 1)
    forward16 = lane16 < HEADS
    tri = (
        lax.broadcasted_iota(jnp.int32, (BLOCK, BLOCK), 0)
        >= lax.broadcasted_iota(jnp.int32, (BLOCK, BLOCK), 1)
    ).astype(F32)
    win[pl.ds(0, HALO), :] = cin_ref[pl.ds(count, HALO), :].astype(F32)
    win[pl.ds(HALO + count, HALO), :] = cin_ref[pl.ds(count + HALO, HALO), :].astype(F32)

    def fill(i, carry):
        start = pl.multiple_of(i * BLOCK, BLOCK)
        win[pl.ds(HALO + start, BLOCK), :] = cin_ref[pl.ds(start, BLOCK), :].astype(F32)
        return carry

    lax.fori_loop(0, blocks, fill, 0)
    traffic_service(0.5)

    def some(which):
        spans = [slice(i * BLOCK, (i + 1) * BLOCK) for i in which]
        steps, decays, convs = [], [], []
        for rows in spans:
            raw = step_ref[rows, 0 : 2 * HEADS]
            steps.append(jnp.maximum(raw, 0.0) + jnp.log1p(jnp.exp(-jnp.abs(raw))))
            rate = jnp.concatenate(
                [rate_ref[:, rows], jnp.zeros((BLOCK - 2 * HEADS, BLOCK), F32)], axis=0
            )
            decays.append(-jnp.exp(rate.T[:, 0 : 2 * HEADS]) * steps[-1])
        cums = [dot(tri, decay, precision=lax.Precision.HIGHEST) for decay in decays]
        tots = [cum[BLOCK - 1 : BLOCK, :] for cum in cums]
        cols = [jnp.where(forward16, cum, cum - decay) for cum, decay in zip(cums, decays)]
        weights = [
            jnp.exp(jnp.where(forward16, tot - col, col)) * step
            for tot, col, step in zip(tots, cols, steps)
        ]
        wides = [spread(weight, spread_m, 2) for weight in weights]
        etots = [spread(jnp.exp(jnp.broadcast_to(tot, (8, 2 * HEADS))), spread_m, 3) for tot in tots]
        rests = jnp.zeros((BLOCK, 128 - 4 * HEADS), F32)
        turned = [jnp.concatenate([col, step, rests], axis=1).T for col, step in zip(cols, steps)]
        for rows in spans:
            acc = 0.0
            for tap in range(5):
                first = rows.start + HALO - 2 + tap
                acc = acc + win[first : first + BLOCK, :] * taps[tap : tap + 1, :]
            convs.append((acc * jax.nn.sigmoid(acc)).astype(BF16))
        pieces = []
        for conv, wide in zip(convs, wides):
            xs = conv[:, 0:channels].astype(F32)
            scaled = (jnp.concatenate([xs, xs], axis=1) * wide).astype(BF16)
            pieces.append(dot(conv[:, channels : channels + STATE], scaled, ((0,), (0,))))
        for n, (i, rows) in enumerate(zip(which, spans)):
            conv_ref[rows, :] = convs[n]
            col_ref[rows, 0 : 2 * HEADS] = cols[n]
            col_ref[rows, 2 * HEADS : 4 * HEADS] = jnp.broadcast_to(tots[n], (BLOCK, 2 * HEADS))
            row_ref[i] = turned[n][0 : 4 * HEADS, :]
            piece_ref[i] = pieces[n]
            etot_ref[i] = etots[n]
        return sum(tots)

    total = jnp.zeros((1, 2 * HEADS), F32)
    for i in range(0, blocks, 2):
        total = total + some((i, i + 1))
        traffic_service(1.6)
    forward = piece_ref[0, :, 0:channels]
    backward = piece_ref[blocks - 1, :, channels : 2 * channels]
    for i in range(1, blocks):
        forward = etot_ref[i, 0:1, 0:channels] * forward + piece_ref[i, :, 0:channels]
        k = blocks - 1 - i
        backward = (
            etot_ref[k, 0:1, channels : 2 * channels] * backward
            + piece_ref[k, :, channels : 2 * channels]
        )
    spread_total = spread(jnp.broadcast_to(total, (16, 2 * HEADS)), spread_m, 3)
    hi, mid, lo = split_bf16(spread_total, 3)
    which = lax.broadcasted_iota(jnp.int32, (16, 2 * channels), 0)
    tail = jnp.where(
        which == 0, hi.astype(F32), jnp.where(which == 1, mid.astype(F32), lo.astype(F32))
    ).astype(BF16)
    for e, state in enumerate((forward, backward)):
        for pair in range(channels // 128):
            lanes = slice(pair * 128, pair * 128 + 128)
            msg_ref[e, pair, 0:STATE, :] = state[:, lanes].astype(BF16)
            msg_ref[e, pair, STATE:MSG, :] = tail[:, e * channels + pair * 128 : e * channels + pair * 128 + 128]


def mixer(conv_ref, col_ref, row_ref, piece_ref, etot_ref, in_ref, gate_ref, gain_ref, out_ref, held):
    count = conv_ref.shape[0]
    blocks = count // BLOCK
    channels = HEADS * HEAD_DIM
    spread_m = spread_matrix()
    gain = as_row(gain_ref)
    for e in range(2):
        state = jnp.concatenate(
            [in_ref[e, p].astype(F32) for p in range(channels // 128)], axis=1
        )
        lanes = slice(e * channels, (e + 1) * channels)
        for i in range(blocks) if e == 0 else reversed(range(blocks)):
            held[i, :, lanes] = state.astype(BF16)
            state = etot_ref[i, 0:1, lanes] * state + piece_ref[i, :, lanes]
    row_at = lax.broadcasted_iota(jnp.int32, (BLOCK, BLOCK), 0)
    col_at = lax.broadcasted_iota(jnp.int32, (BLOCK, BLOCK), 1)
    lower = row_at >= col_at
    diagonal = row_at == col_at
    first_half = col_at < HEAD_DIM
    forward16 = lax.broadcasted_iota(jnp.int32, (BLOCK, 2 * HEADS), 1) < HEADS

    def one(i):
        rows = pl.ds(pl.multiple_of(i * BLOCK, BLOCK), BLOCK)
        inflow = conv_ref[rows, channels : channels + STATE]
        readout = conv_ref[rows, channels + STATE : channels + 2 * STATE]
        inner = dot(readout, inflow, ((1,), (1,)))
        col = col_ref[rows, 0 : 2 * HEADS]
        tot = col_ref[rows, 2 * HEADS : 4 * HEADS]
        reach = spread(jnp.exp(jnp.where(forward16, col, tot - col)), spread_m, 2)
        far = dot(readout, held[i]) * reach
        parts = []
        for pair in range(HEADS // 2):
            weights = []
            for h in (2 * pair, 2 * pair + 1):
                b = HEADS + h
                arg = jnp.where(
                    lower,
                    col[:, h : h + 1] - row_ref[i, h : h + 1, :],
                    row_ref[i, b : b + 1, :] - col[:, b : b + 1],
                )
                step_f = row_ref[i, 2 * HEADS + h : 2 * HEADS + h + 1, :]
                step_b = row_ref[i, 2 * HEADS + b : 2 * HEADS + b + 1, :]
                step = jnp.where(lower, step_f, step_b) + jnp.where(diagonal, step_b, 0.0)
                weights.append((inner * jnp.exp(arg) * step).astype(BF16))
            xs = conv_ref[rows, pair * 128 : pair * 128 + 128]
            zero = jnp.zeros_like(xs)
            stacked = jnp.concatenate(
                [jnp.where(first_half, xs, zero), jnp.where(first_half, zero, xs)], axis=0
            )
            parts.append(dot(jnp.concatenate(weights, axis=1), stacked))
        y = jnp.concatenate(parts, axis=1) + far[:, 0:channels] + far[:, channels:]
        gate = gate_ref[rows, :].astype(F32)
        y = y * (gate * jax.nn.sigmoid(gate))
        y = y * lax.rsqrt(jnp.mean(y * y, axis=1, keepdims=True) + EPS)
        out_ref[rows, :] = (y * gain).astype(BF16)

    return one


def attention(
    count, q_ref, kv_ref, before_ref, after_ref, freq_ref, sink_ref,
    out_ref, log_ref, keys, values, by_row, by_col,
):
    blocks = count // BLOCK
    place = lax.axis_index(SP)
    lane = lax.broadcasted_iota(jnp.int32, (BLOCK, 128), 1)
    low_quarter = lane % 32 < 16
    first_half = lane < HEAD_DIM
    row_lane = (lane % HEAD_DIM < 32)[0:GRID_W]

    grid_rows = by_row.shape[1]
    first_row = place * (count // GRID_W) - WINDOW // GRID_W
    sign = jnp.where(low_quarter, -1.0, 1.0)
    for ref, first, length in ((by_row, first_row, grid_rows), (by_col, 0, GRID_W)):
        at = lax.broadcasted_iota(jnp.int32, (length, 128), 0) + first
        angle = at.astype(F32) * freq_ref[0:1, :]
        ref[0] = jnp.cos(angle)
        ref[1] = jnp.sin(angle) * sign[0:length]

    def tables(slot):
        out = []
        for kind in range(2):
            parts = []
            for r in range(BLOCK // GRID_W):
                row = by_row[kind, pl.ds(slot * (BLOCK // GRID_W) + r, 1), :]
                parts.append(jnp.where(row_lane, row, by_col[kind]))
            out.append(jnp.concatenate(parts, axis=0))
        return out

    def turn(value, table):
        wide = value.astype(F32)
        other = jnp.where(low_quarter, pltpu.roll(wide, 112, 1), pltpu.roll(wide, 16, 1))
        return (wide * table[0] + other * table[1]).astype(BF16)

    def store(raw, slot):
        rows = pl.ds(pl.multiple_of(slot * BLOCK, BLOCK), BLOCK)
        key = turn(raw[:, 0:128], tables(slot)).astype(F32)
        swapped = pltpu.roll(key, 64, 1)
        keys[0, rows, :] = jnp.where(first_half, key, swapped).astype(BF16)
        keys[1, rows, :] = jnp.where(first_half, swapped, key).astype(BF16)
        values[:, rows] = raw[:, 128:256].astype(F32).T.astype(BF16)

    def own_keys():
        def fill(i, carry):
            rows = pl.ds(pl.multiple_of(i * BLOCK, BLOCK), BLOCK)
            store(kv_ref[rows, :], i + 1)
            return carry

        lax.fori_loop(0, blocks, fill, 0)

    def edge_keys():
        store(before_ref[...], 0)
        store(after_ref[...], blocks + 1)

    key_at = lax.broadcasted_iota(jnp.int32, (3 * BLOCK, 2 * BLOCK), 0)
    query_at = lax.broadcasted_iota(jnp.int32, (3 * BLOCK, 2 * BLOCK), 1) % BLOCK
    in_band = (key_at >= query_at) & (key_at <= query_at + 2 * WINDOW)
    first_row_half = lax.broadcasted_iota(jnp.int32, (1, 2 * BLOCK), 1) < BLOCK
    start_at = -place * count
    end_at = start_at + count * lax.axis_size(SP)

    def one(i):
        start = pl.multiple_of(i * BLOCK, BLOCK)
        rows = pl.ds(start, BLOCK)
        here = key_at + (start - WINDOW)
        valid = in_band & (here >= start_at) & (here < end_at)
        table = tables(i + 1)
        band = pl.ds(start, 3 * BLOCK)
        qs = []
        for pair in range(HEADS // 2):
            lanes = slice(pair * 128, pair * 128 + 128)
            q = (turn(q_ref[rows, lanes], table).astype(F32) * HEAD_DIM ** (-0.5)).astype(BF16)
            zero = jnp.zeros_like(q)
            qs.append(jnp.concatenate(
                [jnp.where(first_half, q, zero), jnp.where(first_half, zero, q)], axis=0
            ))
        scores = [dot(keys[pair // 2, band, :], q, ((1,), (1,))) for pair, q in enumerate(qs)]
        outs = []
        for pair in range(HEADS // 2):
            group = pair // 2
            mine = jnp.where(valid, scores[pair], -1e30)
            sink = jnp.where(first_row_half, sink_ref[2 * pair], sink_ref[2 * pair + 1])
            top = jnp.maximum(jnp.max(mine, axis=0, keepdims=True), sink)
            expo = jnp.exp(mine - top)
            total = jnp.sum(expo, axis=0, keepdims=True) + jnp.exp(sink - top)
            value = values[group * HEAD_DIM : (group + 1) * HEAD_DIM, band]
            outs.append(dot(value, expo.astype(BF16)) / total)
            log = top + jnp.log(total)
            log_ref[2 * pair : 2 * pair + 1, rows] = log[:, 0:BLOCK]
            log_ref[2 * pair + 1 : 2 * pair + 2, rows] = log[:, BLOCK:]
        for pair, o in enumerate(outs):
            turned = jnp.concatenate([o[:, 0:BLOCK], o[:, BLOCK:]], axis=0).T
            out_ref[rows, pair * 128 : pair * 128 + 128] = turned.astype(BF16)

    return own_keys, edge_keys, one


LINKS = ("z+", "z-", "y+", "y-")
EARLY = 1664
LATE = 1536
ROUTES = (
    (("A", 0, 0, 1024, 512, "z"), ("B", 0, 1024, 640, 384, "y")),
    (("C", 1, 0, 896, 512, "z"), ("D", 1, 896, 640, 384, "y")),
)
RATE = 46.6e3
HOP = 1.9


def ring(route, axis, other, length):
    name, array, column, total, cut, _ = route
    out = []
    for sign in (1, -1):
        previous = None
        for step in range(length // 2):
            cols = (column, total)
            if step == length // 2 - 1:
                cols = (column, cut) if sign == 1 else (column + cut, total - cut)
            key = (name, axis, other, sign, step)
            out.append(dict(
                key=key, route=name, array=array, axis=axis, sign=sign, along=-sign * step,
                other=other, cols=cols, needs=[previous] if previous else [],
            ))
            previous = key
    return out


def transfers(routes, lengths):
    sends, groups = [], {}
    for route in routes:
        name, _, _, _, _, first = route
        second = "y" if first == "z" else "z"
        length = lengths[first]
        sends += ring(route, first, 0, length)
        for offset in range(-(length // 2) + 1, length // 2 + 1):
            one = ring(route, second, offset, lengths[second])
            needs = []
            if offset == length // 2:
                needs = [(name, first, 0, sign, length // 2 - 1) for sign in (1, -1)]
            elif offset:
                needs = [(name, first, 0, -1 if offset > 0 else 1, abs(offset) - 1)]
            for s in one:
                s["needs"] = s["needs"] or needs
            sends += one
            groups[(name, offset)] = {s["key"] for s in one}
    return sends, groups


class Flow:
    def __init__(self, number, lengths, arrays, sems):
        self.routes = ROUTES[number]
        self.lengths = lengths
        self.arrays = arrays
        self.send_sem, self.recv_sem, self.core_send, self.core_recv = sems
        self.at = dict(zip("zy", (lax.axis_index(SP[0]), lax.axis_index(SP[1]))))
        self.c = lax.axis_index(SP[2])
        self.sends, self.groups = transfers(self.routes, lengths)
        self.number = {s["key"]: i for i, s in enumerate(self.sends)}
        self.by_key = {s["key"]: s for s in self.sends}
        self.group_keys = list(self.groups)
        self.left = {s["key"]: len(s["needs"]) for s in self.sends}
        self.followers = {}
        for s in self.sends:
            for need in s["needs"]:
                self.followers.setdefault(need, []).append(s)
        self.first_axis = {route[0]: route[5] for route in self.routes}
        self.free = dict.fromkeys(LINKS, 0.0)
        self.heap = []
        self.clock = 0.0
        self.started = []

    def wrap(self, axis, shift):
        length = self.lengths[axis]
        return lax.rem(self.at[axis] + shift + length, length)

    def rank(self, s):
        return (s["axis"] != self.first_axis[s["route"]], s["route"])

    def copy_of(self, s, shift):
        along = s["along"] - shift * s["sign"]
        place = {s["axis"]: along, "y" if s["axis"] == "z" else "z": s["other"]}
        ref = self.arrays[s["array"]].at[
            self.wrap("z", place["z"]), self.wrap("y", place["y"]), self.c, :, pl.ds(*s["cols"])
        ]
        i = self.number[s["key"]]
        to = {SP["zy".index(s["axis"])]: self.wrap(s["axis"], s["sign"])}
        return pltpu.make_async_remote_copy(
            src_ref=ref, dst_ref=ref, send_sem=self.send_sem.at[i], recv_sem=self.recv_sem.at[i],
            device_id=to, device_id_type=pl.DeviceIdType.MESH,
        )

    def core_copy(self, key, c):
        name, offset = key
        i = self.group_keys.index(key)
        route = [r for r in self.routes if r[0] == name][0]
        ref = self.arrays[route[1]]
        cols = pl.ds(route[2], route[3])
        if route[5] == "z":
            ref = ref.at[self.wrap("z", offset), :, c, :, cols]
        else:
            ref = ref.at[:, self.wrap("y", offset), c, :, cols]
        return pltpu.make_async_remote_copy(
            src_ref=ref, dst_ref=ref, send_sem=self.core_send.at[i],
            recv_sem=self.core_recv.at[i], device_id={SP[2]: 1 - self.c},
            device_id_type=pl.DeviceIdType.MESH,
        )

    def launch(self, s):
        copy = self.copy_of(s, 0)
        copy.start()
        self.started.append(copy)
        link = s["axis"] + ("+" if s["sign"] == 1 else "-")
        self.free[link] = max(self.free[link], self.clock) + 64 * s["cols"][1] / RATE
        heapq.heappush(self.heap, (self.free[link] + HOP, len(self.started), s["key"]))

    def begin(self):
        for s in sorted((s for s in self.sends if not s["needs"]), key=self.rank):
            self.launch(s)

    def handle(self):
        _, _, key = heapq.heappop(self.heap)
        self.copy_of(self.by_key[key], 1).wait_recv()
        for s in sorted(self.followers.get(key, []), key=self.rank):
            self.left[s["key"]] -= 1
            if self.left[s["key"]] == 0:
                self.launch(s)
        for group, keys in self.groups.items():
            if key in keys:
                keys.remove(key)
                if not keys:
                    copy = self.core_copy(group, self.c)
                    copy.start()
                    self.started.append(copy)

    def service(self, passed):
        self.clock += passed
        while self.heap and self.heap[0][0] <= self.clock:
            self.handle()

    def drain(self):
        while self.heap:
            self.clock = max(self.clock, self.heap[0][0])
            self.handle()
        for group in self.group_keys:
            self.core_copy(group, 1 - self.c).wait_recv()

    def finish(self):
        for copy in self.started:
            copy.wait_send()


def gather(
    early, late, small_copies, enter, tok_ref, gain_ref, step_ref, value_ref, inflow_ref,
    readout_ref, key_ref, vector_ref, gate_ref, query_ref, state_ref, window_ref,
    normed, before, after, held, edge_sem, own_sem,
):
    z, y, c = (lax.axis_index(a) for a in SP)
    length_z, length_y = early.lengths["z"], early.lengths["y"]
    flat = (z * length_y + y) * 2 + c
    count = length_z * length_y * 2
    count_rows = tok_ref.shape[0]
    a_ref, b_ref = early.arrays

    def device_at(index):
        index = lax.rem(index + count, count)
        return {
            SP[0]: index // (2 * length_y),
            SP[1]: lax.rem(index // 2, length_y),
            SP[2]: lax.rem(index, 2),
        }

    moves = []
    for array, refs in (
        (a_ref, (value_ref, inflow_ref, readout_ref, key_ref, vector_ref, query_ref)),
        (b_ref, (gate_ref, state_ref, window_ref)),
    ):
        column = 0
        for ref in refs:
            width = ref.shape[1]
            moves.append((ref, array.at[z, y, c, :, pl.ds(column, width)]))
            column += width
    moves.append((tok_ref, held))
    moves = [pltpu.make_async_copy(*move, own_sem.at[i]) for i, move in enumerate(moves)]
    for move in moves:
        move.start()
    small_copies()
    step = step_ref[...].astype(F32)
    rows, cols = step.shape
    step = jnp.concatenate([step, jnp.zeros((rows, 128 - cols), F32)], axis=1)
    step = jnp.concatenate([step, jnp.zeros((128 - rows, 128), F32)], axis=0)
    a_ref[z, y, c, :, EARLY - 128 : EARLY] = step.T[0:cols, :].astype(BF16)
    for move in moves[:6]:
        move.wait()
    enter()
    edge_copies = []
    for k, (index, dst) in enumerate(((flat - 1, after), (flat + 1, before))):
        edge_copies.append(pltpu.make_async_remote_copy(
            src_ref=tok_ref.at[pl.ds(k * (count_rows - HALO), HALO)], dst_ref=dst,
            send_sem=edge_sem.at[k, 0], recv_sem=edge_sem.at[k, 1],
            device_id=device_at(index), device_id_type=pl.DeviceIdType.MESH,
        ))
    gain = as_row(gain_ref)

    def norm(value):
        wide = value.astype(F32)
        scale = lax.rsqrt(jnp.mean(wide * wide, axis=1, keepdims=True) + EPS)
        return wide * scale * gain

    def norm_blocks(first, last):
        def norm_block(i, carry):
            rows = pl.ds(pl.multiple_of(i * BLOCK, BLOCK), BLOCK)
            normed[rows, :] = norm(held[rows, :]).astype(BF16)
            return carry

        lax.fori_loop(first, last, norm_block, 0)

    early.begin()
    for copy in edge_copies:
        copy.start()
    for move in moves[6:]:
        move.wait()
    blocks = count_rows // BLOCK
    norm_blocks(0, blocks // 2)
    early.service(4.5)
    norm_blocks(blocks // 2, blocks)
    early.service(2.0)
    for copy in edge_copies:
        copy.wait()
    normed[count_rows : count_rows + HALO, :] = jnp.where(flat > 0, norm(before[...]), 0.0).astype(BF16)
    normed[count_rows + HALO : count_rows + 2 * HALO, :] = jnp.where(
        flat < count - 1, norm(after[...]), 0.0
    ).astype(BF16)
    early.service(1.0)
    while sum(early.left.values()) > 0:
        early.clock = max(early.clock, early.heap[0][0])
        early.handle()
    late.clock = early.clock
    late.free = dict(early.free)
    late.begin()
    early.drain()
    late.service(max(early.clock - late.clock, 0.0))


def middle(
    late, normed, a_ref, b_ref, taps_x_ref, taps_b_ref, taps_c_ref, rate_ref, freq_ref, sink_ref,
    out_ref, window_ref, log_ref, gate_ref, conv_ref, col_ref, row_ref, piece_ref, etot_ref,
    cin_ref, kv_ref, q_ref, step_ref, win, near, msg_ref,
    kv_before_ref, kv_after_ref, keys, values, by_row, by_col, part, turned, by_y, summed, by_z,
    back, arrived, nxt, final, carry,
    part_sem, y_sem, z_sem, back_sem, final_sem, kv_sem,
):
    rows = kv_ref.shape[0]
    z, y, c = (lax.axis_index(a) for a in SP)
    length_z, length_y = lax.axis_size(SP[0]), lax.axis_size(SP[1])
    forward = c == 0
    other = 1 - c
    order_z = jnp.where(forward, z, length_z - 1 - z)
    mesh_id = pl.DeviceIdType.MESH
    flat = (z * length_y + y) * 2 + c
    count = length_z * length_y * 2

    def device_at(index):
        index = lax.rem(index + count, count)
        return {
            SP[0]: index // (2 * length_y),
            SP[1]: lax.rem(index // 2, length_y),
            SP[2]: lax.rem(index, 2),
        }

    def project(dst, count, tiles, source, first):
        tile = 256

        def column(j, carry_over):
            cols = pl.ds(pl.multiple_of(j * tile, tile), tile)
            from_cols = pl.ds(pl.multiple_of(first + j * tile, 128), tile)
            dst[:, cols] = dot(normed[0:count, :], source[:, from_cols]).astype(BF16)
            return carry_over

        lax.fori_loop(0, tiles, column, 0)

    project(kv_ref, rows, 1, a_ref, KV_AT)
    late.service(1.1)

    def send(src, dst, sems, peer):
        copy = pltpu.make_async_remote_copy(
            src_ref=src, dst_ref=dst, send_sem=sems.at[0], recv_sem=sems.at[1],
            device_id=peer, device_id_type=mesh_id,
        )
        copy.start()
        return copy

    def state_of(ref, *at):
        return ref[(*at, slice(0, STATE), slice(None))].astype(F32)

    def decay_of(ref, *at):
        tail = ref[(*at, slice(STATE, MSG), slice(None))].astype(F32)
        return tail[0:1] + tail[1:2] + tail[2:3]

    def put(ref, state, decay, *at):
        ref[(*at, slice(0, STATE), slice(None))] = state.astype(BF16)
        hi, mid, lo = (p.astype(F32) for p in split_bf16(decay, 3))
        which = lax.broadcasted_iota(jnp.int32, (MSG - STATE, 128), 0)
        tail = jnp.where(which == 0, hi, jnp.where(which == 1, mid, lo))
        ref[(*at, slice(STATE, MSG), slice(None))] = tail.astype(BF16)

    pairs = msg_ref.shape[1]
    kv_copies = [
        send(
            kv_ref.at[pl.ds(rows - WINDOW, WINDOW)], kv_before_ref, kv_sem.at[0],
            device_at(flat + 1),
        ),
        send(kv_ref.at[pl.ds(0, WINDOW)], kv_after_ref, kv_sem.at[1], device_at(flat - 1)),
    ]
    project(cin_ref.at[:, pl.ds(0, 256)], rows + 2 * HALO, 1, a_ref, 0)
    late.service(1.1)
    project(cin_ref.at[:, pl.ds(256, 512)], rows + 2 * HALO, 2, a_ref, 256)
    step_ref[...] = dot(normed[0:rows, :], a_ref[:, EARLY - 128 : EARLY])
    late.service(2.8)
    conv_state(
        late.service,
        cin_ref, taps_x_ref, taps_b_ref, taps_c_ref, step_ref, rate_ref,
        conv_ref, col_ref, row_ref, piece_ref, etot_ref, msg_ref, win,
    )
    copy = send(msg_ref.at[other], part, part_sem, {SP[2]: other})
    own_keys, edge_keys, attend = attention(
        rows, q_ref, kv_ref, kv_before_ref, kv_after_ref, freq_ref, sink_ref,
        window_ref, log_ref, keys, values, by_row, by_col,
    )

    blocks = rows // BLOCK
    own_keys()
    late.service(1.2)
    copy.wait()
    for j in range(pairs):
        decay = decay_of(part, j)
        put(
            turned,
            jnp.exp(decay) * state_of(msg_ref, c, j) + state_of(part, j),
            decay + decay_of(msg_ref, c, j),
            j,
        )
    copies = []
    for k in range(1, length_y):
        to = lax.rem(y + k, length_y)
        copies.append(send(turned.at[to], by_y.at[k], y_sem.at[k], {SP[1]: to}))
    by_y[0] = turned[y]
    project(q_ref, rows, 2, a_ref, Q_AT)
    late.service(2.4)
    attend(1)
    late.service(1.4)
    for copy in copies:
        copy.wait()
    before = []
    state = jnp.zeros((STATE, 128), F32)
    decay = jnp.zeros((1, 128), F32)
    for q in range(length_y):
        before.append((state, decay))
        slot = jnp.where(forward, lax.rem(y - q + length_y, length_y), lax.rem(y + 1 + q, length_y))
        step = decay_of(by_y, slot)
        state = jnp.exp(step) * state + state_of(by_y, slot)
        decay = decay + step
    put(summed, state, decay)
    for k in range(1, length_z):
        to = lax.rem(z + k, length_z)

        @pl.when((z + k >= length_z) == (c == 1))
        def _():
            send(summed, by_z.at[k], z_sem.at[k], {SP[0]: to})

    carry[...] = jnp.zeros_like(carry)
    for i in range(2, blocks - 1):
        attend(i)
        late.service(1.5)
    for distance in reversed(range(1, length_z)):
        slot = jnp.where(forward, distance, length_z - distance)

        @pl.when(order_z >= distance)
        def _():
            pltpu.make_async_remote_copy(
                src_ref=summed, dst_ref=by_z.at[slot], send_sem=z_sem.at[slot, 0],
                recv_sem=z_sem.at[slot, 1], device_id={SP[0]: z}, device_id_type=mesh_id,
            ).wait_recv()
            carry[...] = jnp.exp(decay_of(by_z, slot)) * carry[...] + state_of(by_z, slot)

    for k in range(1, length_z):
        to = lax.rem(z + k, length_z)

        @pl.when((z + k >= length_z) == (c == 1))
        def _():
            pltpu.make_async_remote_copy(
                src_ref=summed, dst_ref=by_z.at[k], send_sem=z_sem.at[k, 0],
                recv_sem=z_sem.at[k, 1], device_id={SP[0]: to}, device_id_type=mesh_id,
            ).wait_send()

    incoming = carry[...]
    for q in range(length_y):
        to = jnp.where(forward, q, length_y - 1 - q)
        state, decay = before[q]
        back[to] = (jnp.exp(decay) * incoming + state).astype(BF16)
    copies = []
    for k in range(1, length_y):
        to = lax.rem(y + k, length_y)
        copies.append(send(back.at[to], arrived.at[k], back_sem.at[k], {SP[1]: to}))
    arrived[0] = back[y]
    for copy in kv_copies:
        copy.wait()
    edge_keys()
    attend(0)
    late.service(1.7)
    for copy in copies:
        copy.wait()
    for j in range(pairs):
        state = arrived[lax.rem(y - j + length_y, length_y)]
        out_ref[c, j] = state
        nxt[j] = (
            jnp.exp(decay_of(msg_ref, c, j)) * state.astype(F32) + state_of(msg_ref, c, j)
        ).astype(BF16)
    copy = send(nxt, final, final_sem, {SP[2]: other})
    attend(blocks - 1)
    late.service(1.5)
    late.drain()
    project(gate_ref, rows, 2, b_ref, 0)
    copy.wait()
    out_ref[other] = final[...]


def finish(
    window_ref, w_ref, conv_ref, col_ref, row_ref, piece_ref, etot_ref, in_ref, gate_ref, gain_ref,
    out_ref, *refs
):
    state_ref, held, far_out, far_in, near_out, near_in, far_sem, near_sem = refs
    n = lax.axis_size("tp")
    me = lax.axis_index("tp")
    mesh_id = pl.DeviceIdType.MESH
    sides = (1, -1)
    count, channels = state_ref.shape
    mix = mixer(
        conv_ref, col_ref, row_ref, piece_ref, etot_ref, in_ref, gate_ref, gain_ref, state_ref, held
    )
    width = w_ref.shape[0] // n
    half = width // 2
    chunk = far_out.shape[2]
    chunks = count // chunk

    def at(step):
        return lax.rem(me + step + n, n)

    def terms(rows, to):
        outs = pl.ds(pl.multiple_of(to * width, width), width)
        return dot(state_ref[rows, :], w_ref[outs, OUT_AT : OUT_AT + channels], ((1,), (1,))) + dot(
            window_ref[rows, :], w_ref[outs, OUT_AT + channels : OUT_AT + 2 * channels], ((1,), (1,))
        )

    def far_copy(i, k):
        return pltpu.make_async_remote_copy(
            src_ref=far_out.at[k, i], dst_ref=far_in.at[k, i], send_sem=far_sem.at[k, i, 0],
            recv_sem=far_sem.at[k, i, 1], device_id={"tp": at(sides[k])}, device_id_type=mesh_id,
        )

    def near_copy(i, k):
        return pltpu.make_async_remote_copy(
            src_ref=near_out.at[k, i], dst_ref=near_in.at[k, i], send_sem=near_sem.at[k, i, 0],
            recv_sem=near_sem.at[k, i, 1], device_id={"tp": at(sides[k])}, device_id_type=mesh_id,
        )

    def send_far(i, carry):
        rows = pl.ds(pl.multiple_of(i * chunk, chunk), chunk)
        value = terms(rows, at(2)).astype(BF16)
        for k in range(2):
            far_out[k, i] = value[:, k * half : (k + 1) * half]
            far_copy(i, k).start()

        @pl.when(i + 1 < chunks)
        def _():
            mix(i + 1)

        return carry

    mix(0)
    lax.fori_loop(0, chunks, send_far, 0)

    def send_near(i, carry):
        rows = pl.ds(pl.multiple_of(i * chunk, chunk), chunk)
        for k in range(2):
            value = terms(rows, at(sides[k])).astype(BF16).astype(F32)
            lanes = slice(k * half, (k + 1) * half)
            far_copy(i, k).wait_recv()
            near_out[k, i] = value.astype(BF16)
            near_out[k, i, :, lanes] = (value[:, lanes] + far_in[k, i].astype(F32)).astype(BF16)
            near_copy(i, k).start()
        return carry

    lax.fori_loop(0, chunks, send_near, 0)

    def collect(i, carry):
        rows = pl.ds(pl.multiple_of(i * chunk, chunk), chunk)
        value = terms(rows, me).astype(BF16).astype(F32)
        for k in range(2):
            near_copy(i, k).wait_recv()
            value = value + near_in[k, i].astype(F32)
        out_ref[rows, :] = value.astype(BF16)
        for k in range(2):
            far_copy(i, k).wait_send()
            near_copy(i, k).wait_send()
        return carry

    lax.fori_loop(0, chunks, collect, 0)


def layer_kernel(
    lengths, tok_ref, *refs
):
    length_z, length_y = lengths
    smalls_hbm, refs = refs[:8], refs[8:]
    shards, refs = refs[:9], refs[9:]
    sink_ref, mixed_ref, log_ref = refs[:3]
    smalls, refs = refs[3:11], refs[11:]
    small_sem, a_ref, b_ref, normed = refs[:4]
    gather_refs, refs = refs[4:9], refs[9:]
    flow_sems, refs = (refs[0:4], refs[4:8]), refs[8:]
    incoming, window_ref, gate_ref = refs[:3]
    conv_refs, refs = refs[3:8], refs[8:]
    middle_refs, finish_refs = refs[:29], refs[29:]
    gain_ref, step_ref, taps_x, taps_b, taps_c, rate_ref, freq_ref, group_gain_ref = smalls
    z, y, c = (lax.axis_index(a) for a in SP)
    t = lax.axis_index("tp")
    n = lax.axis_size("tp")
    flat = (z * length_y + y) * 2 + c
    count = length_z * length_y * 2
    peers = [{SP[2]: 1 - c}]
    peers += [{SP[1]: lax.rem(y + k, length_y)} for k in range(1, length_y)]
    peers += [{SP[0]: lax.rem(z + k, length_z)} for k in range(1, length_z)]
    peers += [{"tp": lax.rem(t + k, n)} for k in (1, n - 1)]
    for shift in (1, count - 1):
        index = lax.rem(flat + shift, count)
        peers.append({
            SP[0]: index // (2 * length_y),
            SP[1]: lax.rem(index // 2, length_y),
            SP[2]: lax.rem(index, 2),
        })
    barrier = pltpu.get_barrier_semaphore()
    for peer in peers:
        pl.semaphore_signal(barrier, inc=1, device_id=peer, device_id_type=pl.DeviceIdType.MESH)
    copies = [
        pltpu.make_async_copy(src, dst, small_sem.at[i])
        for i, (src, dst) in enumerate(zip(smalls_hbm, smalls))
    ]
    for copy in copies:
        copy.start()

    def small_copies():
        for copy in copies:
            copy.wait()

    def enter():
        pl.semaphore_wait(barrier, len(peers))

    early, late = (
        Flow(i, {"z": length_z, "y": length_y}, (a_ref, b_ref), flow_sems[i]) for i in range(2)
    )
    gather(
        early, late, small_copies, enter, tok_ref, gain_ref, step_ref, *shards,
        normed, *gather_refs,
    )
    flat_a = a_ref.reshape(length_z * length_y * 64, EARLY)
    flat_b = b_ref.reshape(length_z * length_y * 64, LATE)
    middle(
        late, normed, flat_a, flat_b, taps_x, taps_b, taps_c, rate_ref, freq_ref, sink_ref,
        incoming, window_ref, log_ref, gate_ref, *conv_refs, *middle_refs,
    )
    finish(
        window_ref, flat_b, *conv_refs, incoming, gate_ref, group_gain_ref, mixed_ref, *finish_refs
    )
    early.finish()
    late.finish()


def layer(length_z, length_y, n, tokens, smalls, shards, sinks):
    rows, model = tokens.shape
    channels = HEADS * HEAD_DIM
    width = channels + 2 * STATE
    blocks = rows // BLOCK
    pairs = channels // 128
    tile = (STATE, 128)
    full = (MSG, 128)
    lead = (length_z, length_y, 2, 32)
    flows = [transfers(routes, {"z": length_z, "y": length_y}) for routes in ROUTES]
    part = model // n
    dma = pltpu.SemaphoreType.DMA
    vmem = pltpu.VMEM
    hbm = pl.BlockSpec(memory_space=pl.ANY)
    scratch = [
        *(vmem(s.shape, s.dtype) for s in smalls),
        dma((len(smalls),)),
        vmem((*lead, EARLY), BF16),
        vmem((*lead, LATE), BF16),
        vmem((rows + 2 * HALO, model), BF16),
        vmem((HALO, model), BF16), vmem((HALO, model), BF16), vmem((rows, model), BF16),
        dma((2, 2)), dma((len(shards) + 1,)),
        *(dma((len(part),)) for sends, groups in flows for part in (sends, sends, groups, groups)),
        vmem((2, pairs, *tile), BF16),
        vmem((rows, channels), BF16),
        vmem((rows, channels), BF16),
        vmem((rows, width), BF16),
        vmem((rows, 4 * HEADS), F32),
        vmem((blocks, 4 * HEADS, BLOCK), F32),
        vmem((blocks, STATE, 2 * channels), F32),
        vmem((blocks, 8, 2 * channels), F32),
        vmem((rows + 2 * HALO, width), BF16),
        vmem((rows, 256), BF16),
        vmem((rows, channels), BF16),
        vmem((rows, 128), F32),
        vmem((rows + 2 * HALO, width), F32),
        vmem((BLOCK + 2 * HALO, width), F32),
        vmem((2, pairs, *full), BF16),
        vmem((WINDOW, 256), BF16),
        vmem((WINDOW, 256), BF16),
        vmem((2, rows + 2 * BLOCK, 128), BF16),
        vmem((128, rows + 2 * BLOCK), BF16),
        vmem((2, (rows + 2 * WINDOW) // GRID_W, 128), F32),
        vmem((2, GRID_W, 128), F32),
        vmem((pairs, *full), BF16),
        vmem((pairs, *full), BF16),
        vmem((length_y, *full), BF16),
        vmem(full, BF16),
        vmem((length_z, *full), BF16),
        vmem((length_y, *tile), BF16),
        vmem((length_y, *tile), BF16),
        vmem((pairs, *tile), BF16),
        vmem((pairs, *tile), BF16),
        vmem(tile, F32),
        dma((2,)), dma((length_y, 2)), dma((length_z, 2)), dma((length_y, 2)), dma((2,)),
        dma((2, 2)),
        vmem((rows, channels), BF16),
        vmem((blocks, STATE, 2 * channels), BF16),
        vmem((2, blocks, BLOCK, part // 2), BF16),
        vmem((2, blocks, BLOCK, part // 2), BF16),
        vmem((2, blocks, BLOCK, part), BF16),
        vmem((2, blocks, BLOCK, part), BF16),
        dma((2, blocks, 2)), dma((2, blocks, 2)),
    ]
    return pl.pallas_call(
        functools.partial(layer_kernel, (length_z, length_y)),
        in_specs=[hbm] * (1 + len(smalls) + len(shards)) + [pl.BlockSpec(memory_space=pltpu.SMEM)],
        out_specs=[pl.BlockSpec(memory_space=pltpu.VMEM)] * 2,
        out_shape=[
            jax.ShapeDtypeStruct((rows, part), BF16),
            jax.ShapeDtypeStruct((HEADS, rows), F32),
        ],
        scratch_shapes=scratch,
        compiler_params=pltpu.CompilerParams(
            collective_id=1, has_side_effects=True, vmem_limit_bytes=65_800_000
        ),
        cost_estimate=pl.CostEstimate(flops=1 << 33, bytes_accessed=24 << 20, transcendentals=0),
        name="layer",
    )(tokens, *smalls, *shards, sinks)


def flatten_rows(weight):
    return weight.reshape(weight.shape[0], -1)


def shards(
    tokens, input_gain, gate_weight, value_weight, inflow_weight, readout_weight, step_weight,
    conv_values, conv_inflow, conv_readout, log_rate, group_gain, query_weight, key_weight,
    vector_weight, sink_logit, state_out, window_out,
):
    count = tokens.shape[0]
    length_z, length_y = lax.axis_size(SP[0]), lax.axis_size(SP[1])
    quarter = HEAD_DIM // 4
    powers = (np.arange(128) % quarter).astype(np.float32) / np.float32(quarter)
    freqs = np.broadcast_to(np.float32(ROPE_BASE) ** -powers, (8, 128)).astype(np.float32)
    freqs = jnp.asarray(freqs)
    smalls = (
        input_gain.reshape(-1, 128),
        step_weight.transpose(1, 2, 0).reshape(2 * HEADS, -1),
        conv_values, flatten_rows(conv_inflow), flatten_rows(conv_readout),
        log_rate.transpose(0, 2, 1).reshape(2 * HEADS, count),
        freqs,
        group_gain.reshape(-1, 128),
    )
    shards_here = (
        value_weight, flatten_rows(inflow_weight), flatten_rows(readout_weight), key_weight,
        vector_weight, gate_weight, query_weight, state_out.T, window_out.T,
    )
    mixed, logs = layer(
        length_z, length_y, lax.axis_size("tp"), tokens, smalls, shards_here, sink_logit
    )
    return mixed, logs.T


def solution(mesh):
    torus = Mesh(mesh.devices.reshape(8, 4, 2, mesh.shape["tp"]), (*SP, "tp"))
    return jax.shard_map(
        shards,
        mesh=torus,
        in_specs=(
            P(SP, None), P(), P(SP, "tp"), P(SP, "tp"), P(SP, "tp", None), P(SP, "tp", None),
            P(SP, None, "tp"), P(None, "tp"), P(None, "tp", None), P(None, "tp", None),
            P(None, SP, "tp"), P("tp"), P(SP, "tp"), P(SP, "tp"), P(SP, "tp"), P("tp"),
            P("tp", SP), P("tp", SP),
        ),
        out_specs=(P(SP, "tp"), P(SP, "tp")),
        check_vma=False,
    )
```
